512 devices in a mesh: sp: 32 (over z, x), tp: 16 (over y, core).
Axes of the slice: x: 4, y: 8, z: 8, core: 2. Of those that a mesh axis runs over, the one named last changes fastest.
Arguments:
- moe_in: bfloat16 [6144, 2048], P('sp', 'tp'), may hold values from -6 to 6
- cotangent: bfloat16 [6144, 2048], P('sp', 'tp'), may hold values from -6 to 6
- routes: int32 [6144, 2], P('sp'), may hold values from 0 to 31, all different within a row; in each aligned block of 192 rows (0 to 191, 192 to 383, ...) at most 15 rows name the same one
- route_weight: float32 [6144, 2], P('sp'), may hold values from 0.2 to 1
- w_gate: bfloat16 [32, 3584, 2048], P('sp', 'tp'), may hold values from -0.125 to 0.125
- w_up: bfloat16 [32, 3584, 2048], P('sp', 'tp'), may hold values from -0.125 to 0.125
- w_down: bfloat16 [32, 3584, 2048], P('sp', 'tp'), may hold values from -0.09375 to 0.09375
- conv_pre: bfloat16 [6144, 2048], P('sp', 'tp'), may hold values from -6 to 6
- norm_mean: float32 [6144], P('sp'), may hold values from -3 to 3
- norm_rstd: float32 [6144], P('sp'), may hold values from 0.5 to 2
- ln_gain: float32 [2048], P('tp'), may hold values from 0.1 to 1.9
- ln_shift: float32 [2048], P('tp'), may hold values from -3 to 3
- taps: float32 [31, 2048], P(None, 'tp'), may hold values from -1 to 1
- w_proj: bfloat16 [2048, 2048], P('sp', 'tp'), may hold values from -0.125 to 0.125
Outputs:
- grad_up: bfloat16 [32, 3584, 2048], P('sp', 'tp')
- grad_down: bfloat16 [32, 3584, 2048], P('sp', 'tp')
- grad_stream: bfloat16 [6144, 2048], P('sp', 'tp')
- grad_proj: float32 [2048, 2048], P('sp', 'tp')
- grad_conv: bfloat16 [6144, 2048], P('sp', 'tp')
The draws below stay inside these ranges and needn't reach their ends.
Inputs may be any that keep to these rules, and one draw needn't show every extreme that they name: `routes`: each token names 2 different experts. Among the tokens of one index of sp no expert is named more than 15 times, a bound that some block reaches.
All inputs are finite; a program needn't handle non-finite values.
Results may differ from the reference program's by a relative error of at most 0.02.
Values may be sent and summed in bfloat16 or wider, within the bound.
No kernel may reach another device: no remote copies, remote signals or barrier semaphores. Data moves between devices by JAX's collectives and lax.ppermute only.
A program may use at most 64 MiB of HBM per device.

```python
import math
import jax
import jax.numpy as jnp
import numpy as np
from jax import lax

D = 2048
FF_E = 3584
KW = 31
TOP = 2
TOK_DEV = 192
EXPERTS = 32
CAP = 15
TOKENS = 6144
N_SP = 32
N_TP = 16


def raised(drawn, key, source, target, shards_of, factor):
    owner, partner = [(jnp.arange(drawn.shape[dim]) // (drawn.shape[dim] // shards_of)).reshape([-1 if axis == dim else 1 for axis in range(drawn.ndim)]) for dim in (source, target)]
    chosen = jax.random.permutation(key, shards_of)[partner]
    strong = (owner == chosen) | (owner == (partner + shards_of // 2) % shards_of)
    return jnp.where(strong, factor * drawn, drawn)


def level_of(stream_key, shape, shards, low, top_value):
    level, own = 1.0, jax.random.fold_in(stream_key, 6)
    for position, shards_of in shards:
        heights = jnp.exp(jax.random.uniform(jax.random.fold_in(own, position), (shards_of,), jnp.float32, low / len(shards), top_value / len(shards)))
        level = level * jnp.repeat(heights, shape[position] // shards_of).reshape([-1 if axis == position else 1 for axis in range(len(shape))])
    return level


def routed_block(stream_key, own, number, rows, count, top, bound, skew):
    sequence = jax.random.permutation(stream_key, count)
    crowded, common = load_shares(count, rows * top, bound, skew, True), load_shares(count, rows * top, bound, skew, False)
    places = jnp.arange(count)

    def named(lengths, turn):
        used = int((lengths > 0).sum())
        fixed = max(1, used // 4)
        passed = fixed + (places - fixed + turn * (used - fixed)) % max(1, count - fixed)
        return jnp.zeros((count,), jnp.int32).at[sequence[jnp.where(places < fixed, places, passed)]].set(jnp.asarray(lengths, jnp.int32))

    lengths = jnp.where(number % 4 == 0, named(crowded, number // 4), named(common, number - number // 4 - 1))
    mixed = jax.random.permutation(jax.random.fold_in(own, 3), count)
    giver, sink = mixed[0:count // 2 * 2:2], mixed[1:count // 2 * 2:2]
    slack = jnp.minimum(lengths[giver] - 1, bound - lengths[sink]) // 2
    slack = jnp.where((giver == sequence[0]) | (sink == sequence[0]) | (lengths[sink] == 0), 0, jnp.maximum(slack, 0))
    passed = jax.random.randint(jax.random.fold_in(own, 4), (count // 2,), 0, 1 << 20) % (slack + 1)
    lengths = lengths.at[giver].add(-passed).at[sink].add(passed)
    members = jnp.searchsorted(jnp.cumsum(lengths), jnp.arange(rows * top), side="right").astype(jnp.int32)
    grid = members.reshape(top, rows).T
    grid = grid[jax.random.permutation(jax.random.fold_in(own, 1), rows)]
    turn = jax.random.randint(jax.random.fold_in(own, 2), (rows, 1), 0, top)
    return jnp.take_along_axis(grid, (jnp.arange(top)[None, :] + turn) % top, axis=1)


def load_shares(amount, total, limit, skew, full):
    weights = [(1 << 20) // math.isqrt(rank ** skew) + 1 for rank in range(1, amount + 1)]
    largest = limit if full else min(limit, max(-(-total // amount), total * weights[0] // sum(weights)))
    least = 1 if total - largest >= amount - 1 else 0
    given, spare = [largest] + [least] * (amount - 1), total - largest - least * (amount - 1)
    while spare > 0:
        free = [i for i in range(1, amount) if given[i] < largest] or [i for i in range(1, amount) if given[i] < limit]
        whole, left = sum([weights[i] for i in free]), spare
        for i in free:
            addition = min(limit - given[i], max(1, left * weights[i] // whole), spare)
            given[i] = given[i] + addition
            spare = spare - addition
    return np.array(given)


def normal_values(rng, shape, spread, most, shards=(), held_as=jnp.bfloat16):
    loudness = level_of(rng, shape, shards, -0.22, 0.18) if shards else 1.0
    entries = jax.random.normal(rng, shape, jnp.float32) * spread * loudness
    return jnp.minimum(jnp.maximum(entries, -most), most).astype(held_as)


def heavy_noise(stream_key, shape, deviation, bound, split, heavy, kind=jnp.bfloat16):
    entries = deviation * jax.random.normal(stream_key, shape, jnp.float32)
    if split:
        entries = entries * level_of(stream_key, shape, split, -0.22, 0.18)
    return jnp.clip(raised(entries, jax.random.fold_in(stream_key, 3), *heavy), -bound, bound).astype(kind)


def setup_inputs(seed: int = 0) -> dict:
    key_of = jax.random.split(jax.random.key(seed), 15)
    moe_in = normal_values(key_of[0], (TOKENS, D), 1.0, 6.0, ((0, 32), (1, 16)))
    cotangent = heavy_noise(key_of[1], (TOKENS, D), 1.0, 6.0, ((0, 32), (1, 16)), (0, 1, 32, 2.75))
    routes_keys = jax.random.split(jax.random.fold_in(key_of[2], 1), TOKENS // TOK_DEV)
    routes_turns = jax.random.permutation(jax.random.fold_in(key_of[2], 3), TOKENS // TOK_DEV)
    routes = jax.vmap(lambda own, number: routed_block(jax.random.fold_in(key_of[2], 2), own, number, TOK_DEV, EXPERTS, TOP, CAP, 2))(routes_keys, routes_turns).reshape((TOKENS, TOP))
    route_weight = jnp.clip(0.2 + 0.8 * jax.random.uniform(key_of[3], (TOKENS, TOP), jnp.float32) ** level_of(key_of[3], (TOKENS, TOP), ((0, 32),), -0.2, 0.2), 0.2, 1.0)
    w_gate = normal_values(key_of[4], (EXPERTS, FF_E, D), D ** -0.5, 0.125, ((0, 32), (1, 16)))
    w_up = normal_values(key_of[5], (EXPERTS, FF_E, D), D ** -0.5, 0.125, ((0, 32), (1, 16)))
    w_down = normal_values(key_of[6], (EXPERTS, FF_E, D), FF_E ** -0.5, 0.09375, ((0, 32), (1, 16)))
    conv_pre = normal_values(key_of[7], (TOKENS, D), 1.0, 6.0, ((0, 32), (1, 16)))
    norm_mean = normal_values(key_of[8], (TOKENS,), 0.5, 3.0, ((0, 32),), jnp.float32)
    norm_rstd = jnp.clip(jnp.exp(math.log(2.0) - 1.3862944 * jax.random.uniform(key_of[9], (TOKENS,), jnp.float32) ** level_of(key_of[9], (TOKENS,), ((0, 32),), -0.2, 0.2)), 0.5, 2.0)
    ln_gain = jnp.clip(1.0 + 0.18 * jax.random.normal(key_of[10], (D,), jnp.float32), 0.1, 1.9)
    ln_shift = normal_values(key_of[11], (D,), 0.5, 3.0, ((0, 16),), jnp.float32)
    taps = normal_values(key_of[12], (KW, D), KW ** -0.5, 1.0, ((1, 16),), jnp.float32)
    w_proj = normal_values(key_of[13], (D, D), D ** -0.5, 0.125, ((0, 32), (1, 16)))
    return {"moe_in": moe_in, "cotangent": cotangent, "routes": routes, "route_weight": route_weight, "w_gate": w_gate, "w_up": w_up, "w_down": w_down, "conv_pre": conv_pre, "norm_mean": norm_mean, "norm_rstd": norm_rstd, "ln_gain": ln_gain, "ln_shift": ln_shift, "taps": taps, "w_proj": w_proj}


def silu_slope(pre_value, sigmoid_value):
    return sigmoid_value * (1.0 + pre_value * (1.0 - sigmoid_value))


def expert_backward(packed):
    expert_rows, routed_rows, gate_weight, up_weight, down_weight = packed
    gate_pre = lax.dot_general(expert_rows, gate_weight, (((1,), (1,)), ((), ())), preferred_element_type=jnp.float32)
    up_pre = lax.dot_general(expert_rows, up_weight, (((1,), (1,)), ((), ())), preferred_element_type=jnp.float32)
    gate_sigmoid = jax.nn.sigmoid(gate_pre)
    gate_active = gate_pre * gate_sigmoid
    hidden = (gate_active * up_pre).astype(jnp.bfloat16)
    hidden_grad = lax.dot_general(routed_rows, down_weight, (((1,), (1,)), ((), ())), preferred_element_type=jnp.float32)
    grad_down = lax.dot_general(hidden, routed_rows, (((0,), (0,)), ((), ())), preferred_element_type=jnp.float32).astype(jnp.bfloat16)
    gate_grad = (hidden_grad * up_pre * silu_slope(gate_pre, gate_sigmoid)).astype(jnp.bfloat16)
    up_grad = (hidden_grad * gate_active).astype(jnp.bfloat16)
    grad_up = lax.dot_general(up_grad, expert_rows, (((0,), (0,)), ((), ())), preferred_element_type=jnp.float32).astype(jnp.bfloat16)
    row_count = expert_rows.shape[0]
    block_width = gate_weight.shape[0] // N_TP
    gate_blocks = gate_grad.astype(jnp.float32).reshape(row_count, N_TP, block_width)
    up_blocks = up_grad.astype(jnp.float32).reshape(row_count, N_TP, block_width)
    gate_wblocks = gate_weight.astype(jnp.float32).reshape(N_TP, block_width, D)
    up_wblocks = up_weight.astype(jnp.float32).reshape(N_TP, block_width, D)
    partial_rows = jnp.einsum("rbf,bfd->rbd", gate_blocks, gate_wblocks) + jnp.einsum("rbf,bfd->rbd", up_blocks, up_wblocks)
    partial_low = lax.optimization_barrier(partial_rows.astype(jnp.bfloat16))
    pair_grad = jnp.sum(partial_low.astype(jnp.float32), axis=1).astype(jnp.bfloat16)
    return grad_up, grad_down, pair_grad


def reference(moe_in, cotangent, routes, route_weight, w_gate, w_up, w_down, conv_pre, norm_mean, norm_rstd, ln_gain, ln_shift, taps, w_proj):
    per_expert = N_SP * CAP
    route_count = TOP * TOKENS
    route_ids = routes.reshape(N_SP, TOP * TOK_DEV)
    onehot = (route_ids[:, :, None] == jnp.arange(EXPERTS, dtype=jnp.int32)[None, None, :]).astype(jnp.int32)
    earlier = jnp.cumsum(onehot, axis=1) - onehot
    slot_ids = jnp.sum(earlier * onehot, axis=2)
    sources = jnp.arange(N_SP, dtype=jnp.int32)[:, None]
    targets = (route_ids * per_expert + sources * CAP + slot_ids).reshape(-1).astype(jnp.int32)
    table = jnp.full((EXPERTS * per_expert,), route_count, jnp.int32).at[targets].set(jnp.arange(route_count, dtype=jnp.int32))
    filled = (table < route_count)[:, None]
    route_of_slot = jnp.minimum(table, route_count - 1).astype(jnp.int32)
    routed_all = (route_weight[:, :, None] * cotangent.astype(jnp.float32)[:, None, :]).astype(jnp.bfloat16).reshape(route_count, D)
    zero_value = jnp.zeros((), jnp.bfloat16)
    expert_rows = jnp.where(filled, moe_in[route_of_slot // TOP], zero_value).reshape(EXPERTS, per_expert, D)
    routed_rows = jnp.where(filled, routed_all[route_of_slot], zero_value).reshape(EXPERTS, per_expert, D)
    grad_up, grad_down, pair_grad = lax.map(expert_backward, (expert_rows, routed_rows, w_gate, w_up, w_down))
    returned = pair_grad.reshape(EXPERTS * per_expert, D)[targets].astype(jnp.float32).reshape(TOKENS, TOP, D)
    grad_stream = (cotangent.astype(jnp.float32) + jnp.sum(returned, axis=1)).astype(jnp.bfloat16)
    normed = (conv_pre.astype(jnp.float32) - norm_mean[:, None]) * norm_rstd[:, None]
    pre_act = normed * ln_gain[None, :] + ln_shift[None, :]
    act_sigmoid = jax.nn.sigmoid(pre_act)
    activated = (pre_act * act_sigmoid).astype(jnp.bfloat16)
    act_grad = jnp.dot(grad_stream, w_proj, preferred_element_type=jnp.float32)
    grad_proj = lax.dot_general(grad_stream, activated, (((0,), (0,)), ((), ())), preferred_element_type=jnp.float32)
    normed_grad = act_grad * silu_slope(pre_act, act_sigmoid) * ln_gain[None, :]
    mean_first = jnp.mean(normed_grad, axis=1, keepdims=True)
    mean_second = jnp.mean(normed_grad * normed, axis=1, keepdims=True)
    conv_grad = norm_rstd[:, None] * (normed_grad - mean_first - normed * mean_second)
    padded = jnp.concatenate([conv_grad, jnp.zeros((KW - 1, D), jnp.float32)], axis=0)
    grad_conv = jnp.zeros((TOKENS, D), jnp.float32)
    for lag in range(KW):
        grad_conv = grad_conv + taps[lag][None, :] * padded[lag:lag + TOKENS]
    return grad_up, grad_down, grad_stream, grad_proj, grad_conv.astype(jnp.bfloat16)
```

```python
import functools
import jax
import jax.numpy as jnp
from jax import lax
from jax.experimental import pallas as pl
from jax.experimental.pallas import tpu as pltpu
from jax.sharding import PartitionSpec as P

BF16 = jnp.bfloat16
F32 = jnp.float32


def dot(a, b, a_dim, b_dim):
    return lax.dot_general(a, b, (((a_dim,), (b_dim,)), ((), ())), preferred_element_type=F32)


def silu_slope(pre_value, sigmoid_value):
    return sigmoid_value * (1.0 + pre_value * (1.0 - sigmoid_value))


def whole(count, space=pltpu.VMEM):
    return [pl.BlockSpec(memory_space=space)] * count


def send_body(routes, weights, rows, cotangent, sent, place_out, *, experts, slots):
    top, tokens = routes.shape
    expert = lax.broadcasted_iota(jnp.int32, (experts, tokens), 0)
    named = [(expert == routes[k : k + 1, :]).astype(F32) for k in range(top)]
    before = lax.broadcasted_iota(jnp.int32, (tokens, tokens), 0) < lax.broadcasted_iota(
        jnp.int32, (tokens, tokens), 1
    )
    both = functools.reduce(jnp.add, named)
    earlier = dot(both.astype(BF16), before.astype(F32).astype(BF16), 1, 0)
    position = lax.broadcasted_iota(jnp.int32, (experts * slots, tokens), 0)
    place = jnp.zeros((experts * slots, tokens), F32)
    weight = jnp.zeros((experts * slots, 1), F32)
    for k in range(top):
        slot = jnp.sum(earlier * named[k], axis=0, keepdims=True).astype(jnp.int32)
        hit = (position == routes[k : k + 1, :] * slots + slot).astype(F32)
        place = place + hit
        weight = weight + jnp.sum(hit * weights[k : k + 1, :], axis=1, keepdims=True)
    place = place.astype(BF16)
    place_out[...] = place
    channels = rows.shape[1]
    sent[:, :slots, :] = dot(place, rows[...], 1, 0).astype(BF16).reshape(experts, slots, channels)
    routed = (weight * dot(place, cotangent[...], 1, 0)).astype(BF16)
    sent[:, slots:, :] = routed.reshape(experts, slots, channels)


def send_rows(routes, weights, rows, cotangent, experts, slots):
    tokens, channels = rows.shape
    return pl.pallas_call(
        functools.partial(send_body, experts=experts, slots=slots),
        in_specs=whole(4),
        out_specs=whole(2),
        out_shape=(
            jax.ShapeDtypeStruct((experts, 2 * slots, channels), BF16),
            jax.ShapeDtypeStruct((experts * slots, tokens), BF16),
        ),
        name="send_rows",
    )(routes, weights, rows, cotangent)


def block_of(me, j, blocks):
    half = blocks // 2
    chip = lax.rem(me // 2 + j % half, half)
    core = lax.rem(me, 2)
    return 2 * chip + (core if j < half else 1 - core)


def turn_body(me, *refs, blocks):
    count = (len(refs) - 1) // 2
    sems = refs[-1]
    width = refs[0].shape[2] // blocks
    copies = []
    for n in range(count):
        for j in range(blocks):
            at = pl.multiple_of(block_of(me[0], j, blocks) * width, width)
            copies.append(
                pltpu.make_async_copy(
                    refs[n].at[0, :, pl.ds(at, width)],
                    refs[count + n].at[:, pl.ds(j * width, width)],
                    sems.at[n, j],
                )
            )
    for c in copies:
        c.start()
    for c in copies:
        c.wait()


def turned(me, arrays, blocks):
    return pl.pallas_call(
        functools.partial(turn_body, blocks=blocks),
        in_specs=whole(1, pltpu.SMEM) + whole(len(arrays), pl.ANY),
        out_specs=whole(len(arrays), pl.ANY),
        out_shape=[jax.ShapeDtypeStruct(a.shape[1:], a.dtype) for a in arrays],
        scratch_shapes=[pltpu.SemaphoreType.DMA((len(arrays), blocks))],
        name="turned",
    )(me, *arrays)


def expert_body(*refs, blocks, slots):
    parts = refs[:blocks]
    gate_weight, up_weight, down_weight = refs[blocks : blocks + 3]
    rows, routed, hidden_out, up_out, partial = refs[blocks + 3 :]
    experts, _, width = parts[0].shape
    count = experts * slots
    for j, part in enumerate(parts):
        rows[:, j * width : (j + 1) * width] = part[:, :slots, :].reshape(count, width)
        routed[:, j * width : (j + 1) * width] = part[:, slots:, :].reshape(count, width)
    gate_pre = dot(rows[...], gate_weight[...], 1, 1)
    up_pre = dot(rows[...], up_weight[...], 1, 1)
    hidden_grad = dot(routed[...], down_weight[...], 1, 1)
    gate_sigmoid = jax.nn.sigmoid(gate_pre)
    gate_active = gate_pre * gate_sigmoid
    hidden_out[...] = (gate_active * up_pre).astype(BF16)
    gate_grad = (hidden_grad * up_pre * silu_slope(gate_pre, gate_sigmoid)).astype(BF16)
    up_grad = (hidden_grad * gate_active).astype(BF16)
    up_out[...] = up_grad
    step = 2
    for j in range(0, blocks, step):
        cols = slice(j * width, (j + step) * width)
        both = dot(gate_grad, gate_weight[:, cols], 1, 0) + dot(up_grad, up_weight[:, cols], 1, 0)
        for i in range(step):
            partial[j + i] = both[:, i * width : (i + 1) * width].astype(BF16)


def expert_backward(parts, gate_weight, up_weight, down_weight, slots):
    blocks = len(parts)
    experts, _, width = parts[0].shape
    count = experts * slots
    hidden, channels = gate_weight.shape
    work = 2 * count * hidden * channels
    return pl.pallas_call(
        functools.partial(expert_body, blocks=blocks, slots=slots),
        in_specs=whole(blocks + 3),
        out_specs=whole(5),
        out_shape=(
            jax.ShapeDtypeStruct((count, channels), BF16),
            jax.ShapeDtypeStruct((count, channels), BF16),
            jax.ShapeDtypeStruct((count, hidden), BF16),
            jax.ShapeDtypeStruct((count, hidden), BF16),
            jax.ShapeDtypeStruct((blocks, count, width), BF16),
        ),
        cost_estimate=pl.CostEstimate(
            flops=5 * work, transcendentals=count * hidden, bytes_accessed=12 * 1024 * 1024
        ),
        name="expert_backward",
    )(*parts, gate_weight, up_weight, down_weight)


def weight_grad_body(me, left, right, out, held, sems, *, blocks):
    held[...] = dot(left[...], right[...], 0, 0).astype(BF16)
    width = right.shape[1] // blocks
    copies = []
    for j in range(blocks):
        at = pl.multiple_of(block_of(me[0], j, blocks) * width, width)
        copies.append(
            pltpu.make_async_copy(
                held.at[:, pl.ds(j * width, width)], out.at[0, :, pl.ds(at, width)], sems.at[j]
            )
        )
    for c in copies:
        c.start()
    for c in copies:
        c.wait()


def weight_grad(me, left, right, blocks):
    hidden, channels = (left.shape[1], right.shape[1])
    return pl.pallas_call(
        functools.partial(weight_grad_body, blocks=blocks),
        in_specs=whole(1, pltpu.SMEM) + whole(2),
        out_specs=pl.BlockSpec(memory_space=pl.ANY),
        out_shape=jax.ShapeDtypeStruct((1, hidden, channels), BF16),
        scratch_shapes=[pltpu.VMEM((hidden, channels), BF16), pltpu.SemaphoreType.DMA((blocks,))],
        cost_estimate=pl.CostEstimate(
            flops=2 * left.shape[0] * hidden * channels,
            transcendentals=0,
            bytes_accessed=4 * 1024 * 1024,
        ),
        name="weight_grad",
    )(me, left, right)


def along_chips(value, steps):
    count = lax.axis_size("tp")
    return lax.ppermute(value, "tp", [(t, (t + 2 * steps) % count) for t in range(count)])


def to_other_core(value):
    count = lax.axis_size("tp")
    return lax.ppermute(value, "tp", [(t, t ^ 1) for t in range(count)])


def all_blocks(own):
    chips = lax.axis_size("tp") // 2
    held = {0: own}
    for k in range(1, chips // 2 + 1):
        if k < chips - k:
            held[chips - k] = along_chips(held[(chips - k + 1) % chips], 1)
        held[k] = along_chips(held[k - 1], -1)
    mine = [held[k] for k in range(chips)]
    return mine + [to_other_core(part) for part in mine]


def added_up(partial):
    chips = partial.shape[0] // 2
    other = to_other_core(partial[chips:])

    def block(k):
        return partial[k].astype(F32) + other[k].astype(F32)

    up, down = (None, None)
    for k in range(chips // 2, 0, -1):
        value = block(k) if up is None else block(k) + up.astype(F32)
        up = along_chips(value.astype(BF16), 1)
        if k < chips - k:
            value = block(chips - k) if down is None else block(chips - k) + down.astype(F32)
            down = along_chips(value.astype(BF16), -1)
    return (block(0) + up.astype(F32) + down.astype(F32)).astype(BF16)


def sent_to_all(value, axis):
    copies = jnp.broadcast_to(value, (lax.axis_size(axis), *value.shape))
    return lax.all_to_all(copies, axis, split_axis=0, concat_axis=0, tiled=True)


def on_device(
    moe_in,
    cotangent,
    routes,
    route_weight,
    w_gate,
    w_up,
    w_down,
    conv_pre,
    norm_mean,
    norm_rstd,
    ln_gain,
    ln_shift,
    taps,
    w_proj,
):
    devices = lax.axis_size("sp")
    blocks = lax.axis_size("tp")
    local_tokens = routes.shape[0]
    channels = moe_in.shape[1]
    capacity = 5 * local_tokens // (2 * devices)
    slots = capacity + 1
    me = lax.axis_index("tp").astype(jnp.int32).reshape(1)
    sent, place = send_rows(routes.T, route_weight.T, moe_in, cotangent, devices, slots)
    own = lax.all_to_all(sent, "sp", split_axis=0, concat_axis=0, tiled=True)
    gate_weight, up_weight, down_weight = turned(me, (w_gate, w_up, w_down), blocks)
    parts = all_blocks(own)
    proj_in, _ = lax.optimization_barrier((w_proj, own))
    proj = sent_to_all(proj_in, "sp").reshape(-1, channels)
    rows, routed, hidden, up_grad, partial = expert_backward(
        parts, gate_weight, up_weight, down_weight, slots
    )
    shared = added_up(partial).reshape(devices, slots, channels)
    returned = lax.all_to_all(shared, "sp", split_axis=0, concat_axis=0, tiled=True)
    grad_up = weight_grad(me, up_grad, rows, blocks)
    grad_down = weight_grad(me, hidden, routed, blocks)
    grad_stream = (
        cotangent.astype(F32) + dot(place, returned.reshape(devices * slots, channels), 0, 0)
    ).astype(BF16)
    columns = lax.all_gather(grad_stream, "tp", axis=1, tiled=True)
    normed = (conv_pre.astype(F32) - norm_mean[:, None]) * norm_rstd[:, None]
    pre_act = normed * ln_gain[None, :] + ln_shift[None, :]
    act_sigmoid = jax.nn.sigmoid(pre_act)
    activated = (pre_act * act_sigmoid).astype(BF16)
    proj_part = dot(columns, activated, 0, 0).astype(BF16).reshape(devices, -1, channels)
    proj_parts = lax.all_to_all(proj_part, "sp", split_axis=0, concat_axis=0, tiled=True)
    act_grad = dot(columns, proj, 1, 0)
    normed_grad = act_grad * silu_slope(pre_act, act_sigmoid) * ln_gain[None, :]
    sums = jnp.concatenate([jnp.sum(normed_grad, axis=1), jnp.sum(normed_grad * normed, axis=1)])
    sums = jnp.sum(sent_to_all(sums[None], "tp"), axis=(0, 1))
    first_sum, second_sum = (sums[:local_tokens], sums[local_tokens:])
    width = channels * blocks
    conv_grad = norm_rstd[:, None] * (
        normed_grad - first_sum[:, None] / width - normed * (second_sum[:, None] / width)
    )
    lag_count = taps.shape[0]
    rim_rows = lax.ppermute(
        conv_grad[: lag_count - 1], "sp", [(source, source - 1) for source in range(1, devices)]
    )
    extended = jnp.concatenate([conv_grad, rim_rows], axis=0)
    grad_conv = jnp.zeros((local_tokens, channels), F32)
    for lag in range(lag_count):
        grad_conv = grad_conv + taps[lag][None, :] * extended[lag : lag + local_tokens]
    grad_proj = jnp.sum(proj_parts.astype(F32), axis=0)
    return (grad_up, grad_down, grad_stream, grad_proj, grad_conv.astype(BF16))


def solution(mesh):
    placed = (
        P("sp", "tp"),
        P("sp", "tp"),
        P("sp", None),
        P("sp", None),
        P("sp", "tp", None),
        P("sp", "tp", None),
        P("sp", "tp", None),
        P("sp", "tp"),
        P("sp"),
        P("sp"),
        P("tp"),
        P("tp"),
        P(None, "tp"),
        P("sp", "tp"),
    )
    return jax.shard_map(
        on_device,
        mesh=mesh,
        in_specs=placed,
        out_specs=(
            P("sp", "tp", None),
            P("sp", "tp", None),
            P("sp", "tp"),
            P("sp", "tp"),
            P("sp", "tp"),
        ),
        check_vma=False,
    )
```

```python
import functools
import jax
import jax.numpy as jnp
from jax import lax
from jax.experimental import pallas as pl
from jax.experimental.pallas import tpu as pltpu
from jax.sharding import PartitionSpec as P


BF16 = jnp.bfloat16
F32 = jnp.float32


def dot(a, b, a_dim, b_dim):
    return lax.dot_general(a, b, (((a_dim,), (b_dim,)), ((), ())), preferred_element_type=F32)


def silu_slope(pre_value, sigmoid_value):
    return sigmoid_value * (1.0 + pre_value * (1.0 - sigmoid_value))


def whole(count, space=pltpu.VMEM):
    return [pl.BlockSpec(memory_space=space)] * count


def send_body(routes, weights, rows, cotangent, sent, place_out, *, experts, slots):
    top, tokens = routes.shape
    expert = lax.broadcasted_iota(jnp.int32, (experts, tokens), 0)
    named = [(expert == routes[k : k + 1, :]).astype(F32) for k in range(top)]
    before = lax.broadcasted_iota(jnp.int32, (tokens, tokens), 0) < lax.broadcasted_iota(
        jnp.int32, (tokens, tokens), 1
    )
    both = functools.reduce(jnp.add, named)
    earlier = dot(both.astype(BF16), before.astype(F32).astype(BF16), 1, 0)
    position = lax.broadcasted_iota(jnp.int32, (experts * slots, tokens), 0)
    place = jnp.zeros((experts * slots, tokens), F32)
    weight = jnp.zeros((experts * slots, 1), F32)
    for k in range(top):
        slot = jnp.sum(earlier * named[k], axis=0, keepdims=True).astype(jnp.int32)
        hit = (position == routes[k : k + 1, :] * slots + slot).astype(F32)
        place = place + hit
        weight = weight + jnp.sum(hit * weights[k : k + 1, :], axis=1, keepdims=True)
    place = place.astype(BF16)
    place_out[...] = place
    channels = rows.shape[1]
    sent[:, :slots, :] = dot(place, rows[...], 1, 0).astype(BF16).reshape(experts, slots, channels)
    routed = (weight * dot(place, cotangent[...], 1, 0)).astype(BF16)
    sent[:, slots:, :] = routed.reshape(experts, slots, channels)


def send_rows(routes, weights, rows, cotangent, experts, slots):
    tokens, channels = rows.shape
    return pl.pallas_call(
        functools.partial(send_body, experts=experts, slots=slots),
        in_specs=whole(4),
        out_specs=whole(2),
        out_shape=(
            jax.ShapeDtypeStruct((experts, 2 * slots, channels), BF16),
            jax.ShapeDtypeStruct((experts * slots, tokens), BF16),
        ),
        name="send_rows",
    )(routes, weights, rows, cotangent)


def block_of(me, steps, core, blocks):
    chips = blocks // 2
    mine = lax.rem(me, 2)
    sign = 1 - 2 * mine
    chip = lax.rem(me // 2 + sign * steps + chips, chips)
    return 2 * chip + (mine if core == 0 else 1 - mine)


def places(blocks):
    chips = blocks // 2
    ahead = [(k, core) for k in range(1, chips // 2) for core in (1, 0)]
    behind = [(-k, core) for k in range(1, chips // 2) for core in (0, 1)]
    kept = [(0, 0), (chips // 2, 0), *ahead]
    given = [(0, 1), (chips // 2, 1), *behind]
    return kept, given


def expert_body(me, *refs, blocks, slots):
    chips = blocks // 2
    middle = chips // 2
    parts = refs[: 2 * middle + 2]
    gate_weight, up_weight, down_weight = refs[len(parts) : len(parts) + 3]
    rows, routed, hidden_out, up_out, kept, given = refs[len(parts) + 3 :]
    width = parts[0].shape[-1]
    count = parts[0].shape[-3] * slots

    def columns(place):
        at = block_of(me[0], *place, blocks) * width
        return pl.ds(pl.multiple_of(at, width), width)

    def put(place, part):
        cols = columns(place)
        rows[:, cols] = part[:, :slots, :].reshape(count, width)
        routed[:, cols] = part[:, slots:, :].reshape(count, width)

    for core in (0, 1):
        put((0, core), parts[core])
        put((middle, core), parts[2 + core])
        for k in range(1, middle):
            pair = parts[2 + 2 * k + core]
            for i in (0, 1):
                put((k if core else -k, i ^ core), pair[i])
    gate_pre = dot(rows[...], gate_weight[0], 1, 1)
    up_pre = dot(rows[...], up_weight[0], 1, 1)
    hidden_grad = dot(routed[...], down_weight[0], 1, 1)
    gate_sigmoid = jax.nn.sigmoid(gate_pre)
    gate_active = gate_pre * gate_sigmoid
    hidden_out[...] = (gate_active * up_pre).astype(BF16)
    gate_grad = (hidden_grad * up_pre * silu_slope(gate_pre, gate_sigmoid)).astype(BF16)
    up_grad = (hidden_grad * gate_active).astype(BF16)
    up_out[...] = up_grad
    for out, order in zip((kept, given), places(blocks)):
        for j in range(0, chips, 2):
            gate_cols, up_cols = (
                jnp.concatenate([weight[0, :, columns(order[j + i])] for i in (0, 1)], axis=1)
                for weight in (gate_weight, up_weight)
            )
            both = dot(gate_grad, gate_cols, 1, 0) + dot(up_grad, up_cols, 1, 0)
            for i in (0, 1):
                out[j + i] = both[:, i * width : (i + 1) * width].astype(BF16)


def expert_backward(me, parts, gate_weight, up_weight, down_weight, slots, blocks):
    experts, _, width = parts[0].shape
    count = experts * slots
    _, hidden, channels = gate_weight.shape
    work = 2 * count * hidden * channels
    return pl.pallas_call(
        functools.partial(expert_body, blocks=blocks, slots=slots),
        in_specs=whole(1, pltpu.SMEM) + whole(len(parts) + 3),
        out_specs=whole(6),
        out_shape=(
            jax.ShapeDtypeStruct((count, channels), BF16),
            jax.ShapeDtypeStruct((count, channels), BF16),
            jax.ShapeDtypeStruct((count, hidden), BF16),
            jax.ShapeDtypeStruct((count, hidden), BF16),
            jax.ShapeDtypeStruct((blocks // 2, count, width), BF16),
            jax.ShapeDtypeStruct((blocks // 2, count, width), BF16),
        ),
        cost_estimate=pl.CostEstimate(
            flops=5 * work, transcendentals=count * hidden, bytes_accessed=12 * 1024 * 1024
        ),
        name="expert_backward",
    )(me, *parts, gate_weight, up_weight, down_weight)


def passed_on(value):
    count = lax.axis_size("tp")
    return lax.ppermute(
        value, "tp", [(t, (t + (2 if t % 2 == 0 else count - 2)) % count) for t in range(count)]
    )


def swapped(value, hop):
    count = lax.axis_size("tp")
    return lax.ppermute(value, "tp", [(t, t ^ hop) for t in range(count)])


def to_other_core(value):
    return swapped(value, 1)


def all_blocks(own):
    middle = lax.axis_size("tp") // 4
    other = to_other_core(own)
    pair = jnp.stack([own, other])
    pairs = []
    for _ in range(1, middle):
        pair = passed_on(pair)
        pairs.append((pair, to_other_core(pair)))
    last = passed_on(pair[0])
    shared = to_other_core(last)
    return [own, other, last, shared, *[p for both in pairs for p in both]]


def added_up(kept, given):
    middle = kept.shape[0] // 2
    other = to_other_core(given)

    def pair(k):
        at = slice(2 * k, 2 * k + 2)
        return kept[at].astype(F32) + other[at].astype(F32)

    ends = pair(0)
    arrived = passed_on(ends[1].astype(BF16)).astype(F32)
    for k in range(middle - 1, 0, -1):
        value = pair(k)
        if k == middle - 1:
            value = value + jnp.stack([jnp.zeros_like(arrived), arrived])
        else:
            value = value + arrived
        arrived = passed_on(value.astype(BF16)).astype(F32)
    mine = ends[0] + arrived[1]
    return (mine + to_other_core(arrived[0].astype(BF16)).astype(F32)).astype(BF16)


def sent_to_all(value, axis):
    copies = jnp.broadcast_to(value, (lax.axis_size(axis), *value.shape))
    return lax.all_to_all(copies, axis, split_axis=0, concat_axis=0, tiled=True)


def steps(
    moe_in,
    cotangent,
    routes,
    route_weight,
    w_gate,
    w_up,
    w_down,
    conv_pre,
    norm_mean,
    norm_rstd,
    ln_gain,
    ln_shift,
    taps,
    w_proj,
):
    devices = lax.axis_size("sp")
    blocks = lax.axis_size("tp")
    local_tokens = routes.shape[0]
    channels = moe_in.shape[1]
    capacity = 5 * local_tokens // (2 * devices)
    slots = capacity + 1
    me = lax.axis_index("tp").astype(jnp.int32).reshape(1)
    sent, place = send_rows(routes.T, route_weight.T, moe_in, cotangent, devices, slots)
    own = lax.all_to_all(sent, "sp", split_axis=0, concat_axis=0, tiled=True)
    proj = sent_to_all(w_proj, "sp").reshape(-1, channels)
    parts = all_blocks(own)
    rows, routed, hidden, up_grad, kept, given = expert_backward(
        me, parts, w_gate, w_up, w_down, slots, blocks
    )
    shared = added_up(kept, given)
    shared = shared.reshape(devices, slots, channels)
    returned = lax.all_to_all(shared, "sp", split_axis=0, concat_axis=0, tiled=True)
    grad_up = dot(up_grad, rows, 0, 0).astype(BF16)[None]
    grad_down = dot(hidden, routed, 0, 0).astype(BF16)[None]
    grad_stream = (
        cotangent.astype(F32) + dot(place, returned.reshape(devices * slots, channels), 0, 0)
    ).astype(BF16)
    columns = lax.all_gather(grad_stream, "tp", axis=1, tiled=True)
    normed = (conv_pre.astype(F32) - norm_mean[:, None]) * norm_rstd[:, None]
    pre_act = normed * ln_gain[None, :] + ln_shift[None, :]
    act_sigmoid = jax.nn.sigmoid(pre_act)
    activated = (pre_act * act_sigmoid).astype(BF16)
    proj_part = dot(columns, activated, 0, 0).astype(BF16).reshape(devices, -1, channels)
    proj_parts = lax.all_to_all(proj_part, "sp", split_axis=0, concat_axis=0, tiled=True)
    act_grad = dot(columns, proj, 1, 0)
    normed_grad = act_grad * silu_slope(pre_act, act_sigmoid) * ln_gain[None, :]
    sums = jnp.concatenate([jnp.sum(normed_grad, axis=1), jnp.sum(normed_grad * normed, axis=1)])
    hop = 1
    while hop < blocks:
        sums = sums + swapped(sums, hop)
        hop *= 2
    first_sum, second_sum = (sums[:local_tokens], sums[local_tokens:])
    width = channels * blocks
    conv_grad = norm_rstd[:, None] * (
        normed_grad - first_sum[:, None] / width - normed * (second_sum[:, None] / width)
    )
    lag_count = taps.shape[0]
    rim_rows = lax.ppermute(
        conv_grad[: lag_count - 1], "sp", [(source, source - 1) for source in range(1, devices)]
    )
    extended = jnp.concatenate([conv_grad, rim_rows], axis=0)
    grad_conv = jnp.zeros((local_tokens, channels), F32)
    for lag in range(lag_count):
        grad_conv = grad_conv + taps[lag][None, :] * extended[lag : lag + local_tokens]
    grad_proj = jnp.sum(proj_parts.astype(F32), axis=0)
    return (grad_up, grad_down, grad_stream, grad_proj, grad_conv.astype(BF16))


def solution(mesh):
    placed = (
        P("sp", "tp"),
        P("sp", "tp"),
        P("sp", None),
        P("sp", None),
        P("sp", "tp", None),
        P("sp", "tp", None),
        P("sp", "tp", None),
        P("sp", "tp"),
        P("sp"),
        P("sp"),
        P("tp"),
        P("tp"),
        P(None, "tp"),
        P("sp", "tp"),
    )
    return jax.shard_map(
        steps,
        mesh=mesh,
        in_specs=placed,
        out_specs=(
            P("sp", "tp", None),
            P("sp", "tp", None),
            P("sp", "tp"),
            P("sp", "tp"),
            P("sp", "tp"),
        ),
        check_vma=False,
    )
```

```python
import functools
import jax
import jax.numpy as jnp
from jax import lax
from jax.experimental import pallas as pl
from jax.experimental.pallas import tpu as pltpu
from jax.sharding import PartitionSpec as P


TP = ("chip", "core")
EARLY = 1
BF16 = jnp.bfloat16
F32 = jnp.float32


def dot(a, b, a_dim, b_dim):
    return lax.dot_general(a, b, (((a_dim,), (b_dim,)), ((), ())), preferred_element_type=F32)


def silu_slope(pre_value, sigmoid_value):
    return sigmoid_value * (1.0 + pre_value * (1.0 - sigmoid_value))


def whole(count, space=pltpu.VMEM):
    return [pl.BlockSpec(memory_space=space)] * count


def send_body(routes, weights, rows, cotangent, sent, place_out, *, experts, slots):
    top, tokens = routes.shape
    expert = lax.broadcasted_iota(jnp.int32, (experts, tokens), 0)
    named = [(expert == routes[k : k + 1, :]).astype(F32) for k in range(top)]
    before = lax.broadcasted_iota(jnp.int32, (tokens, tokens), 0) < lax.broadcasted_iota(
        jnp.int32, (tokens, tokens), 1
    )
    both = functools.reduce(jnp.add, named)
    earlier = dot(both.astype(BF16), before.astype(F32).astype(BF16), 1, 0)
    position = lax.broadcasted_iota(jnp.int32, (experts * slots, tokens), 0)
    place = jnp.zeros((experts * slots, tokens), F32)
    weight = jnp.zeros((experts * slots, 1), F32)
    for k in range(top):
        slot = jnp.sum(earlier * named[k], axis=0, keepdims=True).astype(jnp.int32)
        hit = (position == routes[k : k + 1, :] * slots + slot).astype(F32)
        place = place + hit
        weight = weight + jnp.sum(hit * weights[k : k + 1, :], axis=1, keepdims=True)
    place = place.astype(BF16)
    place_out[...] = place
    channels = rows.shape[1]
    sent[:, :slots, :] = dot(place, rows[...], 1, 0).astype(BF16).reshape(experts, slots, channels)
    routed = (weight * dot(place, cotangent[...], 1, 0)).astype(BF16)
    sent[:, slots:, :] = routed.reshape(experts, slots, channels)


def send_rows(routes, weights, rows, cotangent, experts, slots):
    tokens, channels = rows.shape
    return pl.pallas_call(
        functools.partial(send_body, experts=experts, slots=slots),
        in_specs=whole(4),
        out_specs=whole(2),
        out_shape=(
            jax.ShapeDtypeStruct((experts, 2 * slots, channels), BF16),
            jax.ShapeDtypeStruct((experts * slots, tokens), BF16),
        ),
        name="send_rows",
    )(routes, weights, rows, cotangent)


def expert_body(me, *refs, blocks, slots):
    chips = blocks // 2
    mine, shared = (refs[:chips], refs[chips : chips + 2])
    gate_weight, up_weight, down_weight = refs[chips + 2 : chips + 5]
    rows, routed, hidden_out, up_out, kept, given = refs[chips + 5 :]
    width = mine[0].shape[-1]
    count = mine[0].shape[-3] * slots
    my_chip, my_core = (me[0] // 2, lax.rem(me[0], 2))

    def columns(chip, core):
        return pl.ds(pl.multiple_of((2 * chip + core) * width, width), width)

    def put(cols, part):
        rows[:, cols] = part[:, :slots, :].reshape(count, width)
        routed[:, cols] = part[:, slots:, :].reshape(count, width)

    early = 2 * EARLY + 1
    for n, steps in enumerate(ring_order(chips)):
        chip = lax.rem(my_chip + steps + chips, chips)
        put(columns(chip, my_core), mine[n])
        batch, at = (shared[0], n) if n < early else (shared[1], n - early)
        put(columns(chip, 1 - my_core), batch[at])
    gate_pre = dot(rows[...], gate_weight[0], 1, 1)
    up_pre = dot(rows[...], up_weight[0], 1, 1)
    hidden_grad = dot(routed[...], down_weight[0], 1, 1)
    gate_sigmoid = jax.nn.sigmoid(gate_pre)
    gate_active = gate_pre * gate_sigmoid
    hidden_out[...] = (gate_active * up_pre).astype(BF16)
    gate_grad = (hidden_grad * up_pre * silu_slope(gate_pre, gate_sigmoid)).astype(BF16)
    up_grad = (hidden_grad * gate_active).astype(BF16)
    up_out[...] = up_grad
    for out, core in ((given, 1 - my_core), (kept, my_core)):
        for j in range(0, chips, 2):
            gate_cols, up_cols = (
                jnp.concatenate([weight[0, :, columns(j + i, core)] for i in (0, 1)], axis=1)
                for weight in (gate_weight, up_weight)
            )
            both = dot(gate_grad, gate_cols, 1, 0) + dot(up_grad, up_cols, 1, 0)
            for i in (0, 1):
                out[j + i] = both[:, i * width : (i + 1) * width].astype(BF16)


def expert_backward(me, parts, gate_weight, up_weight, down_weight, slots, blocks):
    experts, _, width = parts[0].shape
    count = experts * slots
    _, hidden, channels = gate_weight.shape
    work = 2 * count * hidden * channels
    return pl.pallas_call(
        functools.partial(expert_body, blocks=blocks, slots=slots),
        in_specs=whole(1, pltpu.SMEM) + whole(len(parts) + 3),
        out_specs=whole(6),
        out_shape=(
            jax.ShapeDtypeStruct((count, channels), BF16),
            jax.ShapeDtypeStruct((count, channels), BF16),
            jax.ShapeDtypeStruct((count, hidden), BF16),
            jax.ShapeDtypeStruct((count, hidden), BF16),
            jax.ShapeDtypeStruct((blocks // 2, count, width), BF16),
            jax.ShapeDtypeStruct((blocks // 2, count, width), BF16),
        ),
        cost_estimate=pl.CostEstimate(
            flops=5 * work, transcendentals=count * hidden, bytes_accessed=12 * 1024 * 1024
        ),
        name="expert_backward",
    )(me, *parts, gate_weight, up_weight, down_weight)


def along_chips(value, steps):
    count = lax.axis_size("chip")
    return lax.ppermute(value, "chip", [(y, (y + steps) % count) for y in range(count)])


def to_other_core(value):
    return lax.ppermute(value, "core", [(0, 1), (1, 0)])


def ring_order(chips):
    return [0, *[k for step in range(1, chips // 2) for k in (-step, step)], -(chips // 2)]


def all_blocks(own):
    chips = lax.axis_size("chip")
    arrived = [own]
    for n, steps in enumerate(ring_order(chips)[1:]):
        arrived.append(along_chips(arrived[max(0, n - 1)], 1 if steps < 0 else -1))
    early = 2 * EARLY + 1
    first = to_other_core(jnp.stack(arrived[:early]))
    second = to_other_core(jnp.stack(arrived[early:]))
    return [*arrived, first, second]


def added_up(kept, given):
    both = kept.astype(F32) + to_other_core(given).astype(F32)
    arrived = lax.all_to_all(both.astype(BF16), "chip", split_axis=0, concat_axis=0, tiled=True)
    return jnp.sum(arrived.astype(F32), axis=0).astype(BF16)


def sent_to_all(value, axis):
    copies = jnp.broadcast_to(value, (lax.axis_size(axis), *value.shape))
    return lax.all_to_all(copies, axis, split_axis=0, concat_axis=0, tiled=True)


def steps(
    moe_in,
    cotangent,
    routes,
    route_weight,
    w_gate,
    w_up,
    w_down,
    conv_pre,
    norm_mean,
    norm_rstd,
    ln_gain,
    ln_shift,
    taps,
    w_proj,
):
    devices = lax.axis_size("sp")
    blocks = lax.axis_size(TP)
    local_tokens = routes.shape[0]
    channels = moe_in.shape[1]
    capacity = 5 * local_tokens // (2 * devices)
    slots = capacity + 1
    me = lax.axis_index(TP).astype(jnp.int32).reshape(1)
    sent, place = send_rows(routes.T, route_weight.T, moe_in, cotangent, devices, slots)
    own = lax.all_to_all(sent, "sp", split_axis=0, concat_axis=0, tiled=True)
    proj = sent_to_all(w_proj, "sp").reshape(-1, channels)
    parts = all_blocks(own)
    rows, routed, hidden, up_grad, kept, given = expert_backward(
        me, parts, w_gate, w_up, w_down, slots, blocks
    )
    shared = added_up(kept, given)
    shared = shared.reshape(devices, slots, channels)
    returned = lax.all_to_all(shared, "sp", split_axis=0, concat_axis=0, tiled=True)
    grad_up = dot(up_grad, rows, 0, 0).astype(BF16)[None]
    grad_down = dot(hidden, routed, 0, 0).astype(BF16)[None]
    grad_stream = (
        cotangent.astype(F32) + dot(place, returned.reshape(devices * slots, channels), 0, 0)
    ).astype(BF16)
    columns = lax.all_gather(grad_stream, TP, axis=1, tiled=True)
    normed = (conv_pre.astype(F32) - norm_mean[:, None]) * norm_rstd[:, None]
    pre_act = normed * ln_gain[None, :] + ln_shift[None, :]
    act_sigmoid = jax.nn.sigmoid(pre_act)
    activated = (pre_act * act_sigmoid).astype(BF16)
    proj_part = dot(columns, activated, 0, 0).astype(BF16).reshape(devices, -1, channels)
    proj_parts = lax.all_to_all(proj_part, "sp", split_axis=0, concat_axis=0, tiled=True)
    act_grad = dot(columns, proj, 1, 0)
    normed_grad = act_grad * silu_slope(pre_act, act_sigmoid) * ln_gain[None, :]
    sums = jnp.concatenate([jnp.sum(normed_grad, axis=1), jnp.sum(normed_grad * normed, axis=1)])
    sums = sent_to_all(sums[None], TP)
    sums = jnp.sum(sums, axis=(0, 1))
    first_sum, second_sum = (sums[:local_tokens], sums[local_tokens:])
    width = channels * blocks
    conv_grad = norm_rstd[:, None] * (
        normed_grad - first_sum[:, None] / width - normed * (second_sum[:, None] / width)
    )
    lag_count = taps.shape[0]
    rim_rows = lax.ppermute(
        conv_grad[: lag_count - 1], "sp", [(source, source - 1) for source in range(1, devices)]
    )
    extended = jnp.concatenate([conv_grad, rim_rows], axis=0)
    grad_conv = jnp.zeros((local_tokens, channels), F32)
    for lag in range(lag_count):
        grad_conv = grad_conv + taps[lag][None, :] * extended[lag : lag + local_tokens]
    grad_proj = jnp.sum(proj_parts.astype(F32), axis=0)
    return (grad_up, grad_down, grad_stream, grad_proj, grad_conv.astype(BF16))


def solution(mesh):
    placed = (
        P("sp", TP),
        P("sp", TP),
        P("sp", None),
        P("sp", None),
        P("sp", TP, None),
        P("sp", TP, None),
        P("sp", TP, None),
        P("sp", TP),
        P("sp"),
        P("sp"),
        P(TP),
        P(TP),
        P(None, TP),
        P("sp", TP),
    )
    lines = jax.sharding.Mesh(
        mesh.devices.reshape(mesh.devices.shape[0], -1, 2), ("sp", "chip", "core")
    )
    return jax.shard_map(
        steps,
        mesh=lines,
        in_specs=placed,
        out_specs=(
            P("sp", TP, None),
            P("sp", TP, None),
            P("sp", TP),
            P("sp", TP),
            P("sp", TP),
        ),
        check_vma=False,
    )
```

```python
import functools
import jax
import jax.numpy as jnp
from jax import lax
from jax.experimental import pallas as pl
from jax.experimental.pallas import tpu as pltpu
from jax.sharding import PartitionSpec as P


TP = ("chip", "core")
BATCHES = (3, 2, 2, 1)
EARLY = 2
BF16 = jnp.bfloat16
F32 = jnp.float32


def dot(a, b, a_dim, b_dim):
    return lax.dot_general(a, b, (((a_dim,), (b_dim,)), ((), ())), preferred_element_type=F32)


def silu_slope(pre_value, sigmoid_value):
    return sigmoid_value * (1.0 + pre_value * (1.0 - sigmoid_value))


def near(*arrays):
    return tuple(pltpu.with_memory_space_constraint(a, pltpu.VMEM) for a in arrays)


def whole(count, space=pltpu.VMEM):
    return [pl.BlockSpec(memory_space=space)] * count


def send_body(routes, weights, rows, cotangent, sent, place_out, *, experts, slots):
    top, tokens = routes.shape
    expert = lax.broadcasted_iota(jnp.int32, (experts, tokens), 0)
    named = [(expert == routes[k : k + 1, :]).astype(F32) for k in range(top)]
    before = lax.broadcasted_iota(jnp.int32, (tokens, tokens), 0) < lax.broadcasted_iota(
        jnp.int32, (tokens, tokens), 1
    )
    both = functools.reduce(jnp.add, named)
    earlier = dot(both.astype(BF16), before.astype(F32).astype(BF16), 1, 0)
    position = lax.broadcasted_iota(jnp.int32, (experts * slots, tokens), 0)
    place = jnp.zeros((experts * slots, tokens), F32)
    weight = jnp.zeros((experts * slots, 1), F32)
    for k in range(top):
        slot = jnp.sum(earlier * named[k], axis=0, keepdims=True).astype(jnp.int32)
        hit = (position == routes[k : k + 1, :] * slots + slot).astype(F32)
        place = place + hit
        weight = weight + jnp.sum(hit * weights[k : k + 1, :], axis=1, keepdims=True)
    place = place.astype(BF16)
    place_out[...] = place
    channels = rows.shape[1]
    sent[:, :slots, :] = dot(place, rows[...], 1, 0).astype(BF16).reshape(experts, slots, channels)
    routed = (weight * dot(place, cotangent[...], 1, 0)).astype(BF16)
    sent[:, slots:, :] = routed.reshape(experts, slots, channels)


def send_rows(routes, weights, rows, cotangent, experts, slots):
    tokens, channels = rows.shape
    return pl.pallas_call(
        functools.partial(send_body, experts=experts, slots=slots),
        in_specs=whole(4),
        out_specs=whole(2),
        out_shape=(
            jax.ShapeDtypeStruct((experts, 2 * slots, channels), BF16),
            jax.ShapeDtypeStruct((experts * slots, tokens), BF16),
        ),
        name="send_rows",
    )(routes, weights, rows, cotangent)


def columns(chip, core, width):
    return pl.ds(pl.multiple_of((2 * chip + core) * width, width), width)


def put_blocks(me, steps, mine, others, rows, routed, blocks, slots):
    chips = blocks // 2
    width = mine[0].shape[-1]
    count = mine[0].shape[-3] * slots
    my_chip, my_core = (me[0] // 2, lax.rem(me[0], 2))
    found = []
    for step, part, (batch, at) in zip(steps, mine, others):
        chip = lax.rem(my_chip + step + chips, chips)
        for core, value in ((my_core, part), (1 - my_core, batch.at[at])):
            cols = columns(chip, core, width)
            rows[:, cols] = value[:, :slots, :].reshape(count, width)
            routed[:, cols] = value[:, slots:, :].reshape(count, width)
        found.append(pl.ds(pl.multiple_of(chip * 2 * width, 2 * width), 2 * width))
    return found


def products(rows, routed, weights, found):
    sums = [None] * 3
    for cols in found:
        for n, (left, weight) in enumerate(zip((rows, rows, routed), weights)):
            part = dot(left[:, cols], weight[:, cols], 1, 1)
            sums[n] = part if sums[n] is None else sums[n] + part
    return sums


def first_body(me, *refs, blocks, slots, batches):
    count = sum(batches)
    mine, shared = (refs[:count], refs[count : count + len(batches)])
    weights = refs[count + len(batches) : count + len(batches) + 3]
    rows, routed, *sums, held0, held1, held2 = refs[count + len(batches) + 3 :]
    others = [(batch, at) for batch, size in zip(shared, batches) for at in range(size)]
    held = (held0, held1, held2)
    for weight, keep in zip(weights, held):
        keep[...] = weight[0]
    steps = ring_order(blocks // 2)[:count]
    found = put_blocks(me, steps, mine, others, rows, routed, blocks, slots)
    for out, value in zip(sums, products(rows, routed, held, found)):
        out[...] = value


def first_products(me, mine, shared, weights, slots, blocks):
    batches = [b.shape[0] for b in shared]
    experts, _, _ = mine[0].shape
    count, hidden, channels = (experts * slots, weights[0].shape[1], weights[0].shape[2])
    return pl.pallas_call(
        functools.partial(first_body, blocks=blocks, slots=slots, batches=batches),
        in_specs=whole(1, pltpu.SMEM) + whole(len(mine) + len(shared) + 3),
        out_specs=whole(8),
        out_shape=(
            *[pltpu.VMEM((count, channels), BF16)] * 2,
            *[pltpu.VMEM((count, hidden), F32)] * 3,
            *[pltpu.VMEM((hidden, channels), BF16)] * 3,
        ),
        cost_estimate=pl.CostEstimate(
            flops=4 * count * hidden * channels, transcendentals=0, bytes_accessed=12 * 1024 * 1024
        ),
        compiler_params=pltpu.CompilerParams(vmem_limit_bytes=12 * 1024 * 1024),
        name="first_products",
    )(me, *mine, *shared, *weights)


def rest_body(me, *refs, blocks, slots, batches):
    chips = blocks // 2
    count = sum(batches)
    mine, shared = (refs[:count], refs[count : count + len(batches)])
    _, _, gate_sum, up_sum, down_sum, *weights = refs[count + len(batches) : count + len(batches) + 8]
    rows, routed, hidden_out, up_out, kept, given = refs[count + len(batches) + 8 :]
    others = [(batch, at) for batch, size in zip(shared, batches) for at in range(size)]
    steps = ring_order(chips)[-count:]
    found = put_blocks(me, steps, mine, others, rows, routed, blocks, slots)
    gate_pre, up_pre, hidden_grad = products(rows, routed, weights, found)
    gate_pre = gate_pre + gate_sum[...]
    up_pre = up_pre + up_sum[...]
    hidden_grad = hidden_grad + down_sum[...]
    gate_weight, up_weight = weights[:2]
    width = mine[0].shape[-1]
    my_core = lax.rem(me[0], 2)
    gate_sigmoid = jax.nn.sigmoid(gate_pre)
    gate_active = gate_pre * gate_sigmoid
    hidden_out[...] = (gate_active * up_pre).astype(BF16)
    gate_grad = (hidden_grad * up_pre * silu_slope(gate_pre, gate_sigmoid)).astype(BF16)
    up_grad = (hidden_grad * gate_active).astype(BF16)
    up_out[...] = up_grad
    for out, core in ((given, 1 - my_core), (kept, my_core)):
        for j in range(0, chips, 2):
            gate_cols, up_cols = (
                jnp.concatenate([weight[:, columns(j + i, core, width)] for i in (0, 1)], axis=1)
                for weight in (gate_weight, up_weight)
            )
            both = dot(gate_grad, gate_cols, 1, 0) + dot(up_grad, up_cols, 1, 0)
            for i in (0, 1):
                out[j + i] = both[:, i * width : (i + 1) * width].astype(BF16)


def rest_products(me, mine, shared, early, slots, blocks):
    batches = [b.shape[0] for b in shared]
    count, channels = early[0].shape
    hidden = early[2].shape[1]
    first = 1 + len(mine) + len(shared)
    return pl.pallas_call(
        functools.partial(rest_body, blocks=blocks, slots=slots, batches=batches),
        in_specs=whole(1, pltpu.SMEM) + whole(len(mine) + len(shared) + 8),
        out_specs=whole(6),
        out_shape=(
            *[pltpu.VMEM((count, channels), BF16)] * 2,
            *[pltpu.VMEM((count, hidden), BF16)] * 2,
            *[pltpu.VMEM((blocks // 2, count, channels // blocks), BF16)] * 2,
        ),
        input_output_aliases={first: 0, first + 1: 1},
        cost_estimate=pl.CostEstimate(
            flops=6 * count * hidden * channels,
            transcendentals=count * hidden,
            bytes_accessed=12 * 1024 * 1024,
        ),
        compiler_params=pltpu.CompilerParams(vmem_limit_bytes=12 * 1024 * 1024),
        name="rest_products",
    )(me, *mine, *shared, *near(*early))


def along_chips(value, steps):
    count = lax.axis_size("chip")
    return lax.ppermute(value, "chip", [(y, (y + steps) % count) for y in range(count)])


def to_other_core(value):
    return lax.ppermute(value, "core", [(0, 1), (1, 0)])


def ring_order(chips):
    return [0, *[k for step in range(1, chips // 2) for k in (-step, step)], -(chips // 2)]


def all_blocks(own):
    chips = lax.axis_size("chip")
    arrived = [own]
    for n, steps in enumerate(ring_order(chips)[1:]):
        arrived.append(along_chips(arrived[max(0, n - 1)], 1 if steps < 0 else -1))
    shared, at = ([], 0)
    for size in BATCHES:
        shared.append(to_other_core(jnp.stack(arrived[at : at + size])))
        at += size
    return arrived, shared


def added_up(kept, given):
    both = kept.astype(F32) + to_other_core(given).astype(F32)
    arrived = lax.all_to_all(both.astype(BF16), "chip", split_axis=0, concat_axis=0, tiled=True)
    return jnp.sum(arrived.astype(F32), axis=0).astype(BF16)


def sent_to_all(value, axis):
    copies = jnp.broadcast_to(value, (lax.axis_size(axis), *value.shape))
    return lax.all_to_all(copies, axis, split_axis=0, concat_axis=0, tiled=True)


def steps(
    moe_in,
    cotangent,
    routes,
    route_weight,
    w_gate,
    w_up,
    w_down,
    conv_pre,
    norm_mean,
    norm_rstd,
    ln_gain,
    ln_shift,
    taps,
    w_proj,
):
    devices = lax.axis_size("sp")
    blocks = lax.axis_size(TP)
    local_tokens = routes.shape[0]
    channels = moe_in.shape[1]
    capacity = 5 * local_tokens // (2 * devices)
    slots = capacity + 1
    me = lax.axis_index(TP).astype(jnp.int32).reshape(1)
    sent, place = send_rows(routes.T, route_weight.T, moe_in, cotangent, devices, slots)
    own = lax.all_to_all(sent, "sp", split_axis=0, concat_axis=0, tiled=True)
    proj = sent_to_all(w_proj, "sp").reshape(-1, channels)
    mine, others = all_blocks(own)
    done = sum(BATCHES[:EARLY])
    early = first_products(me, mine[:done], others[:EARLY], (w_gate, w_up, w_down), slots, blocks)
    rows, routed, hidden, up_grad, kept, given = rest_products(
        me, mine[done:], others[EARLY:], early, slots, blocks
    )
    shared = added_up(kept, given)
    shared = shared.reshape(devices, slots, channels)
    returned = lax.all_to_all(shared, "sp", split_axis=0, concat_axis=0, tiled=True)
    grad_up = dot(up_grad, rows, 0, 0).astype(BF16)[None]
    grad_down = dot(hidden, routed, 0, 0).astype(BF16)[None]
    grad_stream = (
        cotangent.astype(F32) + dot(place, returned.reshape(devices * slots, channels), 0, 0)
    ).astype(BF16)
    columns = lax.all_gather(grad_stream, TP, axis=1, tiled=True)
    normed = (conv_pre.astype(F32) - norm_mean[:, None]) * norm_rstd[:, None]
    pre_act = normed * ln_gain[None, :] + ln_shift[None, :]
    act_sigmoid = jax.nn.sigmoid(pre_act)
    activated = (pre_act * act_sigmoid).astype(BF16)
    proj_part = dot(columns, activated, 0, 0).astype(BF16).reshape(devices, -1, channels)
    proj_parts = lax.all_to_all(proj_part, "sp", split_axis=0, concat_axis=0, tiled=True)
    act_grad = dot(columns, proj, 1, 0)
    normed_grad = act_grad * silu_slope(pre_act, act_sigmoid) * ln_gain[None, :]
    sums = jnp.concatenate([jnp.sum(normed_grad, axis=1), jnp.sum(normed_grad * normed, axis=1)])
    sums = lax.all_gather(sums, TP, axis=0, tiled=False)
    sums = jnp.sum(sums, axis=0)
    first_sum, second_sum = (sums[:local_tokens], sums[local_tokens:])
    width = channels * blocks
    conv_grad = norm_rstd[:, None] * (
        normed_grad - first_sum[:, None] / width - normed * (second_sum[:, None] / width)
    )
    lag_count = taps.shape[0]
    rim_rows = lax.ppermute(
        conv_grad[: lag_count - 1], "sp", [(source, source - 1) for source in range(1, devices)]
    )
    extended = jnp.concatenate([conv_grad, rim_rows], axis=0)
    grad_conv = jnp.zeros((local_tokens, channels), F32)
    for lag in range(lag_count):
        grad_conv = grad_conv + taps[lag][None, :] * extended[lag : lag + local_tokens]
    grad_proj = jnp.sum(proj_parts.astype(F32), axis=0)
    return (grad_up, grad_down, grad_stream, grad_proj, grad_conv.astype(BF16))


def solution(mesh):
    placed = (
        P("sp", TP),
        P("sp", TP),
        P("sp", None),
        P("sp", None),
        P("sp", TP, None),
        P("sp", TP, None),
        P("sp", TP, None),
        P("sp", TP),
        P("sp"),
        P("sp"),
        P(TP),
        P(TP),
        P(None, TP),
        P("sp", TP),
    )
    lines = jax.sharding.Mesh(
        mesh.devices.reshape(mesh.devices.shape[0], -1, 2), ("sp", "chip", "core")
    )
    return jax.shard_map(
        steps,
        mesh=lines,
        in_specs=placed,
        out_specs=(
            P("sp", TP, None),
            P("sp", TP, None),
            P("sp", TP),
            P("sp", TP),
            P("sp", TP),
        ),
        check_vma=False,
    )
```

```python
import functools
import jax
import jax.numpy as jnp
from jax import lax
from jax.experimental import pallas as pl
from jax.experimental.pallas import tpu as pltpu
from jax.sharding import PartitionSpec as P


TP = ("chip", "core")
BATCHES = (3, 2, 2, 1)
EARLY = 2
BF16 = jnp.bfloat16
F32 = jnp.float32


def dot(a, b, a_dim, b_dim):
    return lax.dot_general(a, b, (((a_dim,), (b_dim,)), ((), ())), preferred_element_type=F32)


def silu_slope(pre_value, sigmoid_value):
    return sigmoid_value * (1.0 + pre_value * (1.0 - sigmoid_value))


def far(*arrays):
    return tuple(pltpu.with_memory_space_constraint(a, pltpu.HBM) for a in arrays)


def near(*arrays):
    return tuple(pltpu.with_memory_space_constraint(a, pltpu.VMEM) for a in arrays)


def whole(count, space=pltpu.VMEM):
    return [pl.BlockSpec(memory_space=space)] * count


def send_body(routes, weights, rows, cotangent, sent, place_out, *, experts, slots):
    top, tokens = routes.shape
    expert = lax.broadcasted_iota(jnp.int32, (experts, tokens), 0)
    named = [(expert == routes[k : k + 1, :]).astype(F32) for k in range(top)]
    before = lax.broadcasted_iota(jnp.int32, (tokens, tokens), 0) < lax.broadcasted_iota(
        jnp.int32, (tokens, tokens), 1
    )
    both = functools.reduce(jnp.add, named)
    earlier = dot(both.astype(BF16), before.astype(F32).astype(BF16), 1, 0)
    position = lax.broadcasted_iota(jnp.int32, (experts * slots, tokens), 0)
    place = jnp.zeros((experts * slots, tokens), F32)
    weight = jnp.zeros((experts * slots, 1), F32)
    for k in range(top):
        slot = jnp.sum(earlier * named[k], axis=0, keepdims=True).astype(jnp.int32)
        hit = (position == routes[k : k + 1, :] * slots + slot).astype(F32)
        place = place + hit
        weight = weight + jnp.sum(hit * weights[k : k + 1, :], axis=1, keepdims=True)
    place = place.astype(BF16)
    place_out[...] = place
    channels = rows.shape[1]
    sent[:, :slots, :] = dot(place, rows[...], 1, 0).astype(BF16).reshape(experts, slots, channels)
    routed = (weight * dot(place, cotangent[...], 1, 0)).astype(BF16)
    sent[:, slots:, :] = routed.reshape(experts, slots, channels)


def send_rows(routes, weights, rows, cotangent, experts, slots):
    tokens, channels = rows.shape
    return pl.pallas_call(
        functools.partial(send_body, experts=experts, slots=slots),
        in_specs=whole(4),
        out_specs=whole(2),
        out_shape=(
            jax.ShapeDtypeStruct((experts, 2 * slots, channels), BF16),
            jax.ShapeDtypeStruct((experts * slots, tokens), BF16),
        ),
        name="send_rows",
    )(routes, weights, rows, cotangent)


def columns(chip, core, width):
    return pl.ds(pl.multiple_of((2 * chip + core) * width, width), width)


def put_blocks(me, steps, mine, others, rows, routed, blocks, slots):
    chips = blocks // 2
    width = mine[0].shape[-1]
    my_chip, my_core = (me[0] // 2, lax.rem(me[0], 2))
    found = []
    for step, part, (batch, at) in zip(steps, mine, others):
        chip = lax.rem(my_chip + step + chips, chips)
        for core, value in ((my_core, part), (1 - my_core, batch.at[at])):
            cols = columns(chip, core, width)
            rows[:, :, cols] = value[:, :slots, :]
            routed[:, :, cols] = value[:, slots:, :]
        found.append(pl.ds(pl.multiple_of(chip * 2 * width, 2 * width), 2 * width))
    return found


def products(rows, routed, weights, found):
    sums = [None] * 3
    for cols in found:
        for n, (left, weight) in enumerate(zip((rows, rows, routed), weights)):
            taken = left[..., cols].reshape(-1, cols.size)
            part = dot(taken, weight[:, cols], 1, 1)
            sums[n] = part if sums[n] is None else sums[n] + part
    return sums


def first_body(me, *refs, blocks, slots, batches):
    chips = blocks // 2
    count = sum(batches)
    mine, shared = (refs[:count], refs[count : count + len(batches)])
    weights = refs[count + len(batches) : count + len(batches) + 3]
    rows, routed, *sums, held0, held1, held2, sems, weight_sems = refs[count + len(batches) + 3 :]
    others = [(batch, at) for batch, size in zip(shared, batches) for at in range(size)]
    held = (held0, held1, held2)
    width = mine[0].shape[-1]
    my_chip, my_core = (me[0] // 2, lax.rem(me[0], 2))
    copies = [
        pltpu.make_async_copy(weight.at[0], keep, weight_sems.at[n])
        for n, (weight, keep) in enumerate(zip(weights, held))
    ]
    found = []
    for n, (step, (batch, at)) in enumerate(zip(ring_order(chips), others)):
        chip = lax.rem(my_chip + step + chips, chips)
        for i, (core, source) in enumerate(((my_core, mine[n]), (1 - my_core, batch.at[at]))):
            cols = columns(chip, core, width)
            for k, target in enumerate((rows, routed)):
                part = source.at[:, pl.ds(k * slots, slots), :]
                copies.append(pltpu.make_async_copy(part, target.at[:, :, cols], sems.at[n, i, k]))
        found.append(pl.ds(pl.multiple_of(chip * 2 * width, 2 * width), 2 * width))
    for copy in copies:
        copy.start()
    for copy in copies:
        copy.wait()
    for out, value in zip(sums, products(rows, routed, held, found)):
        out[...] = value


def first_products(me, mine, shared, weights, slots, blocks):
    batches = [b.shape[0] for b in shared]
    experts, _, _ = mine[0].shape
    count, hidden, channels = (experts * slots, weights[0].shape[1], weights[0].shape[2])
    return pl.pallas_call(
        functools.partial(first_body, blocks=blocks, slots=slots, batches=batches),
        in_specs=whole(1, pltpu.SMEM)
        + whole(len(mine) + len(shared) + 3, pltpu.HBM),
        out_specs=whole(8),
        scratch_shapes=[
            pltpu.SemaphoreType.DMA((len(mine), 2, 2)),
            pltpu.SemaphoreType.DMA((3,)),
        ],
        out_shape=(
            *[pltpu.VMEM((experts, slots, channels), BF16)] * 2,
            *[pltpu.VMEM((count, hidden), F32)] * 3,
            *[pltpu.VMEM((hidden, channels), BF16)] * 3,
        ),
        cost_estimate=pl.CostEstimate(
            flops=4 * count * hidden * channels, transcendentals=0, bytes_accessed=12 * 1024 * 1024
        ),
        compiler_params=pltpu.CompilerParams(vmem_limit_bytes=12 * 1024 * 1024),
        name="first_products",
    )(me, *far(*mine, *shared, *weights))


def rest_body(me, *refs, blocks, slots, batches):
    chips = blocks // 2
    count = sum(batches)
    mine, shared = (refs[:count], refs[count : count + len(batches)])
    _, _, gate_sum, up_sum, down_sum, *weights = refs[count + len(batches) : count + len(batches) + 8]
    outs = refs[count + len(batches) + 8 :]
    rows, routed, kept, given, *far_outs = outs[:8]
    hidden_held, up_held, sems = outs[8:]
    sends = [
        pltpu.make_async_copy(held, out, sems.at[n])
        for n, (held, out) in enumerate(zip((rows, routed, hidden_held, up_held), far_outs))
    ]
    others = [(batch, at) for batch, size in zip(shared, batches) for at in range(size)]
    steps = ring_order(chips)[-count:]
    found = put_blocks(me, steps, mine, others, rows, routed, blocks, slots)
    sends[0].start()
    sends[1].start()
    gate_pre, up_pre, hidden_grad = products(rows, routed, weights, found)
    gate_pre = gate_pre + gate_sum[...]
    up_pre = up_pre + up_sum[...]
    hidden_grad = hidden_grad + down_sum[...]
    gate_weight, up_weight = weights[:2]
    width = mine[0].shape[-1]
    my_core = lax.rem(me[0], 2)
    gate_sigmoid = jax.nn.sigmoid(gate_pre)
    gate_active = gate_pre * gate_sigmoid
    hidden_held[...] = (gate_active * up_pre).astype(BF16)
    gate_grad = (hidden_grad * up_pre * silu_slope(gate_pre, gate_sigmoid)).astype(BF16)
    up_grad = (hidden_grad * gate_active).astype(BF16)
    up_held[...] = up_grad
    sends[2].start()
    sends[3].start()
    for out, core in ((given, 1 - my_core), (kept, my_core)):
        for j in range(0, chips, 2):
            gate_cols, up_cols = (
                jnp.concatenate([weight[:, columns(j + i, core, width)] for i in (0, 1)], axis=1)
                for weight in (gate_weight, up_weight)
            )
            both = dot(gate_grad, gate_cols, 1, 0) + dot(up_grad, up_cols, 1, 0)
            for i in (0, 1):
                out[j + i] = both[:, i * width : (i + 1) * width].astype(BF16)
    for send in sends:
        send.wait()


def rest_products(me, mine, shared, early, slots, blocks):
    batches = [b.shape[0] for b in shared]
    experts, _, channels = early[0].shape
    count, hidden = early[2].shape
    first = 1 + len(mine) + len(shared)
    return pl.pallas_call(
        functools.partial(rest_body, blocks=blocks, slots=slots, batches=batches),
        in_specs=whole(1, pltpu.SMEM) + whole(len(mine) + len(shared) + 8),
        out_specs=whole(4) + whole(4, pl.ANY),
        out_shape=(
            *[pltpu.VMEM((experts, slots, channels), BF16)] * 2,
            *[pltpu.VMEM((blocks // 2, count, channels // blocks), BF16)] * 2,
            *[pltpu.HBM((experts, slots, channels), BF16)] * 2,
            *[pltpu.HBM((count, hidden), BF16)] * 2,
        ),
        scratch_shapes=[pltpu.VMEM((count, hidden), BF16)] * 2 + [pltpu.SemaphoreType.DMA((4,))],
        input_output_aliases={first: 0, first + 1: 1},
        cost_estimate=pl.CostEstimate(
            flops=6 * count * hidden * channels,
            transcendentals=count * hidden,
            bytes_accessed=12 * 1024 * 1024,
        ),
        compiler_params=pltpu.CompilerParams(vmem_limit_bytes=12 * 1024 * 1024),
        name="rest_products",
    )(me, *mine, *shared, *near(*early))


def along_chips(value, steps):
    count = lax.axis_size("chip")
    return lax.ppermute(value, "chip", [(y, (y + steps) % count) for y in range(count)])


def to_other_core(value):
    return lax.ppermute(value, "core", [(0, 1), (1, 0)])


def ring_order(chips):
    return [0, *[k for step in range(1, chips // 2) for k in (-step, step)], -(chips // 2)]


def all_blocks(own):
    chips = lax.axis_size("chip")
    arrived = [own]
    for n, steps in enumerate(ring_order(chips)[1:]):
        arrived.append(along_chips(arrived[max(0, n - 1)], 1 if steps < 0 else -1))
    shared, at = ([], 0)
    for size in BATCHES:
        shared.append(to_other_core(jnp.stack(arrived[at : at + size])))
        at += size
    return arrived, shared


def added_up(kept, given):
    both = kept.astype(F32) + to_other_core(given).astype(F32)
    arrived = lax.all_to_all(both.astype(BF16), "chip", split_axis=0, concat_axis=0, tiled=True)
    return jnp.sum(arrived.astype(F32), axis=0).astype(BF16)


def sent_to_all(value, axis):
    copies = jnp.broadcast_to(value, (lax.axis_size(axis), *value.shape))
    return lax.all_to_all(copies, axis, split_axis=0, concat_axis=0, tiled=True)


def steps(
    moe_in,
    cotangent,
    routes,
    route_weight,
    w_gate,
    w_up,
    w_down,
    conv_pre,
    norm_mean,
    norm_rstd,
    ln_gain,
    ln_shift,
    taps,
    w_proj,
):
    devices = lax.axis_size("sp")
    blocks = lax.axis_size(TP)
    local_tokens = routes.shape[0]
    channels = moe_in.shape[1]
    capacity = 5 * local_tokens // (2 * devices)
    slots = capacity + 1
    me = lax.axis_index(TP).astype(jnp.int32).reshape(1)
    sent, place = send_rows(routes.T, route_weight.T, moe_in, cotangent, devices, slots)
    own = lax.all_to_all(sent, "sp", split_axis=0, concat_axis=0, tiled=True)
    proj = sent_to_all(w_proj, "sp").reshape(-1, channels)
    mine, others = all_blocks(own)
    done = sum(BATCHES[:EARLY])
    early = first_products(me, mine[:done], others[:EARLY], (w_gate, w_up, w_down), slots, blocks)
    _, _, kept, given, rows, routed, hidden, up_grad = rest_products(
        me, mine[done:], others[EARLY:], early, slots, blocks
    )
    shared = added_up(kept, given)
    shared = shared.reshape(devices, slots, channels)
    returned = lax.all_to_all(shared, "sp", split_axis=0, concat_axis=0, tiled=True)
    grad_up = dot(up_grad, rows.reshape(-1, rows.shape[2]), 0, 0).astype(BF16)[None]
    grad_down = dot(hidden, routed.reshape(-1, routed.shape[2]), 0, 0).astype(BF16)[None]
    grad_stream = (
        cotangent.astype(F32) + dot(place, returned.reshape(devices * slots, channels), 0, 0)
    ).astype(BF16)
    columns = lax.all_gather(grad_stream, TP, axis=1, tiled=True)
    normed = (conv_pre.astype(F32) - norm_mean[:, None]) * norm_rstd[:, None]
    pre_act = normed * ln_gain[None, :] + ln_shift[None, :]
    act_sigmoid = jax.nn.sigmoid(pre_act)
    activated = (pre_act * act_sigmoid).astype(BF16)
    proj_part = dot(columns, activated, 0, 0).astype(BF16).reshape(devices, -1, channels)
    proj_parts = lax.all_to_all(proj_part, "sp", split_axis=0, concat_axis=0, tiled=True)
    act_grad = dot(columns, proj, 1, 0)
    normed_grad = act_grad * silu_slope(pre_act, act_sigmoid) * ln_gain[None, :]
    sums = jnp.concatenate([jnp.sum(normed_grad, axis=1), jnp.sum(normed_grad * normed, axis=1)])
    sums = lax.all_gather(sums, TP, axis=0, tiled=False)
    sums = jnp.sum(sums, axis=0)
    first_sum, second_sum = (sums[:local_tokens], sums[local_tokens:])
    width = channels * blocks
    conv_grad = norm_rstd[:, None] * (
        normed_grad - first_sum[:, None] / width - normed * (second_sum[:, None] / width)
    )
    lag_count = taps.shape[0]
    rim_rows = lax.ppermute(
        conv_grad[: lag_count - 1], "sp", [(source, source - 1) for source in range(1, devices)]
    )
    extended = jnp.concatenate([conv_grad, rim_rows], axis=0)
    grad_conv = jnp.zeros((local_tokens, channels), F32)
    for lag in range(lag_count):
        grad_conv = grad_conv + taps[lag][None, :] * extended[lag : lag + local_tokens]
    grad_proj = jnp.sum(proj_parts.astype(F32), axis=0)
    return (grad_up, grad_down, grad_stream, grad_proj, grad_conv.astype(BF16))


def solution(mesh):
    placed = (
        P("sp", TP),
        P("sp", TP),
        P("sp", None),
        P("sp", None),
        P("sp", TP, None),
        P("sp", TP, None),
        P("sp", TP, None),
        P("sp", TP),
        P("sp"),
        P("sp"),
        P(TP),
        P(TP),
        P(None, TP),
        P("sp", TP),
    )
    lines = jax.sharding.Mesh(
        mesh.devices.reshape(mesh.devices.shape[0], -1, 2), ("sp", "chip", "core")
    )
    return jax.shard_map(
        steps,
        mesh=lines,
        in_specs=placed,
        out_specs=(
            P("sp", TP, None),
            P("sp", TP, None),
            P("sp", TP),
            P("sp", TP),
            P("sp", TP),
        ),
        check_vma=False,
    )
```

```python
import functools
import jax
import jax.numpy as jnp
from jax import lax
from jax.experimental import pallas as pl
from jax.experimental.pallas import tpu as pltpu
from jax.sharding import PartitionSpec as P


TP = ("chip", "core")
BATCHES = (3, 2, 2, 1)
EARLY = 2
BF16 = jnp.bfloat16
F32 = jnp.float32


def dot(a, b, a_dim, b_dim):
    return lax.dot_general(a, b, (((a_dim,), (b_dim,)), ((), ())), preferred_element_type=F32)


def silu_slope(pre_value, sigmoid_value):
    return sigmoid_value * (1.0 + pre_value * (1.0 - sigmoid_value))


def far(*arrays):
    return tuple(pltpu.with_memory_space_constraint(a, pltpu.HBM) for a in arrays)


def near(*arrays):
    return tuple(pltpu.with_memory_space_constraint(a, pltpu.VMEM) for a in arrays)


def whole(count, space=pltpu.VMEM):
    return [pl.BlockSpec(memory_space=space)] * count


def send_body(routes, weights, rows, cotangent, sent, place_out, *, experts, slots):
    top, tokens = routes.shape
    expert = lax.broadcasted_iota(jnp.int32, (experts, tokens), 0)
    named = [(expert == routes[k : k + 1, :]).astype(F32) for k in range(top)]
    before = lax.broadcasted_iota(jnp.int32, (tokens, tokens), 0) < lax.broadcasted_iota(
        jnp.int32, (tokens, tokens), 1
    )
    both = functools.reduce(jnp.add, named)
    earlier = dot(both.astype(BF16), before.astype(F32).astype(BF16), 1, 0)
    position = lax.broadcasted_iota(jnp.int32, (experts * slots, tokens), 0)
    place = jnp.zeros((experts * slots, tokens), F32)
    weight = jnp.zeros((experts * slots, 1), F32)
    for k in range(top):
        slot = jnp.sum(earlier * named[k], axis=0, keepdims=True).astype(jnp.int32)
        hit = (position == routes[k : k + 1, :] * slots + slot).astype(F32)
        place = place + hit
        weight = weight + jnp.sum(hit * weights[k : k + 1, :], axis=1, keepdims=True)
    place = place.astype(BF16)
    place_out[...] = place
    channels = rows.shape[1]
    sent[:, :slots, :] = dot(place, rows[...], 1, 0).astype(BF16).reshape(experts, slots, channels)
    routed = (weight * dot(place, cotangent[...], 1, 0)).astype(BF16)
    sent[:, slots:, :] = routed.reshape(experts, slots, channels)


def send_rows(routes, weights, rows, cotangent, experts, slots):
    tokens, channels = rows.shape
    return pl.pallas_call(
        functools.partial(send_body, experts=experts, slots=slots),
        in_specs=whole(4),
        out_specs=whole(2),
        out_shape=(
            jax.ShapeDtypeStruct((experts, 2 * slots, channels), BF16),
            jax.ShapeDtypeStruct((experts * slots, tokens), BF16),
        ),
        name="send_rows",
    )(routes, weights, rows, cotangent)


def columns(chip, core, width):
    return pl.ds(pl.multiple_of((2 * chip + core) * width, width), width)


def put_blocks(me, steps, mine, others, rows, routed, blocks, slots):
    chips = blocks // 2
    width = mine[0].shape[-1]
    my_chip, my_core = (me[0] // 2, lax.rem(me[0], 2))
    found = []
    for step, part, (batch, at) in zip(steps, mine, others):
        chip = lax.rem(my_chip + step + chips, chips)
        for core, value in ((my_core, part), (1 - my_core, batch.at[at])):
            cols = columns(chip, core, width)
            rows[:, :, cols] = value[:, :slots, :]
            routed[:, :, cols] = value[:, slots:, :]
        found.append(pl.ds(pl.multiple_of(chip * 2 * width, 2 * width), 2 * width))
    return found


def products(rows, routed, weights, found):
    sums = [None] * 3
    for cols in found:
        for n, (left, weight) in enumerate(zip((rows, rows, routed), weights)):
            taken = left[..., cols].reshape(-1, cols.size)
            part = dot(taken, weight[:, cols], 1, 1)
            sums[n] = part if sums[n] is None else sums[n] + part
    return sums


def first_body(me, *refs, blocks, slots, batches):
    chips = blocks // 2
    count = sum(batches)
    mine, shared = (refs[:count], refs[count : count + len(batches)])
    weights = refs[count + len(batches) : count + len(batches) + 3]
    rows, routed, *sums, held0, held1, held2, sems, weight_sems = refs[count + len(batches) + 3 :]
    others = [(batch, at) for batch, size in zip(shared, batches) for at in range(size)]
    held = (held0, held1, held2)
    width = mine[0].shape[-1]
    my_chip, my_core = (me[0] // 2, lax.rem(me[0], 2))
    copies = [
        pltpu.make_async_copy(weight.at[0], keep, weight_sems.at[n])
        for n, (weight, keep) in enumerate(zip(weights, held))
    ]
    found = []
    for n, (step, (batch, at)) in enumerate(zip(ring_order(chips), others)):
        chip = lax.rem(my_chip + step + chips, chips)
        for i, (core, source) in enumerate(((my_core, mine[n]), (1 - my_core, batch.at[at]))):
            cols = columns(chip, core, width)
            for k, target in enumerate((rows, routed)):
                part = source.at[:, pl.ds(k * slots, slots), :]
                copies.append(pltpu.make_async_copy(part, target.at[:, :, cols], sems.at[n, i, k]))
        found.append(pl.ds(pl.multiple_of(chip * 2 * width, 2 * width), 2 * width))
    for copy in copies:
        copy.start()
    for copy in copies:
        copy.wait()
    for out, value in zip(sums, products(rows, routed, held, found)):
        out[...] = value


def first_products(me, mine, shared, weights, slots, blocks):
    batches = [b.shape[0] for b in shared]
    experts, _, _ = mine[0].shape
    count, hidden, channels = (experts * slots, weights[0].shape[1], weights[0].shape[2])
    return pl.pallas_call(
        functools.partial(first_body, blocks=blocks, slots=slots, batches=batches),
        in_specs=whole(1, pltpu.SMEM)
        + whole(len(mine) + len(shared) + 3, pltpu.HBM),
        out_specs=whole(8),
        scratch_shapes=[
            pltpu.SemaphoreType.DMA((len(mine), 2, 2)),
            pltpu.SemaphoreType.DMA((3,)),
        ],
        out_shape=(
            *[pltpu.VMEM((experts, slots, channels), BF16)] * 2,
            *[pltpu.VMEM((count, hidden), F32)] * 3,
            *[pltpu.VMEM((hidden, channels), BF16)] * 3,
        ),
        cost_estimate=pl.CostEstimate(
            flops=4 * count * hidden * channels, transcendentals=0, bytes_accessed=12 * 1024 * 1024
        ),
        compiler_params=pltpu.CompilerParams(vmem_limit_bytes=12 * 1024 * 1024),
        name="first_products",
    )(me, *far(*mine, *shared, *weights))


def rest_body(me, *refs, blocks, slots, batches):
    chips = blocks // 2
    count = sum(batches)
    mine, shared = (refs[:count], refs[count : count + len(batches)])
    _, _, gate_sum, up_sum, down_sum, *weights = refs[count + len(batches) : count + len(batches) + 8]
    outs = refs[count + len(batches) + 8 :]
    rows, routed, kept, given, *far_outs = outs[:8]
    hidden_held, up_held, sems = outs[8:]
    sends = [
        pltpu.make_async_copy(held, out, sems.at[n])
        for n, (held, out) in enumerate(zip((rows, routed, hidden_held, up_held), far_outs))
    ]
    others = [(batch, at) for batch, size in zip(shared, batches) for at in range(size)]
    steps = ring_order(chips)[-count:]
    found = put_blocks(me, steps, mine, others, rows, routed, blocks, slots)
    sends[0].start()
    sends[1].start()
    gate_pre, up_pre, hidden_grad = products(rows, routed, weights, found)
    gate_pre = gate_pre + gate_sum[...]
    up_pre = up_pre + up_sum[...]
    hidden_grad = hidden_grad + down_sum[...]
    gate_weight, up_weight = weights[:2]
    width = mine[0].shape[-1]
    my_core = lax.rem(me[0], 2)
    gate_sigmoid = jax.nn.sigmoid(gate_pre)
    gate_active = gate_pre * gate_sigmoid
    hidden_held[...] = (gate_active * up_pre).astype(BF16)
    gate_grad = (hidden_grad * up_pre * silu_slope(gate_pre, gate_sigmoid)).astype(BF16)
    up_grad = (hidden_grad * gate_active).astype(BF16)
    up_held[...] = up_grad
    sends[2].start()
    sends[3].start()
    for out, core in ((given, 1 - my_core), (kept, my_core)):
        for j in range(0, chips, 2):
            gate_cols, up_cols = (
                jnp.concatenate([weight[:, columns(j + i, core, width)] for i in (0, 1)], axis=1)
                for weight in (gate_weight, up_weight)
            )
            both = dot(gate_grad, gate_cols, 1, 0) + dot(up_grad, up_cols, 1, 0)
            for i in (0, 1):
                out[j + i] = both[:, i * width : (i + 1) * width].astype(BF16)
    for send in sends:
        send.wait()


def rest_products(me, mine, shared, early, slots, blocks):
    batches = [b.shape[0] for b in shared]
    experts, _, channels = early[0].shape
    count, hidden = early[2].shape
    first = 1 + len(mine) + len(shared)
    return pl.pallas_call(
        functools.partial(rest_body, blocks=blocks, slots=slots, batches=batches),
        in_specs=whole(1, pltpu.SMEM) + whole(len(mine) + len(shared) + 8),
        out_specs=whole(4) + whole(4, pl.ANY),
        out_shape=(
            *[pltpu.VMEM((experts, slots, channels), BF16)] * 2,
            *[pltpu.VMEM((blocks // 2, count, channels // blocks), BF16)] * 2,
            *[pltpu.HBM((experts, slots, channels), BF16)] * 2,
            *[pltpu.HBM((count, hidden), BF16)] * 2,
        ),
        scratch_shapes=[pltpu.VMEM((count, hidden), BF16)] * 2 + [pltpu.SemaphoreType.DMA((4,))],
        input_output_aliases={first: 0, first + 1: 1},
        cost_estimate=pl.CostEstimate(
            flops=6 * count * hidden * channels,
            transcendentals=count * hidden,
            bytes_accessed=12 * 1024 * 1024,
        ),
        compiler_params=pltpu.CompilerParams(vmem_limit_bytes=12 * 1024 * 1024),
        name="rest_products",
    )(me, *mine, *shared, *near(*early))


def along_chips(value, steps):
    count = lax.axis_size("chip")
    return lax.ppermute(value, "chip", [(y, (y + steps) % count) for y in range(count)])


def to_other_core(value):
    return lax.ppermute(value, "core", [(0, 1), (1, 0)])


def ring_order(chips):
    return [0, *[k for step in range(1, chips // 2) for k in (-step, step)], -(chips // 2)]


def all_blocks(own):
    chips = lax.axis_size("chip")
    arrived = [own]
    for n, steps in enumerate(ring_order(chips)[1:-1]):
        arrived.append(along_chips(arrived[max(0, n - 1)], 1 if steps < 0 else -1))
    half = own.shape[0] // 2
    low = along_chips(arrived[-4][:half], 2)
    high = along_chips(arrived[-3][half:], -2)
    arrived.append(jnp.concatenate([low, high], axis=0))
    shared, at = ([], 0)
    for size in BATCHES:
        shared.append(to_other_core(jnp.stack(arrived[at : at + size])))
        at += size
    return arrived, shared


def added_up(kept, given):
    both = kept.astype(F32) + to_other_core(given).astype(F32)
    arrived = lax.all_to_all(both.astype(BF16), "chip", split_axis=0, concat_axis=0, tiled=True)
    return jnp.sum(arrived.astype(F32), axis=0).astype(BF16)


def sent_to_all(value, axis):
    copies = jnp.broadcast_to(value, (lax.axis_size(axis), *value.shape))
    return lax.all_to_all(copies, axis, split_axis=0, concat_axis=0, tiled=True)


def steps(
    moe_in,
    cotangent,
    routes,
    route_weight,
    w_gate,
    w_up,
    w_down,
    conv_pre,
    norm_mean,
    norm_rstd,
    ln_gain,
    ln_shift,
    taps,
    w_proj,
):
    devices = lax.axis_size("sp")
    blocks = lax.axis_size(TP)
    local_tokens = routes.shape[0]
    channels = moe_in.shape[1]
    capacity = 5 * local_tokens // (2 * devices)
    slots = capacity + 1
    me = lax.axis_index(TP).astype(jnp.int32).reshape(1)
    sent, place = send_rows(routes.T, route_weight.T, moe_in, cotangent, devices, slots)
    own = lax.all_to_all(sent, "sp", split_axis=0, concat_axis=0, tiled=True)
    proj = sent_to_all(w_proj, "sp").reshape(-1, channels)
    mine, others = all_blocks(own)
    done = sum(BATCHES[:EARLY])
    early = first_products(me, mine[:done], others[:EARLY], (w_gate, w_up, w_down), slots, blocks)
    _, _, kept, given, rows, routed, hidden, up_grad = rest_products(
        me, mine[done:], others[EARLY:], early, slots, blocks
    )
    shared = added_up(kept, given)
    shared = shared.reshape(devices, slots, channels)
    returned = lax.all_to_all(shared, "sp", split_axis=0, concat_axis=0, tiled=True)
    grad_up = dot(up_grad, rows.reshape(-1, rows.shape[2]), 0, 0).astype(BF16)[None]
    grad_down = dot(hidden, routed.reshape(-1, routed.shape[2]), 0, 0).astype(BF16)[None]
    grad_stream = (
        cotangent.astype(F32) + dot(place, returned.reshape(devices * slots, channels), 0, 0)
    ).astype(BF16)
    columns = lax.all_gather(grad_stream, TP, axis=1, tiled=True)
    normed = (conv_pre.astype(F32) - norm_mean[:, None]) * norm_rstd[:, None]
    pre_act = normed * ln_gain[None, :] + ln_shift[None, :]
    act_sigmoid = jax.nn.sigmoid(pre_act)
    activated = (pre_act * act_sigmoid).astype(BF16)
    proj_part = dot(columns, activated, 0, 0).astype(BF16).reshape(devices, -1, channels)
    proj_parts = lax.all_to_all(proj_part, "sp", split_axis=0, concat_axis=0, tiled=True)
    act_grad = dot(columns, proj, 1, 0)
    normed_grad = act_grad * silu_slope(pre_act, act_sigmoid) * ln_gain[None, :]
    sums = jnp.concatenate([jnp.sum(normed_grad, axis=1), jnp.sum(normed_grad * normed, axis=1)])
    sums = lax.all_gather(sums, TP, axis=0, tiled=False)
    sums = jnp.sum(sums, axis=0)
    first_sum, second_sum = (sums[:local_tokens], sums[local_tokens:])
    width = channels * blocks
    conv_grad = norm_rstd[:, None] * (
        normed_grad - first_sum[:, None] / width - normed * (second_sum[:, None] / width)
    )
    lag_count = taps.shape[0]
    rim_rows = lax.ppermute(
        conv_grad[: lag_count - 1], "sp", [(source, source - 1) for source in range(1, devices)]
    )
    extended = jnp.concatenate([conv_grad, rim_rows], axis=0)
    grad_conv = jnp.zeros((local_tokens, channels), F32)
    for lag in range(lag_count):
        grad_conv = grad_conv + taps[lag][None, :] * extended[lag : lag + local_tokens]
    grad_proj = jnp.sum(proj_parts.astype(F32), axis=0)
    return (grad_up, grad_down, grad_stream, grad_proj, grad_conv.astype(BF16))


def solution(mesh):
    placed = (
        P("sp", TP),
        P("sp", TP),
        P("sp", None),
        P("sp", None),
        P("sp", TP, None),
        P("sp", TP, None),
        P("sp", TP, None),
        P("sp", TP),
        P("sp"),
        P("sp"),
        P(TP),
        P(TP),
        P(None, TP),
        P("sp", TP),
    )
    lines = jax.sharding.Mesh(
        mesh.devices.reshape(mesh.devices.shape[0], -1, 2), ("sp", "chip", "core")
    )
    return jax.shard_map(
        steps,
        mesh=lines,
        in_specs=placed,
        out_specs=(
            P("sp", TP, None),
            P("sp", TP, None),
            P("sp", TP),
            P("sp", TP),
            P("sp", TP),
        ),
        check_vma=False,
    )
```

```python
import functools
import jax
import jax.numpy as jnp
from jax import lax
from jax.experimental import pallas as pl
from jax.experimental.pallas import tpu as pltpu
from jax.sharding import PartitionSpec as P


TP = ("chip", "core")
BATCHES = (3, 2, 2, 1)
EARLY = 2
BF16 = jnp.bfloat16
F32 = jnp.float32


def dot(a, b, a_dim, b_dim):
    return lax.dot_general(a, b, (((a_dim,), (b_dim,)), ((), ())), preferred_element_type=F32)


def silu_slope(pre_value, sigmoid_value):
    return sigmoid_value * (1.0 + pre_value * (1.0 - sigmoid_value))


def far(*arrays):
    return tuple(pltpu.with_memory_space_constraint(a, pltpu.HBM) for a in arrays)


def near(*arrays):
    return tuple(pltpu.with_memory_space_constraint(a, pltpu.VMEM) for a in arrays)


def whole(count, space=pltpu.VMEM):
    return [pl.BlockSpec(memory_space=space)] * count


def places(routes, weights, experts, slots):
    top, tokens = routes.shape
    expert = lax.broadcasted_iota(jnp.int32, (experts, tokens), 0)
    named = [(expert == routes[k : k + 1, :]).astype(F32) for k in range(top)]
    before = lax.broadcasted_iota(jnp.int32, (tokens, tokens), 0) < lax.broadcasted_iota(
        jnp.int32, (tokens, tokens), 1
    )
    both = functools.reduce(jnp.add, named)
    earlier = dot(both.astype(BF16), before.astype(F32).astype(BF16), 1, 0)
    position = lax.broadcasted_iota(jnp.int32, (experts * slots, tokens), 0)
    place = jnp.zeros((experts * slots, tokens), F32)
    weight = jnp.zeros((experts * slots, 1), F32)
    for k in range(top):
        slot = jnp.sum(earlier * named[k], axis=0, keepdims=True).astype(jnp.int32)
        hit = (position == routes[k : k + 1, :] * slots + slot).astype(F32)
        place = place + hit
        if weights is not None:
            weight = weight + jnp.sum(hit * weights[k : k + 1, :], axis=1, keepdims=True)
    return place, weight


def send_body(routes, weights, rows, cotangent, sent, place_out, *, experts, slots):
    place, weight = places(routes, weights, experts, slots)
    place = place.astype(BF16)
    place_out[...] = place
    channels = rows.shape[1]
    sent[:, :slots, :] = dot(place, rows[...], 1, 0).astype(BF16).reshape(experts, slots, channels)
    routed = (weight * dot(place, cotangent[...], 1, 0)).astype(BF16)
    sent[:, slots:, :] = routed.reshape(experts, slots, channels)


def send_rows(routes, weights, rows, cotangent, experts, slots):
    tokens, channels = rows.shape
    return pl.pallas_call(
        functools.partial(send_body, experts=experts, slots=slots),
        in_specs=whole(4),
        out_specs=whole(2),
        out_shape=(
            jax.ShapeDtypeStruct((experts, 2 * slots, channels), BF16),
            jax.ShapeDtypeStruct((experts * slots, tokens), BF16),
        ),
        name="send_rows",
    )(routes, weights, rows, cotangent)


def rim_body(routes, place_out, *, experts, slots):
    place, _ = places(routes, None, experts, slots)
    place_out[...] = place.astype(BF16)


def rim_places(routes, experts, slots):
    return pl.pallas_call(
        functools.partial(rim_body, experts=experts, slots=slots),
        in_specs=whole(1),
        out_specs=whole(1)[0],
        out_shape=jax.ShapeDtypeStruct((experts * slots, routes.shape[1]), BF16),
        name="rim_places",
    )(routes)


def summed_body(arrived, out):
    experts, both, width = out.shape
    total = functools.reduce(jnp.add, [part[...].astype(F32) for part in [arrived.at[k] for k in range(arrived.shape[0])]])
    total = total.astype(BF16).reshape(experts, both // 2, width)
    out[:, : both // 2, :] = total
    out[: experts - 1, both // 2 :, :] = total[1:]
    out[experts - 1 :, both // 2 :, :] = total[:1]


def summed(arrived, experts):
    _, count, width = arrived.shape
    return pl.pallas_call(
        summed_body,
        in_specs=whole(1),
        out_specs=whole(1)[0],
        out_shape=pltpu.VMEM((experts, 2 * count // experts, width), BF16),
        compiler_params=pltpu.CompilerParams(vmem_limit_bytes=12 * 1024 * 1024),
        name="summed",
    )(arrived)


def combined_body(returned, place, rim_place, cotangent, rim_cotangent, out):
    _, both, width = returned.shape
    tokens = cotangent.shape[0]
    mine = returned[:, : both // 2, :].reshape(-1, width)
    after = returned[:, both // 2 :, :].reshape(-1, width)
    out[:tokens, :] = (cotangent[...].astype(F32) + dot(place[...], mine, 0, 0)).astype(BF16)
    rim = rim_cotangent[...].astype(F32) + dot(rim_place[...], after, 0, 0)
    out[tokens:, :] = rim.astype(BF16)


def combined(returned, place, rim_place, cotangent, rim_cotangent):
    tokens = cotangent.shape[0] + rim_cotangent.shape[0]
    return pl.pallas_call(
        combined_body,
        in_specs=whole(5),
        out_specs=whole(1)[0],
        out_shape=pltpu.VMEM((tokens, cotangent.shape[1]), BF16),
        compiler_params=pltpu.CompilerParams(vmem_limit_bytes=12 * 1024 * 1024),
        name="combined",
    )(returned, place, rim_place, cotangent, rim_cotangent)


def columns(chip, core, width):
    return pl.ds(pl.multiple_of((2 * chip + core) * width, width), width)


def put_blocks(me, steps, mine, others, rows, routed, blocks, slots):
    chips = blocks // 2
    width = mine[0].shape[-1]
    my_chip, my_core = (me[0] // 2, lax.rem(me[0], 2))
    found = []
    for step, part, (batch, at) in zip(steps, mine, others):
        chip = lax.rem(my_chip + step + chips, chips)
        for core, value in ((my_core, part), (1 - my_core, batch.at[at])):
            cols = columns(chip, core, width)
            rows[:, :, cols] = value[:, :slots, :]
            routed[:, :, cols] = value[:, slots:, :]
        found.append(pl.ds(pl.multiple_of(chip * 2 * width, 2 * width), 2 * width))
    return found


def products(rows, routed, weights, found):
    sums = [None] * 3
    for cols in found:
        for n, (left, weight) in enumerate(zip((rows, rows, routed), weights)):
            taken = left[..., cols].reshape(-1, cols.size)
            part = dot(taken, weight[:, cols], 1, 1)
            sums[n] = part if sums[n] is None else sums[n] + part
    return sums


def first_body(me, *refs, blocks, slots, batches):
    chips = blocks // 2
    count = sum(batches)
    mine, shared = (refs[:count], refs[count : count + len(batches)])
    weights = refs[count + len(batches) : count + len(batches) + 3]
    rows, routed, *sums, held0, held1, held2, sems, weight_sems = refs[count + len(batches) + 3 :]
    others = [(batch, at) for batch, size in zip(shared, batches) for at in range(size)]
    held = (held0, held1, held2)
    width = mine[0].shape[-1]
    my_chip, my_core = (me[0] // 2, lax.rem(me[0], 2))
    copies = [
        pltpu.make_async_copy(weight.at[0], keep, weight_sems.at[n])
        for n, (weight, keep) in enumerate(zip(weights, held))
    ]
    found = []
    for n, (step, (batch, at)) in enumerate(zip(ring_order(chips), others)):
        chip = lax.rem(my_chip + step + chips, chips)
        for i, (core, source) in enumerate(((my_core, mine[n]), (1 - my_core, batch.at[at]))):
            cols = columns(chip, core, width)
            for k, target in enumerate((rows, routed)):
                part = source.at[:, pl.ds(k * slots, slots), :]
                copies.append(pltpu.make_async_copy(part, target.at[:, :, cols], sems.at[n, i, k]))
        found.append(pl.ds(pl.multiple_of(chip * 2 * width, 2 * width), 2 * width))
    for copy in copies:
        copy.start()
    for copy in copies:
        copy.wait()
    for out, value in zip(sums, products(rows, routed, held, found)):
        out[...] = value


def first_products(me, mine, shared, weights, slots, blocks):
    batches = [b.shape[0] for b in shared]
    experts, _, _ = mine[0].shape
    count, hidden, channels = (experts * slots, weights[0].shape[1], weights[0].shape[2])
    return pl.pallas_call(
        functools.partial(first_body, blocks=blocks, slots=slots, batches=batches),
        in_specs=whole(1, pltpu.SMEM)
        + whole(len(mine) + len(shared) + 3, pltpu.HBM),
        out_specs=whole(8),
        scratch_shapes=[
            pltpu.SemaphoreType.DMA((len(mine), 2, 2)),
            pltpu.SemaphoreType.DMA((3,)),
        ],
        out_shape=(
            *[pltpu.VMEM((experts, slots, channels), BF16)] * 2,
            *[pltpu.VMEM((count, hidden), F32)] * 3,
            *[pltpu.VMEM((hidden, channels), BF16)] * 3,
        ),
        cost_estimate=pl.CostEstimate(
            flops=4 * count * hidden * channels, transcendentals=0, bytes_accessed=12 * 1024 * 1024
        ),
        compiler_params=pltpu.CompilerParams(vmem_limit_bytes=12 * 1024 * 1024),
        name="first_products",
    )(me, *far(*mine, *shared, *weights))


def rest_body(me, *refs, blocks, slots, batches):
    chips = blocks // 2
    count = sum(batches)
    mine, shared = (refs[:count], refs[count : count + len(batches)])
    _, _, gate_sum, up_sum, down_sum, *weights = refs[count + len(batches) : count + len(batches) + 8]
    outs = refs[count + len(batches) + 8 :]
    rows, routed, kept, given, *far_outs = outs[:8]
    hidden_held, up_held, sems = outs[8:]
    sends = [
        pltpu.make_async_copy(held, out, sems.at[n])
        for n, (held, out) in enumerate(zip((rows, routed, hidden_held, up_held), far_outs))
    ]
    others = [(batch, at) for batch, size in zip(shared, batches) for at in range(size)]
    steps = ring_order(chips)[-count:]
    found = put_blocks(me, steps, mine, others, rows, routed, blocks, slots)
    sends[0].start()
    sends[1].start()
    gate_pre, up_pre, hidden_grad = products(rows, routed, weights, found)
    gate_pre = gate_pre + gate_sum[...]
    up_pre = up_pre + up_sum[...]
    hidden_grad = hidden_grad + down_sum[...]
    gate_weight, up_weight = weights[:2]
    width = mine[0].shape[-1]
    my_core = lax.rem(me[0], 2)
    gate_sigmoid = jax.nn.sigmoid(gate_pre)
    gate_active = gate_pre * gate_sigmoid
    hidden_held[...] = (gate_active * up_pre).astype(BF16)
    gate_grad = (hidden_grad * up_pre * silu_slope(gate_pre, gate_sigmoid)).astype(BF16)
    up_grad = (hidden_grad * gate_active).astype(BF16)
    up_held[...] = up_grad
    sends[2].start()
    sends[3].start()
    for out, core in ((given, 1 - my_core), (kept, my_core)):
        for j in range(0, chips, 2):
            gate_cols, up_cols = (
                jnp.concatenate([weight[:, columns(j + i, core, width)] for i in (0, 1)], axis=1)
                for weight in (gate_weight, up_weight)
            )
            both = dot(gate_grad, gate_cols, 1, 0) + dot(up_grad, up_cols, 1, 0)
            for i in (0, 1):
                out[j + i] = both[:, i * width : (i + 1) * width].astype(BF16)
    for send in sends:
        send.wait()


def rest_products(me, mine, shared, early, slots, blocks):
    batches = [b.shape[0] for b in shared]
    experts, _, channels = early[0].shape
    count, hidden = early[2].shape
    first = 1 + len(mine) + len(shared)
    return pl.pallas_call(
        functools.partial(rest_body, blocks=blocks, slots=slots, batches=batches),
        in_specs=whole(1, pltpu.SMEM) + whole(len(mine) + len(shared) + 8),
        out_specs=whole(4) + whole(4, pl.ANY),
        out_shape=(
            *[pltpu.VMEM((experts, slots, channels), BF16)] * 2,
            *[pltpu.VMEM((blocks // 2, count, channels // blocks), BF16)] * 2,
            *[pltpu.HBM((experts, slots, channels), BF16)] * 2,
            *[pltpu.HBM((count, hidden), BF16)] * 2,
        ),
        scratch_shapes=[pltpu.VMEM((count, hidden), BF16)] * 2 + [pltpu.SemaphoreType.DMA((4,))],
        input_output_aliases={first: 0, first + 1: 1},
        cost_estimate=pl.CostEstimate(
            flops=6 * count * hidden * channels,
            transcendentals=count * hidden,
            bytes_accessed=12 * 1024 * 1024,
        ),
        compiler_params=pltpu.CompilerParams(vmem_limit_bytes=12 * 1024 * 1024),
        name="rest_products",
    )(me, *mine, *shared, *near(*early))


def along_chips(value, steps):
    count = lax.axis_size("chip")
    return lax.ppermute(value, "chip", [(y, (y + steps) % count) for y in range(count)])


def from_after(value):
    count = lax.axis_size("sp")
    return lax.ppermute(value, "sp", [(source, source - 1) for source in range(1, count)])


def to_other_core(value):
    return lax.ppermute(value, "core", [(0, 1), (1, 0)])


def ring_order(chips):
    return [0, *[k for step in range(1, chips // 2) for k in (-step, step)], -(chips // 2)]


def all_blocks(own):
    chips = lax.axis_size("chip")
    arrived = [own]
    for n, steps in enumerate(ring_order(chips)[1:]):
        arrived.append(along_chips(arrived[max(0, n - 1)], 1 if steps < 0 else -1))
    shared, at = ([], 0)
    for size in BATCHES:
        shared.append(to_other_core(jnp.stack(arrived[at : at + size])))
        at += size
    return arrived, shared


def added_up(kept, given):
    both = kept.astype(F32) + to_other_core(given).astype(F32)
    arrived = lax.all_to_all(both.astype(BF16), "chip", split_axis=0, concat_axis=0, tiled=True)
    return arrived


def affine(value, mean, rstd, gain, shift):
    normed = (value.astype(F32) - mean[:, None]) * rstd[:, None]
    return normed, normed * gain[None, :] + shift[None, :]


def sent_to_all(value, axis):
    copies = jnp.broadcast_to(value, (lax.axis_size(axis), *value.shape))
    return lax.all_to_all(copies, axis, split_axis=0, concat_axis=0, tiled=True)


def steps(
    moe_in,
    cotangent,
    routes,
    route_weight,
    w_gate,
    w_up,
    w_down,
    conv_pre,
    norm_mean,
    norm_rstd,
    ln_gain,
    ln_shift,
    taps,
    w_proj,
):
    devices = lax.axis_size("sp")
    blocks = lax.axis_size(TP)
    local_tokens = routes.shape[0]
    channels = moe_in.shape[1]
    capacity = 5 * local_tokens // (2 * devices)
    slots = capacity + 1
    me = lax.axis_index(TP).astype(jnp.int32).reshape(1)
    sent, place = send_rows(routes.T, route_weight.T, moe_in, cotangent, devices, slots)
    own = lax.all_to_all(sent, "sp", split_axis=0, concat_axis=0, tiled=True)
    proj = sent_to_all(w_proj, "sp").reshape(-1, channels)
    mine, others = all_blocks(own)
    done = sum(BATCHES[:EARLY])
    early = first_products(me, mine[:done], others[:EARLY], (w_gate, w_up, w_down), slots, blocks)
    _, _, kept, given, rows, routed, hidden, up_grad = rest_products(
        me, mine[done:], others[EARLY:], early, slots, blocks
    )
    rim = 8 * (-(-(taps.shape[0] - 1) // 8))
    rim_cotangent, rim_pre = from_after(jnp.stack([cotangent[:rim], conv_pre[:rim]]))
    facts = [routes[:rim, 0].astype(F32), routes[:rim, 1].astype(F32)]
    facts = from_after(jnp.stack([*facts, norm_mean[:rim], norm_rstd[:rim]]))
    rim_place = rim_places(facts[:2].astype(jnp.int32), devices, slots)
    shared = summed(added_up(kept, given), devices)
    returned = lax.all_to_all(shared, "sp", split_axis=0, concat_axis=0, tiled=True)
    grad_up = dot(up_grad, rows.reshape(-1, rows.shape[2]), 0, 0).astype(BF16)[None]
    grad_down = dot(hidden, routed.reshape(-1, routed.shape[2]), 0, 0).astype(BF16)[None]
    stream = combined(returned, place, rim_place, cotangent, rim_cotangent)
    grad_stream = stream[:local_tokens]
    columns = lax.all_gather(stream, TP, axis=1, tiled=True)
    own_act = affine(conv_pre, norm_mean, norm_rstd, ln_gain, ln_shift)[1]
    activated = (own_act * jax.nn.sigmoid(own_act)).astype(BF16)
    proj_part = dot(columns[:local_tokens], activated, 0, 0).astype(BF16)
    proj_part = proj_part.reshape(devices, -1, channels)
    proj_parts = lax.all_to_all(proj_part, "sp", split_axis=0, concat_axis=0, tiled=True)
    mean = jnp.concatenate([norm_mean, facts[2]])
    rstd = jnp.concatenate([norm_rstd, facts[3]])
    wide_pre = jnp.concatenate([conv_pre, rim_pre], axis=0)
    normed, pre_act = affine(wide_pre, mean, rstd, ln_gain, ln_shift)
    act_sigmoid = jax.nn.sigmoid(pre_act)
    act_grad = dot(columns, proj, 1, 0)
    normed_grad = act_grad * silu_slope(pre_act, act_sigmoid) * ln_gain[None, :]
    sums = jnp.stack([jnp.sum(normed_grad, axis=1), jnp.sum(normed_grad * normed, axis=1)])
    spare = -sums.shape[1] % 128
    sums = jnp.pad(sums, ((0, 0), (0, spare))).reshape(-1)
    sums = lax.all_gather(sums, TP, axis=0, tiled=False)
    sums = jnp.sum(sums, axis=0)
    first_sum, second_sum = sums.reshape(2, -1)[:, : local_tokens + rim]
    width = channels * blocks
    extended = rstd[:, None] * (
        normed_grad - first_sum[:, None] / width - normed * (second_sum[:, None] / width)
    )
    lag_count = taps.shape[0]
    grad_conv = jnp.zeros((local_tokens, channels), F32)
    for lag in range(lag_count):
        grad_conv = grad_conv + taps[lag][None, :] * extended[lag : lag + local_tokens]
    grad_proj = jnp.sum(proj_parts.astype(F32), axis=0)
    return (grad_up, grad_down, grad_stream, grad_proj, grad_conv.astype(BF16))


def solution(mesh):
    placed = (
        P("sp", TP),
        P("sp", TP),
        P("sp", None),
        P("sp", None),
        P("sp", TP, None),
        P("sp", TP, None),
        P("sp", TP, None),
        P("sp", TP),
        P("sp"),
        P("sp"),
        P(TP),
        P(TP),
        P(None, TP),
        P("sp", TP),
    )
    lines = jax.sharding.Mesh(
        mesh.devices.reshape(mesh.devices.shape[0], -1, 2), ("sp", "chip", "core")
    )
    return jax.shard_map(
        steps,
        mesh=lines,
        in_specs=placed,
        out_specs=(
            P("sp", TP, None),
            P("sp", TP, None),
            P("sp", TP),
            P("sp", TP),
            P("sp", TP),
        ),
        check_vma=False,
    )
```

```python
import functools
import jax
import jax.numpy as jnp
from jax import lax
from jax.experimental import pallas as pl
from jax.experimental.pallas import tpu as pltpu
from jax.sharding import PartitionSpec as P


TP = ("chip", "core")
BATCHES = (3, 2, 2, 1)
EARLY = 2
BF16 = jnp.bfloat16
F32 = jnp.float32


def dot(a, b, a_dim, b_dim):
    return lax.dot_general(a, b, (((a_dim,), (b_dim,)), ((), ())), preferred_element_type=F32)


def silu_slope(pre_value, sigmoid_value):
    return sigmoid_value * (1.0 + pre_value * (1.0 - sigmoid_value))


def far(*arrays):
    return tuple(pltpu.with_memory_space_constraint(a, pltpu.HBM) for a in arrays)


def near(*arrays):
    return tuple(pltpu.with_memory_space_constraint(a, pltpu.VMEM) for a in arrays)


def whole(count, space=pltpu.VMEM):
    return [pl.BlockSpec(memory_space=space)] * count


def places(routes, weights, experts, slots):
    top, tokens = routes.shape
    expert = lax.broadcasted_iota(jnp.int32, (experts, tokens), 0)
    named = [(expert == routes[k : k + 1, :]).astype(F32) for k in range(top)]
    before = lax.broadcasted_iota(jnp.int32, (tokens, tokens), 0) < lax.broadcasted_iota(
        jnp.int32, (tokens, tokens), 1
    )
    both = functools.reduce(jnp.add, named)
    earlier = dot(both.astype(BF16), before.astype(F32).astype(BF16), 1, 0)
    position = lax.broadcasted_iota(jnp.int32, (experts * slots, tokens), 0)
    place = jnp.zeros((experts * slots, tokens), F32)
    weight = jnp.zeros((experts * slots, 1), F32)
    for k in range(top):
        slot = jnp.sum(earlier * named[k], axis=0, keepdims=True).astype(jnp.int32)
        hit = (position == routes[k : k + 1, :] * slots + slot).astype(F32)
        place = place + hit
        if weights is not None:
            weight = weight + jnp.sum(hit * weights[k : k + 1, :], axis=1, keepdims=True)
    return place, weight


def send_body(routes, weights, rows, cotangent, sent, place_out, *, experts, slots):
    place, weight = places(routes, weights, experts, slots)
    place = place.astype(BF16)
    place_out[...] = place
    channels = rows.shape[1]
    sent[:, :slots, :] = dot(place, rows[...], 1, 0).astype(BF16).reshape(experts, slots, channels)
    routed = (weight * dot(place, cotangent[...], 1, 0)).astype(BF16)
    sent[:, slots:, :] = routed.reshape(experts, slots, channels)


def send_rows(routes, weights, rows, cotangent, experts, slots):
    tokens, channels = rows.shape
    return pl.pallas_call(
        functools.partial(send_body, experts=experts, slots=slots),
        in_specs=whole(4),
        out_specs=whole(2),
        out_shape=(
            jax.ShapeDtypeStruct((experts, 2 * slots, channels), BF16),
            jax.ShapeDtypeStruct((experts * slots, tokens), BF16),
        ),
        name="send_rows",
    )(routes, weights, rows, cotangent)


def rim_body(routes, place_out, *, experts, slots):
    place, _ = places(routes, None, experts, slots)
    place_out[...] = place.astype(BF16)


def rim_places(routes, experts, slots):
    return pl.pallas_call(
        functools.partial(rim_body, experts=experts, slots=slots),
        in_specs=whole(1),
        out_specs=whole(1)[0],
        out_shape=pltpu.VMEM((experts * slots, routes.shape[1]), BF16),
        compiler_params=pltpu.CompilerParams(vmem_limit_bytes=12 * 1024 * 1024),
        name="rim_places",
    )(routes)


def summed_body(arrived, out):
    experts, both, width = out.shape
    total = functools.reduce(jnp.add, [part[...].astype(F32) for part in [arrived.at[k] for k in range(arrived.shape[0])]])
    total = total.astype(BF16).reshape(experts, both // 2, width)
    out[:, : both // 2, :] = total
    out[: experts - 1, both // 2 :, :] = total[1:]
    out[experts - 1 :, both // 2 :, :] = total[:1]


def summed(arrived, experts):
    _, count, width = arrived.shape
    return pl.pallas_call(
        summed_body,
        in_specs=whole(1),
        out_specs=whole(1)[0],
        out_shape=pltpu.VMEM((experts, 2 * count // experts, width), BF16),
        compiler_params=pltpu.CompilerParams(vmem_limit_bytes=12 * 1024 * 1024),
        name="summed",
    )(arrived)


def combined_body(returned, place, rim_place, cotangent, rim_cotangent, out, own_out):
    _, both, width = returned.shape
    tokens = cotangent.shape[0]
    mine = returned[:, : both // 2, :].reshape(-1, width)
    after = returned[:, both // 2 :, :].reshape(-1, width)
    own = (cotangent[...].astype(F32) + dot(place[...], mine, 0, 0)).astype(BF16)
    out[:tokens, :] = own
    own_out[...] = own
    rim = rim_cotangent[...].astype(F32) + dot(rim_place[...], after, 0, 0)
    out[tokens:, :] = rim.astype(BF16)


def combined(returned, place, rim_place, cotangent, rim_cotangent):
    tokens = cotangent.shape[0] + rim_cotangent.shape[0]
    return pl.pallas_call(
        combined_body,
        in_specs=whole(5),
        out_specs=whole(2),
        out_shape=(
            pltpu.VMEM((tokens, cotangent.shape[1]), BF16),
            pltpu.VMEM(cotangent.shape, BF16),
        ),
        compiler_params=pltpu.CompilerParams(vmem_limit_bytes=12 * 1024 * 1024),
        name="combined",
    )(returned, place, rim_place, cotangent, rim_cotangent)


def columns(chip, core, width):
    return pl.ds(pl.multiple_of((2 * chip + core) * width, width), width)


def put_blocks(me, steps, mine, others, rows, routed, blocks, slots):
    chips = blocks // 2
    width = mine[0].shape[-1]
    my_chip, my_core = (me[0] // 2, lax.rem(me[0], 2))
    found = []
    for step, part, (batch, at) in zip(steps, mine, others):
        chip = lax.rem(my_chip + step + chips, chips)
        for core, value in ((my_core, part), (1 - my_core, batch.at[at])):
            cols = columns(chip, core, width)
            rows[:, :, cols] = value[:, :slots, :]
            routed[:, :, cols] = value[:, slots:, :]
        found.append(pl.ds(pl.multiple_of(chip * 2 * width, 2 * width), 2 * width))
    return found


def products(rows, routed, weights, found):
    sums = [None] * 3
    for cols in found:
        for n, (left, weight) in enumerate(zip((rows, rows, routed), weights)):
            taken = left[..., cols].reshape(-1, cols.size)
            part = dot(taken, weight[:, cols], 1, 1)
            sums[n] = part if sums[n] is None else sums[n] + part
    return sums


def first_body(me, *refs, blocks, slots, batches):
    chips = blocks // 2
    count = sum(batches)
    mine, shared = (refs[:count], refs[count : count + len(batches)])
    weights = refs[count + len(batches) : count + len(batches) + 3]
    rows, routed, *sums, held0, held1, held2, sems, weight_sems = refs[count + len(batches) + 3 :]
    others = [(batch, at) for batch, size in zip(shared, batches) for at in range(size)]
    held = (held0, held1, held2)
    width = mine[0].shape[-1]
    my_chip, my_core = (me[0] // 2, lax.rem(me[0], 2))
    copies = [
        pltpu.make_async_copy(weight.at[0], keep, weight_sems.at[n])
        for n, (weight, keep) in enumerate(zip(weights, held))
    ]
    found = []
    for n, (step, (batch, at)) in enumerate(zip(ring_order(chips), others)):
        chip = lax.rem(my_chip + step + chips, chips)
        for i, (core, source) in enumerate(((my_core, mine[n]), (1 - my_core, batch.at[at]))):
            cols = columns(chip, core, width)
            for k, target in enumerate((rows, routed)):
                part = source.at[:, pl.ds(k * slots, slots), :]
                copies.append(pltpu.make_async_copy(part, target.at[:, :, cols], sems.at[n, i, k]))
        found.append(pl.ds(pl.multiple_of(chip * 2 * width, 2 * width), 2 * width))
    for copy in copies:
        copy.start()
    for copy in copies:
        copy.wait()
    for out, value in zip(sums, products(rows, routed, held, found)):
        out[...] = value


def first_products(me, mine, shared, weights, slots, blocks):
    batches = [b.shape[0] for b in shared]
    experts, _, _ = mine[0].shape
    count, hidden, channels = (experts * slots, weights[0].shape[1], weights[0].shape[2])
    return pl.pallas_call(
        functools.partial(first_body, blocks=blocks, slots=slots, batches=batches),
        in_specs=whole(1, pltpu.SMEM)
        + whole(len(mine) + len(shared) + 3, pltpu.HBM),
        out_specs=whole(8),
        scratch_shapes=[
            pltpu.SemaphoreType.DMA((len(mine), 2, 2)),
            pltpu.SemaphoreType.DMA((3,)),
        ],
        out_shape=(
            *[pltpu.VMEM((experts, slots, channels), BF16)] * 2,
            *[pltpu.VMEM((count, hidden), F32)] * 3,
            *[pltpu.VMEM((hidden, channels), BF16)] * 3,
        ),
        cost_estimate=pl.CostEstimate(
            flops=4 * count * hidden * channels, transcendentals=0, bytes_accessed=12 * 1024 * 1024
        ),
        compiler_params=pltpu.CompilerParams(vmem_limit_bytes=12 * 1024 * 1024),
        name="first_products",
    )(me, *far(*mine, *shared, *weights))


def rest_body(me, *refs, blocks, slots, batches):
    chips = blocks // 2
    count = sum(batches)
    mine, shared = (refs[:count], refs[count : count + len(batches)])
    _, _, gate_sum, up_sum, down_sum, *weights = refs[count + len(batches) : count + len(batches) + 8]
    outs = refs[count + len(batches) + 8 :]
    rows, routed, kept, given, *far_outs = outs[:8]
    hidden_held, up_held, sems = outs[8:]
    sends = [
        pltpu.make_async_copy(held, out, sems.at[n])
        for n, (held, out) in enumerate(zip((rows, routed, hidden_held, up_held), far_outs))
    ]
    others = [(batch, at) for batch, size in zip(shared, batches) for at in range(size)]
    steps = ring_order(chips)[-count:]
    found = put_blocks(me, steps, mine, others, rows, routed, blocks, slots)
    sends[0].start()
    sends[1].start()
    gate_pre, up_pre, hidden_grad = products(rows, routed, weights, found)
    gate_pre = gate_pre + gate_sum[...]
    up_pre = up_pre + up_sum[...]
    hidden_grad = hidden_grad + down_sum[...]
    gate_weight, up_weight = weights[:2]
    width = mine[0].shape[-1]
    my_core = lax.rem(me[0], 2)
    gate_sigmoid = jax.nn.sigmoid(gate_pre)
    gate_active = gate_pre * gate_sigmoid
    hidden_held[...] = (gate_active * up_pre).astype(BF16)
    gate_grad = (hidden_grad * up_pre * silu_slope(gate_pre, gate_sigmoid)).astype(BF16)
    up_grad = (hidden_grad * gate_active).astype(BF16)
    up_held[...] = up_grad
    sends[2].start()
    sends[3].start()
    for out, core in ((given, 1 - my_core), (kept, my_core)):
        for j in range(0, chips, 2):
            gate_cols, up_cols = (
                jnp.concatenate([weight[:, columns(j + i, core, width)] for i in (0, 1)], axis=1)
                for weight in (gate_weight, up_weight)
            )
            both = dot(gate_grad, gate_cols, 1, 0) + dot(up_grad, up_cols, 1, 0)
            for i in (0, 1):
                out[j + i] = both[:, i * width : (i + 1) * width].astype(BF16)
    for send in sends:
        send.wait()


def rest_products(me, mine, shared, early, slots, blocks):
    batches = [b.shape[0] for b in shared]
    experts, _, channels = early[0].shape
    count, hidden = early[2].shape
    first = 1 + len(mine) + len(shared)
    return pl.pallas_call(
        functools.partial(rest_body, blocks=blocks, slots=slots, batches=batches),
        in_specs=whole(1, pltpu.SMEM) + whole(len(mine) + len(shared) + 8),
        out_specs=whole(4) + whole(4, pl.ANY),
        out_shape=(
            *[pltpu.VMEM((experts, slots, channels), BF16)] * 2,
            *[pltpu.VMEM((blocks // 2, count, channels // blocks), BF16)] * 2,
            *[pltpu.HBM((experts, slots, channels), BF16)] * 2,
            *[pltpu.HBM((count, hidden), BF16)] * 2,
        ),
        scratch_shapes=[pltpu.VMEM((count, hidden), BF16)] * 2 + [pltpu.SemaphoreType.DMA((4,))],
        input_output_aliases={first: 0, first + 1: 1},
        cost_estimate=pl.CostEstimate(
            flops=6 * count * hidden * channels,
            transcendentals=count * hidden,
            bytes_accessed=12 * 1024 * 1024,
        ),
        compiler_params=pltpu.CompilerParams(vmem_limit_bytes=12 * 1024 * 1024),
        name="rest_products",
    )(me, *mine, *shared, *near(*early))


def along_chips(value, steps):
    count = lax.axis_size("chip")
    return lax.ppermute(value, "chip", [(y, (y + steps) % count) for y in range(count)])


def from_after(value):
    count = lax.axis_size("sp")
    return lax.ppermute(value, "sp", [(source, source - 1) for source in range(1, count)])


def to_other_core(value):
    return lax.ppermute(value, "core", [(0, 1), (1, 0)])


def ring_order(chips):
    return [0, *[k for step in range(1, chips // 2) for k in (-step, step)], -(chips // 2)]


def all_blocks(own):
    chips = lax.axis_size("chip")
    arrived = [own]
    for n, steps in enumerate(ring_order(chips)[1:-1]):
        arrived.append(along_chips(arrived[max(0, n - 1)], 1 if steps < 0 else -1))
    half = own.shape[0] // 2
    low = along_chips(arrived[-4][:half], 2)
    high = along_chips(arrived[-3][half:], -2)
    arrived.append(jnp.concatenate([low, high], axis=0))
    shared, at = ([], 0)
    for size in BATCHES:
        shared.append(to_other_core(jnp.stack(arrived[at : at + size])))
        at += size
    return arrived, shared


def added_up(kept, given):
    both = kept.astype(F32) + to_other_core(given).astype(F32)
    arrived = lax.all_to_all(both.astype(BF16), "chip", split_axis=0, concat_axis=0, tiled=True)
    return arrived


def affine(value, mean, rstd, gain, shift):
    normed = (value.astype(F32) - mean[:, None]) * rstd[:, None]
    return normed, normed * gain[None, :] + shift[None, :]


def sent_to_all(value, axis):
    copies = jnp.broadcast_to(value, (lax.axis_size(axis), *value.shape))
    return lax.all_to_all(copies, axis, split_axis=0, concat_axis=0, tiled=True)


def steps(
    moe_in,
    cotangent,
    routes,
    route_weight,
    w_gate,
    w_up,
    w_down,
    conv_pre,
    norm_mean,
    norm_rstd,
    ln_gain,
    ln_shift,
    taps,
    w_proj,
):
    devices = lax.axis_size("sp")
    blocks = lax.axis_size(TP)
    local_tokens = routes.shape[0]
    channels = moe_in.shape[1]
    capacity = 5 * local_tokens // (2 * devices)
    slots = capacity + 1
    me = lax.axis_index(TP).astype(jnp.int32).reshape(1)
    sent, place = send_rows(routes.T, route_weight.T, moe_in, cotangent, devices, slots)
    own = lax.all_to_all(sent, "sp", split_axis=0, concat_axis=0, tiled=True)
    proj = sent_to_all(w_proj, "sp").reshape(-1, channels)
    mine, others = all_blocks(own)
    done = sum(BATCHES[:EARLY])
    early = first_products(me, mine[:done], others[:EARLY], (w_gate, w_up, w_down), slots, blocks)
    _, _, kept, given, rows, routed, hidden, up_grad = rest_products(
        me, mine[done:], others[EARLY:], early, slots, blocks
    )
    rim = 8 * (-(-(taps.shape[0] - 1) // 8))
    rim_cotangent, rim_pre = from_after(jnp.stack([cotangent[:rim], conv_pre[:rim]]))
    facts = [routes[:rim, 0].astype(F32), routes[:rim, 1].astype(F32)]
    facts = from_after(jnp.stack([*facts, norm_mean[:rim], norm_rstd[:rim]]))
    rim_place = rim_places(facts[:2].astype(jnp.int32), devices, slots)
    shared = summed(added_up(kept, given), devices)
    returned = lax.all_to_all(shared, "sp", split_axis=0, concat_axis=0, tiled=True)
    grad_up = dot(up_grad, rows.reshape(-1, rows.shape[2]), 0, 0).astype(BF16)[None]
    grad_down = dot(hidden, routed.reshape(-1, routed.shape[2]), 0, 0).astype(BF16)[None]
    stream, grad_stream = combined(returned, place, rim_place, cotangent, rim_cotangent)
    columns = lax.all_gather(stream, TP, axis=1, tiled=True)
    own_act = affine(conv_pre, norm_mean, norm_rstd, ln_gain, ln_shift)[1]
    activated = (own_act * jax.nn.sigmoid(own_act)).astype(BF16)
    proj_part = dot(columns[:local_tokens], activated, 0, 0).astype(BF16)
    proj_part = proj_part.reshape(devices, -1, channels)
    proj_parts = lax.all_to_all(proj_part, "sp", split_axis=0, concat_axis=0, tiled=True)
    mean = jnp.concatenate([norm_mean, facts[2]])
    rstd = jnp.concatenate([norm_rstd, facts[3]])
    wide_pre = jnp.concatenate([conv_pre, rim_pre], axis=0)
    normed, pre_act = affine(wide_pre, mean, rstd, ln_gain, ln_shift)
    act_sigmoid = jax.nn.sigmoid(pre_act)
    act_grad = dot(columns, proj, 1, 0)
    normed_grad = act_grad * silu_slope(pre_act, act_sigmoid) * ln_gain[None, :]
    sums = jnp.stack([jnp.sum(normed_grad, axis=1), jnp.sum(normed_grad * normed, axis=1)])
    spare = -sums.shape[1] % 128
    sums = jnp.pad(sums, ((0, 0), (0, spare))).reshape(-1)
    sums = lax.all_gather(sums, TP, axis=0, tiled=False)
    sums = jnp.sum(sums, axis=0)
    first_sum, second_sum = sums.reshape(2, -1)[:, : local_tokens + rim]
    width = channels * blocks
    extended = rstd[:, None] * (
        normed_grad - first_sum[:, None] / width - normed * (second_sum[:, None] / width)
    )
    lag_count = taps.shape[0]
    grad_conv = jnp.zeros((local_tokens, channels), F32)
    for lag in range(lag_count):
        grad_conv = grad_conv + taps[lag][None, :] * extended[lag : lag + local_tokens]
    grad_proj = jnp.sum(proj_parts.astype(F32), axis=0)
    return (grad_up, grad_down, grad_stream, grad_proj, grad_conv.astype(BF16))


def solution(mesh):
    placed = (
        P("sp", TP),
        P("sp", TP),
        P("sp", None),
        P("sp", None),
        P("sp", TP, None),
        P("sp", TP, None),
        P("sp", TP, None),
        P("sp", TP),
        P("sp"),
        P("sp"),
        P(TP),
        P(TP),
        P(None, TP),
        P("sp", TP),
    )
    lines = jax.sharding.Mesh(
        mesh.devices.reshape(mesh.devices.shape[0], -1, 2), ("sp", "chip", "core")
    )
    return jax.shard_map(
        steps,
        mesh=lines,
        in_specs=placed,
        out_specs=(
            P("sp", TP, None),
            P("sp", TP, None),
            P("sp", TP),
            P("sp", TP),
            P("sp", TP),
        ),
        check_vma=False,
    )
```

```python
import functools
import jax
import jax.numpy as jnp
from jax import lax
from jax.experimental import pallas as pl
from jax.experimental.pallas import tpu as pltpu
from jax.sharding import PartitionSpec as P


TP = ("chip", "core")
BATCHES = (3, 2, 2, 1)
EARLY = 2
BF16 = jnp.bfloat16
F32 = jnp.float32


def dot(a, b, a_dim, b_dim):
    return lax.dot_general(a, b, (((a_dim,), (b_dim,)), ((), ())), preferred_element_type=F32)


def silu_slope(pre_value, sigmoid_value):
    return sigmoid_value * (1.0 + pre_value * (1.0 - sigmoid_value))


def far(*arrays):
    return tuple(pltpu.with_memory_space_constraint(a, pltpu.HBM) for a in arrays)


def near(*arrays):
    return tuple(pltpu.with_memory_space_constraint(a, pltpu.VMEM) for a in arrays)


def whole(count, space=pltpu.VMEM):
    return [pl.BlockSpec(memory_space=space)] * count


def places(routes, weights, experts, slots):
    top, tokens = routes.shape
    expert = lax.broadcasted_iota(jnp.int32, (experts, tokens), 0)
    named = [(expert == routes[k : k + 1, :]).astype(F32) for k in range(top)]
    before = lax.broadcasted_iota(jnp.int32, (tokens, tokens), 0) < lax.broadcasted_iota(
        jnp.int32, (tokens, tokens), 1
    )
    both = functools.reduce(jnp.add, named)
    earlier = dot(both.astype(BF16), before.astype(F32).astype(BF16), 1, 0)
    position = lax.broadcasted_iota(jnp.int32, (experts * slots, tokens), 0)
    place = jnp.zeros((experts * slots, tokens), F32)
    weight = jnp.zeros((experts * slots, 1), F32)
    for k in range(top):
        slot = jnp.sum(earlier * named[k], axis=0, keepdims=True).astype(jnp.int32)
        hit = (position == routes[k : k + 1, :] * slots + slot).astype(F32)
        place = place + hit
        if weights is not None:
            weight = weight + jnp.sum(hit * weights[k : k + 1, :], axis=1, keepdims=True)
    return place, weight


def send_body(routes, weights, rows, cotangent, sent, place_out, *, experts, slots):
    place, weight = places(routes, weights, experts, slots)
    place = place.astype(BF16)
    place_out[...] = place
    channels = rows.shape[1]
    sent[:, :slots, :] = dot(place, rows[...], 1, 0).astype(BF16).reshape(experts, slots, channels)
    routed = (weight * dot(place, cotangent[...], 1, 0)).astype(BF16)
    sent[:, slots:, :] = routed.reshape(experts, slots, channels)


def send_rows(routes, weights, rows, cotangent, experts, slots):
    tokens, channels = rows.shape
    return pl.pallas_call(
        functools.partial(send_body, experts=experts, slots=slots),
        in_specs=whole(4),
        out_specs=whole(2),
        out_shape=(
            jax.ShapeDtypeStruct((experts, 2 * slots, channels), BF16),
            jax.ShapeDtypeStruct((experts * slots, tokens), BF16),
        ),
        name="send_rows",
    )(routes, weights, rows, cotangent)


def rim_body(routes, place_out, *, experts, slots):
    place, _ = places(routes, None, experts, slots)
    place_out[...] = place.astype(BF16)


def rim_places(routes, experts, slots):
    return pl.pallas_call(
        functools.partial(rim_body, experts=experts, slots=slots),
        in_specs=whole(1),
        out_specs=whole(1)[0],
        out_shape=pltpu.VMEM((experts * slots, routes.shape[1]), BF16),
        compiler_params=pltpu.CompilerParams(vmem_limit_bytes=12 * 1024 * 1024),
        name="rim_places",
    )(routes)


def summed_body(arrived, out):
    experts, both, width = out.shape
    total = functools.reduce(jnp.add, [part[...].astype(F32) for part in [arrived.at[k] for k in range(arrived.shape[0])]])
    total = total.astype(BF16).reshape(experts, both // 2, width)
    out[:, : both // 2, :] = total
    out[: experts - 1, both // 2 :, :] = total[1:]
    out[experts - 1 :, both // 2 :, :] = total[:1]


def summed(arrived, experts):
    _, count, width = arrived.shape
    return pl.pallas_call(
        summed_body,
        in_specs=whole(1),
        out_specs=whole(1)[0],
        out_shape=pltpu.VMEM((experts, 2 * count // experts, width), BF16),
        compiler_params=pltpu.CompilerParams(vmem_limit_bytes=12 * 1024 * 1024),
        name="summed",
    )(arrived)


def combined_body(returned, place, rim_place, cotangent, rim_cotangent, out, own_out):
    _, both, width = returned.shape
    tokens = cotangent.shape[0]
    mine = returned[:, : both // 2, :].reshape(-1, width)
    after = returned[:, both // 2 :, :].reshape(-1, width)
    own = (cotangent[...].astype(F32) + dot(place[...], mine, 0, 0)).astype(BF16)
    out[:tokens, :] = own
    own_out[...] = own
    rim = rim_cotangent[...].astype(F32) + dot(rim_place[...], after, 0, 0)
    out[tokens:, :] = rim.astype(BF16)


def combined(returned, place, rim_place, cotangent, rim_cotangent):
    tokens = cotangent.shape[0] + rim_cotangent.shape[0]
    return pl.pallas_call(
        combined_body,
        in_specs=whole(5),
        out_specs=whole(2),
        out_shape=(
            pltpu.VMEM((tokens, cotangent.shape[1]), BF16),
            jax.ShapeDtypeStruct(cotangent.shape, BF16),
        ),
        compiler_params=pltpu.CompilerParams(vmem_limit_bytes=12 * 1024 * 1024),
        name="combined",
    )(returned, place, rim_place, cotangent, rim_cotangent)


def columns(chip, core, width):
    return pl.ds(pl.multiple_of((2 * chip + core) * width, width), width)


def put_blocks(me, steps, mine, others, rows, routed, blocks, slots):
    chips = blocks // 2
    width = mine[0].shape[-1]
    my_chip, my_core = (me[0] // 2, lax.rem(me[0], 2))
    found = []
    for step, part, (batch, at) in zip(steps, mine, others):
        chip = lax.rem(my_chip + step + chips, chips)
        for core, value in ((my_core, part), (1 - my_core, batch.at[at])):
            cols = columns(chip, core, width)
            rows[:, :, cols] = value[:, :slots, :]
            routed[:, :, cols] = value[:, slots:, :]
        found.append(pl.ds(pl.multiple_of(chip * 2 * width, 2 * width), 2 * width))
    return found


def products(rows, routed, weights, found):
    sums = [None] * 3
    for cols in found:
        for n, (left, weight) in enumerate(zip((rows, rows, routed), weights)):
            taken = left[..., cols].reshape(-1, cols.size)
            part = dot(taken, weight[:, cols], 1, 1)
            sums[n] = part if sums[n] is None else sums[n] + part
    return sums


def first_body(me, *refs, blocks, slots, batches):
    chips = blocks // 2
    count = sum(batches)
    mine, shared = (refs[:count], refs[count : count + len(batches)])
    weights = refs[count + len(batches) : count + len(batches) + 3]
    rows, routed, *sums, held0, held1, held2, sems, weight_sems = refs[count + len(batches) + 3 :]
    others = [(batch, at) for batch, size in zip(shared, batches) for at in range(size)]
    held = (held0, held1, held2)
    width = mine[0].shape[-1]
    my_chip, my_core = (me[0] // 2, lax.rem(me[0], 2))
    copies = [
        pltpu.make_async_copy(weight.at[0], keep, weight_sems.at[n])
        for n, (weight, keep) in enumerate(zip(weights, held))
    ]
    found = []
    for n, (step, (batch, at)) in enumerate(zip(ring_order(chips), others)):
        chip = lax.rem(my_chip + step + chips, chips)
        for i, (core, source) in enumerate(((my_core, mine[n]), (1 - my_core, batch.at[at]))):
            cols = columns(chip, core, width)
            for k, target in enumerate((rows, routed)):
                part = source.at[:, pl.ds(k * slots, slots), :]
                copies.append(pltpu.make_async_copy(part, target.at[:, :, cols], sems.at[n, i, k]))
        found.append(pl.ds(pl.multiple_of(chip * 2 * width, 2 * width), 2 * width))
    for copy in copies:
        copy.start()
    for copy in copies:
        copy.wait()
    for out, value in zip(sums, products(rows, routed, held, found)):
        out[...] = value


def first_products(me, mine, shared, weights, slots, blocks):
    batches = [b.shape[0] for b in shared]
    experts, _, _ = mine[0].shape
    count, hidden, channels = (experts * slots, weights[0].shape[1], weights[0].shape[2])
    return pl.pallas_call(
        functools.partial(first_body, blocks=blocks, slots=slots, batches=batches),
        in_specs=whole(1, pltpu.SMEM)
        + whole(len(mine) + len(shared) + 3, pltpu.HBM),
        out_specs=whole(8),
        scratch_shapes=[
            pltpu.SemaphoreType.DMA((len(mine), 2, 2)),
            pltpu.SemaphoreType.DMA((3,)),
        ],
        out_shape=(
            *[pltpu.VMEM((experts, slots, channels), BF16)] * 2,
            *[pltpu.VMEM((count, hidden), F32)] * 3,
            *[pltpu.VMEM((hidden, channels), BF16)] * 3,
        ),
        cost_estimate=pl.CostEstimate(
            flops=4 * count * hidden * channels, transcendentals=0, bytes_accessed=12 * 1024 * 1024
        ),
        compiler_params=pltpu.CompilerParams(vmem_limit_bytes=12 * 1024 * 1024),
        name="first_products",
    )(me, *far(*mine, *shared, *weights))


def partial_rows(out, gate_grad, up_grad, gate_weight, up_weight, core):
    chips, _, width = out.shape
    for j in range(0, chips, 2):
        gate_cols, up_cols = (
            jnp.concatenate([weight[:, columns(j + i, core, width)] for i in (0, 1)], axis=1)
            for weight in (gate_weight, up_weight)
        )
        both = dot(gate_grad, gate_cols, 1, 0) + dot(up_grad, up_cols, 1, 0)
        for i in (0, 1):
            out[j + i] = both[:, i * width : (i + 1) * width].astype(BF16)


def kept_body(me, gate_grad, up_grad, gate_weight, up_weight, out):
    core = lax.rem(me[0], 2)
    partial_rows(out, gate_grad[...], up_grad[...], gate_weight, up_weight, core)


def kept_products(me, gate_grad, up_grad, gate_weight, up_weight, blocks):
    count, hidden = gate_grad.shape
    channels = gate_weight.shape[1]
    return pl.pallas_call(
        kept_body,
        in_specs=whole(1, pltpu.SMEM) + whole(4),
        out_specs=whole(1)[0],
        out_shape=pltpu.VMEM((blocks // 2, count, channels // blocks), BF16),
        cost_estimate=pl.CostEstimate(
            flops=2 * count * hidden * channels, transcendentals=0, bytes_accessed=4 * 1024 * 1024
        ),
        compiler_params=pltpu.CompilerParams(vmem_limit_bytes=12 * 1024 * 1024),
        name="kept_products",
    )(me, *near(gate_grad, up_grad, gate_weight, up_weight))


def rest_body(me, *refs, blocks, slots, batches):
    chips = blocks // 2
    count = sum(batches)
    mine, shared = (refs[:count], refs[count : count + len(batches)])
    _, _, gate_sum, up_sum, down_sum, *weights = refs[count + len(batches) : count + len(batches) + 8]
    outs = refs[count + len(batches) + 8 :]
    rows, routed, given, gate_out, up_out, *far_outs = outs[:9]
    hidden_held, up_held, sems = outs[9:]
    sends = [
        pltpu.make_async_copy(held, out, sems.at[n])
        for n, (held, out) in enumerate(zip((rows, routed, hidden_held, up_held), far_outs))
    ]
    others = [(batch, at) for batch, size in zip(shared, batches) for at in range(size)]
    steps = ring_order(chips)[-count:]
    found = put_blocks(me, steps, mine, others, rows, routed, blocks, slots)
    sends[0].start()
    sends[1].start()
    gate_pre, up_pre, hidden_grad = products(rows, routed, weights, found)
    gate_pre = gate_pre + gate_sum[...]
    up_pre = up_pre + up_sum[...]
    hidden_grad = hidden_grad + down_sum[...]
    gate_weight, up_weight = weights[:2]
    my_core = lax.rem(me[0], 2)
    gate_sigmoid = jax.nn.sigmoid(gate_pre)
    gate_active = gate_pre * gate_sigmoid
    hidden_held[...] = (gate_active * up_pre).astype(BF16)
    gate_grad = (hidden_grad * up_pre * silu_slope(gate_pre, gate_sigmoid)).astype(BF16)
    up_grad = (hidden_grad * gate_active).astype(BF16)
    up_held[...] = up_grad
    sends[2].start()
    sends[3].start()
    partial_rows(given, gate_grad, up_grad, gate_weight, up_weight, 1 - my_core)
    gate_out[...] = gate_grad
    up_out[...] = up_grad
    for send in sends:
        send.wait()


def rest_products(me, mine, shared, early, slots, blocks):
    batches = [b.shape[0] for b in shared]
    experts, _, channels = early[0].shape
    count, hidden = early[2].shape
    first = 1 + len(mine) + len(shared)
    return pl.pallas_call(
        functools.partial(rest_body, blocks=blocks, slots=slots, batches=batches),
        in_specs=whole(1, pltpu.SMEM) + whole(len(mine) + len(shared) + 8),
        out_specs=whole(5) + whole(4, pl.ANY),
        out_shape=(
            *[pltpu.VMEM((experts, slots, channels), BF16)] * 2,
            pltpu.VMEM((blocks // 2, count, channels // blocks), BF16),
            *[pltpu.VMEM((count, hidden), BF16)] * 2,
            *[pltpu.HBM((experts, slots, channels), BF16)] * 2,
            *[pltpu.HBM((count, hidden), BF16)] * 2,
        ),
        scratch_shapes=[pltpu.VMEM((count, hidden), BF16)] * 2 + [pltpu.SemaphoreType.DMA((4,))],
        input_output_aliases={first: 0, first + 1: 1},
        cost_estimate=pl.CostEstimate(
            flops=6 * count * hidden * channels,
            transcendentals=count * hidden,
            bytes_accessed=12 * 1024 * 1024,
        ),
        compiler_params=pltpu.CompilerParams(vmem_limit_bytes=12 * 1024 * 1024),
        name="rest_products",
    )(me, *mine, *shared, *near(*early))


def along_chips(value, steps):
    count = lax.axis_size("chip")
    return lax.ppermute(value, "chip", [(y, (y + steps) % count) for y in range(count)])


def from_after(value):
    count = lax.axis_size("sp")
    return lax.ppermute(value, "sp", [(source, source - 1) for source in range(1, count)])


def to_other_core(value):
    return lax.ppermute(value, "core", [(0, 1), (1, 0)])


def ring_order(chips):
    return [0, *[k for step in range(1, chips // 2) for k in (-step, step)], -(chips // 2)]


def all_blocks(own):
    chips = lax.axis_size("chip")
    arrived = [own]
    for n, steps in enumerate(ring_order(chips)[1:]):
        arrived.append(along_chips(arrived[max(0, n - 1)], 1 if steps < 0 else -1))
    shared, at = ([], 0)
    for size in BATCHES[:-1]:
        shared.append(to_other_core(jnp.stack(arrived[at : at + size])))
        at += size
    count = lax.axis_size(TP)
    across = [(t, ((t - 2) % count) ^ 1) for t in range(count)]
    shared.append(lax.ppermute(arrived[-2], TP, across)[None])
    return arrived, shared


def added_up(kept, other):
    both = kept.astype(F32) + other.astype(F32)
    arrived = lax.all_to_all(both.astype(BF16), "chip", split_axis=0, concat_axis=0, tiled=True)
    return arrived


def affine(value, mean, rstd, gain, shift):
    normed = (value.astype(F32) - mean[:, None]) * rstd[:, None]
    return normed, normed * gain[None, :] + shift[None, :]


def sent_to_all(value, axis):
    copies = jnp.broadcast_to(value, (lax.axis_size(axis), *value.shape))
    return lax.all_to_all(copies, axis, split_axis=0, concat_axis=0, tiled=True)


def steps(
    moe_in,
    cotangent,
    routes,
    route_weight,
    w_gate,
    w_up,
    w_down,
    conv_pre,
    norm_mean,
    norm_rstd,
    ln_gain,
    ln_shift,
    taps,
    w_proj,
):
    devices = lax.axis_size("sp")
    blocks = lax.axis_size(TP)
    local_tokens = routes.shape[0]
    channels = moe_in.shape[1]
    capacity = 5 * local_tokens // (2 * devices)
    slots = capacity + 1
    me = lax.axis_index(TP).astype(jnp.int32).reshape(1)
    sent, place = send_rows(routes.T, route_weight.T, moe_in, cotangent, devices, slots)
    own = lax.all_to_all(sent, "sp", split_axis=0, concat_axis=0, tiled=True)
    proj = sent_to_all(w_proj, "sp").reshape(-1, channels)
    mine, others = all_blocks(own)
    done = sum(BATCHES[:EARLY])
    early = first_products(me, mine[:done], others[:EARLY], (w_gate, w_up, w_down), slots, blocks)
    _, _, given, gate_rows, up_rows, rows, routed, hidden, up_grad = rest_products(
        me, mine[done:], others[EARLY:], early, slots, blocks
    )
    rim = 8 * (-(-(taps.shape[0] - 1) // 8))
    rim_cotangent, rim_pre = from_after(jnp.stack([cotangent[:rim], conv_pre[:rim]]))
    facts = [routes[:rim, 0].astype(F32), routes[:rim, 1].astype(F32)]
    facts = from_after(jnp.stack([*facts, norm_mean[:rim], norm_rstd[:rim]]))
    rim_place = rim_places(facts[:2].astype(jnp.int32), devices, slots)
    other = to_other_core(given)
    kept = kept_products(me, gate_rows, up_rows, early[5], early[6], blocks)
    shared = summed(added_up(kept, other), devices)
    returned = lax.all_to_all(shared, "sp", split_axis=0, concat_axis=0, tiled=True)
    grad_up = dot(up_grad, rows.reshape(-1, rows.shape[2]), 0, 0).astype(BF16)[None]
    grad_down = dot(hidden, routed.reshape(-1, routed.shape[2]), 0, 0).astype(BF16)[None]
    stream, grad_stream = combined(returned, place, rim_place, cotangent, rim_cotangent)
    columns = lax.all_gather(stream, TP, axis=1, tiled=True)
    own_act = affine(conv_pre, norm_mean, norm_rstd, ln_gain, ln_shift)[1]
    activated = (own_act * jax.nn.sigmoid(own_act)).astype(BF16)
    proj_part = dot(columns[:local_tokens], activated, 0, 0).astype(BF16)
    proj_part = proj_part.reshape(devices, -1, channels)
    proj_parts = lax.all_to_all(proj_part, "sp", split_axis=0, concat_axis=0, tiled=True)
    mean = jnp.concatenate([norm_mean, facts[2]])
    rstd = jnp.concatenate([norm_rstd, facts[3]])
    wide_pre = jnp.concatenate([conv_pre, rim_pre], axis=0)
    normed, pre_act = affine(wide_pre, mean, rstd, ln_gain, ln_shift)
    act_sigmoid = jax.nn.sigmoid(pre_act)
    act_grad = dot(columns, proj, 1, 0)
    normed_grad = act_grad * silu_slope(pre_act, act_sigmoid) * ln_gain[None, :]
    sums = jnp.stack([jnp.sum(normed_grad, axis=1), jnp.sum(normed_grad * normed, axis=1)])
    spare = -sums.shape[1] % 128
    sums = jnp.pad(sums, ((0, 0), (0, spare))).reshape(-1)
    sums = lax.all_gather(sums, TP, axis=0, tiled=False)
    sums = jnp.sum(sums, axis=0)
    first_sum, second_sum = sums.reshape(2, -1)[:, : local_tokens + rim]
    width = channels * blocks
    extended = rstd[:, None] * (
        normed_grad - first_sum[:, None] / width - normed * (second_sum[:, None] / width)
    )
    lag_count = taps.shape[0]
    grad_conv = jnp.zeros((local_tokens, channels), F32)
    for lag in range(lag_count):
        grad_conv = grad_conv + taps[lag][None, :] * extended[lag : lag + local_tokens]
    grad_proj = jnp.sum(proj_parts.astype(F32), axis=0)
    return (grad_up, grad_down, grad_stream, grad_proj, grad_conv.astype(BF16))


def solution(mesh):
    placed = (
        P("sp", TP),
        P("sp", TP),
        P("sp", None),
        P("sp", None),
        P("sp", TP, None),
        P("sp", TP, None),
        P("sp", TP, None),
        P("sp", TP),
        P("sp"),
        P("sp"),
        P(TP),
        P(TP),
        P(None, TP),
        P("sp", TP),
    )
    lines = jax.sharding.Mesh(
        mesh.devices.reshape(mesh.devices.shape[0], -1, 2), ("sp", "chip", "core")
    )
    return jax.shard_map(
        steps,
        mesh=lines,
        in_specs=placed,
        out_specs=(
            P("sp", TP, None),
            P("sp", TP, None),
            P("sp", TP),
            P("sp", TP),
            P("sp", TP),
        ),
        check_vma=False,
    )
```

```python
import functools
import jax
import jax.numpy as jnp
from jax import lax
from jax.experimental import pallas as pl
from jax.experimental.pallas import tpu as pltpu
from jax.sharding import PartitionSpec as P


TP = ("chip", "core")
BATCHES = (5, 2, 1)
EARLY = 1
BF16 = jnp.bfloat16
F32 = jnp.float32


def dot(a, b, a_dim, b_dim):
    return lax.dot_general(a, b, (((a_dim,), (b_dim,)), ((), ())), preferred_element_type=F32)


def silu_slope(pre_value, sigmoid_value):
    return sigmoid_value * (1.0 + pre_value * (1.0 - sigmoid_value))


def far(*arrays):
    return tuple(pltpu.with_memory_space_constraint(a, pltpu.HBM) for a in arrays)


def near(*arrays):
    return tuple(pltpu.with_memory_space_constraint(a, pltpu.VMEM) for a in arrays)


def whole(count, space=pltpu.VMEM):
    return [pl.BlockSpec(memory_space=space)] * count


def places(routes, weights, experts, slots):
    top, tokens = routes.shape
    expert = lax.broadcasted_iota(jnp.int32, (experts, tokens), 0)
    named = [(expert == routes[k : k + 1, :]).astype(F32) for k in range(top)]
    before = lax.broadcasted_iota(jnp.int32, (tokens, tokens), 0) < lax.broadcasted_iota(
        jnp.int32, (tokens, tokens), 1
    )
    both = functools.reduce(jnp.add, named)
    earlier = dot(both.astype(BF16), before.astype(F32).astype(BF16), 1, 0)
    position = lax.broadcasted_iota(jnp.int32, (experts * slots, tokens), 0)
    place = jnp.zeros((experts * slots, tokens), F32)
    weight = jnp.zeros((experts * slots, 1), F32)
    for k in range(top):
        slot = jnp.sum(earlier * named[k], axis=0, keepdims=True).astype(jnp.int32)
        hit = (position == routes[k : k + 1, :] * slots + slot).astype(F32)
        place = place + hit
        if weights is not None:
            weight = weight + jnp.sum(hit * weights[k : k + 1, :], axis=1, keepdims=True)
    return place, weight


def send_body(routes, weights, rows, cotangent, sent, place_out, *, experts, slots):
    place, weight = places(routes, weights, experts, slots)
    place = place.astype(BF16)
    place_out[...] = place
    channels = rows.shape[1]
    sent[:, :slots, :] = dot(place, rows[...], 1, 0).astype(BF16).reshape(experts, slots, channels)
    routed = (weight * dot(place, cotangent[...], 1, 0)).astype(BF16)
    sent[:, slots:, :] = routed.reshape(experts, slots, channels)


def send_rows(routes, weights, rows, cotangent, experts, slots):
    tokens, channels = rows.shape
    return pl.pallas_call(
        functools.partial(send_body, experts=experts, slots=slots),
        in_specs=whole(4),
        out_specs=whole(2),
        out_shape=(
            jax.ShapeDtypeStruct((experts, 2 * slots, channels), BF16),
            jax.ShapeDtypeStruct((experts * slots, tokens), BF16),
        ),
        name="send_rows",
    )(routes, weights, rows, cotangent)


def rim_body(routes, place_out, *, experts, slots):
    place, _ = places(routes, None, experts, slots)
    place_out[...] = place.astype(BF16)


def rim_places(routes, experts, slots):
    return pl.pallas_call(
        functools.partial(rim_body, experts=experts, slots=slots),
        in_specs=whole(1),
        out_specs=whole(1)[0],
        out_shape=pltpu.VMEM((experts * slots, routes.shape[1]), BF16),
        compiler_params=pltpu.CompilerParams(vmem_limit_bytes=12 * 1024 * 1024),
        name="rim_places",
    )(routes)


def summed_body(arrived, out):
    experts, both, width = out.shape
    total = functools.reduce(jnp.add, [part[...].astype(F32) for part in [arrived.at[k] for k in range(arrived.shape[0])]])
    total = total.astype(BF16).reshape(experts, both // 2, width)
    out[:, : both // 2, :] = total
    out[: experts - 1, both // 2 :, :] = total[1:]
    out[experts - 1 :, both // 2 :, :] = total[:1]


def summed(arrived, experts):
    _, count, width = arrived.shape
    return pl.pallas_call(
        summed_body,
        in_specs=whole(1),
        out_specs=whole(1)[0],
        out_shape=pltpu.VMEM((experts, 2 * count // experts, width), BF16),
        compiler_params=pltpu.CompilerParams(vmem_limit_bytes=12 * 1024 * 1024),
        name="summed",
    )(arrived)


def combined_body(returned, place, rim_place, cotangent, rim_cotangent, out, own_out):
    _, both, width = returned.shape
    tokens = cotangent.shape[0]
    mine = returned[:, : both // 2, :].reshape(-1, width)
    after = returned[:, both // 2 :, :].reshape(-1, width)
    own = (cotangent[...].astype(F32) + dot(place[...], mine, 0, 0)).astype(BF16)
    out[:tokens, :] = own
    own_out[...] = own
    rim = rim_cotangent[...].astype(F32) + dot(rim_place[...], after, 0, 0)
    out[tokens:, :] = rim.astype(BF16)


def combined(returned, place, rim_place, cotangent, rim_cotangent):
    tokens = cotangent.shape[0] + rim_cotangent.shape[0]
    return pl.pallas_call(
        combined_body,
        in_specs=whole(5),
        out_specs=whole(2),
        out_shape=(
            pltpu.VMEM((tokens, cotangent.shape[1]), BF16),
            jax.ShapeDtypeStruct(cotangent.shape, BF16),
        ),
        compiler_params=pltpu.CompilerParams(vmem_limit_bytes=12 * 1024 * 1024),
        name="combined",
    )(returned, place, rim_place, cotangent, rim_cotangent)


def columns(chip, core, width):
    return pl.ds(pl.multiple_of((2 * chip + core) * width, width), width)


def put_blocks(me, steps, mine, others, rows, routed, blocks, slots):
    chips = blocks // 2
    width = mine[0].shape[-1]
    my_chip, my_core = (me[0] // 2, lax.rem(me[0], 2))
    found = []
    for step, part, (batch, at) in zip(steps, mine, others):
        chip = lax.rem(my_chip + step + chips, chips)
        for core, value in ((my_core, part), (1 - my_core, batch.at[at])):
            cols = columns(chip, core, width)
            rows[:, :, cols] = value[:, :slots, :]
            routed[:, :, cols] = value[:, slots:, :]
        found.append(pl.ds(pl.multiple_of(chip * 2 * width, 2 * width), 2 * width))
    return found


def products(rows, routed, weights, found):
    sums = [None] * 3
    for cols in found:
        for n, (left, weight) in enumerate(zip((rows, rows, routed), weights)):
            taken = left[..., cols].reshape(-1, cols.size)
            part = dot(taken, weight[:, cols], 1, 1)
            sums[n] = part if sums[n] is None else sums[n] + part
    return sums


def held_body(*refs):
    count = len(refs) // 2
    copies = [
        pltpu.make_async_copy(refs[n].at[0], refs[count + n], refs[-1].at[n]) for n in range(count)
    ]
    for copy in copies:
        copy.start()
    for copy in copies:
        copy.wait()


def held_weights(weights):
    return pl.pallas_call(
        held_body,
        in_specs=whole(len(weights), pltpu.HBM),
        out_specs=whole(len(weights)),
        out_shape=[pltpu.VMEM(w.shape[1:], w.dtype) for w in weights],
        scratch_shapes=[pltpu.SemaphoreType.DMA((len(weights),))],
        compiler_params=pltpu.CompilerParams(vmem_limit_bytes=12 * 1024 * 1024),
        name="held_weights",
    )(*far(*weights))


def first_body(me, *refs, blocks, slots, batches):
    chips = blocks // 2
    count = sum(batches)
    mine, shared = (refs[:count], refs[count : count + len(batches)])
    held = refs[count + len(batches) : count + len(batches) + 3]
    rows, routed, *sums, sems = refs[count + len(batches) + 3 :]
    others = [(batch, at) for batch, size in zip(shared, batches) for at in range(size)]
    width = mine[0].shape[-1]
    my_chip, my_core = (me[0] // 2, lax.rem(me[0], 2))
    copies, found = ([], [])
    for n, (step, (batch, at)) in enumerate(zip(ring_order(chips), others)):
        chip = lax.rem(my_chip + step + chips, chips)
        copies.append([])
        for i, (core, source) in enumerate(((my_core, mine[n]), (1 - my_core, batch.at[at]))):
            cols = columns(chip, core, width)
            for k, target in enumerate((rows, routed)):
                part = source.at[:, pl.ds(k * slots, slots), :]
                copies[n].append(
                    pltpu.make_async_copy(part, target.at[:, :, cols], sems.at[n, i, k])
                )
        found.append(pl.ds(pl.multiple_of(chip * 2 * width, 2 * width), 2 * width))
        for copy in copies[n]:
            copy.start()
    totals = [None] * 3
    for n in range(count):
        for copy in copies[n]:
            copy.wait()
        parts = products(rows, routed, held, found[n : n + 1])
        totals = [p if t is None else t + p for t, p in zip(totals, parts)]
    for out, value in zip(sums, totals):
        out[...] = value


def first_products(me, mine, shared, held, slots, blocks):
    batches = [b.shape[0] for b in shared]
    experts, _, _ = mine[0].shape
    count, (hidden, channels) = (experts * slots, held[0].shape)
    return pl.pallas_call(
        functools.partial(first_body, blocks=blocks, slots=slots, batches=batches),
        in_specs=whole(1, pltpu.SMEM) + whole(len(mine) + len(shared), pltpu.HBM) + whole(3),
        out_specs=whole(5),
        scratch_shapes=[pltpu.SemaphoreType.DMA((len(mine), 2, 2))],
        out_shape=(
            *[pltpu.VMEM((experts, slots, channels), BF16)] * 2,
            *[pltpu.VMEM((count, hidden), F32)] * 3,
        ),
        cost_estimate=pl.CostEstimate(
            flops=4 * count * hidden * channels, transcendentals=0, bytes_accessed=6 * 1024 * 1024
        ),
        compiler_params=pltpu.CompilerParams(vmem_limit_bytes=12 * 1024 * 1024),
        name="first_products",
    )(me, *far(*mine, *shared), *near(*held))


def partial_rows(out, gate_grad, up_grad, gate_weight, up_weight, core):
    chips, _, width = out.shape
    for j in range(0, chips, 2):
        gate_cols, up_cols = (
            jnp.concatenate([weight[:, columns(j + i, core, width)] for i in (0, 1)], axis=1)
            for weight in (gate_weight, up_weight)
        )
        both = dot(gate_grad, gate_cols, 1, 0) + dot(up_grad, up_cols, 1, 0)
        for i in (0, 1):
            out[j + i] = both[:, i * width : (i + 1) * width].astype(BF16)


def kept_body(me, gate_grad, up_grad, gate_weight, up_weight, out):
    core = lax.rem(me[0], 2)
    partial_rows(out, gate_grad[...], up_grad[...], gate_weight, up_weight, core)


def kept_products(me, gate_grad, up_grad, gate_weight, up_weight, blocks):
    count, hidden = gate_grad.shape
    channels = gate_weight.shape[1]
    return pl.pallas_call(
        kept_body,
        in_specs=whole(1, pltpu.SMEM) + whole(4),
        out_specs=whole(1)[0],
        out_shape=pltpu.VMEM((blocks // 2, count, channels // blocks), BF16),
        cost_estimate=pl.CostEstimate(
            flops=2 * count * hidden * channels, transcendentals=0, bytes_accessed=4 * 1024 * 1024
        ),
        compiler_params=pltpu.CompilerParams(vmem_limit_bytes=12 * 1024 * 1024),
        name="kept_products",
    )(me, *near(gate_grad, up_grad, gate_weight, up_weight))


def rest_body(me, *refs, blocks, slots, batches):
    chips = blocks // 2
    count = sum(batches)
    mine, shared = (refs[:count], refs[count : count + len(batches)])
    _, _, gate_sum, up_sum, down_sum, *weights = refs[count + len(batches) : count + len(batches) + 8]
    outs = refs[count + len(batches) + 8 :]
    rows, routed, given, gate_out, up_out, *far_outs = outs[:9]
    hidden_held, up_held, sems = outs[9:]
    sends = [
        pltpu.make_async_copy(held, out, sems.at[n])
        for n, (held, out) in enumerate(zip((rows, routed, hidden_held, up_held), far_outs))
    ]
    others = [(batch, at) for batch, size in zip(shared, batches) for at in range(size)]
    steps = ring_order(chips)[-count:]
    found = put_blocks(me, steps, mine, others, rows, routed, blocks, slots)
    sends[0].start()
    sends[1].start()
    gate_pre, up_pre, hidden_grad = products(rows, routed, weights, found)
    gate_pre = gate_pre + gate_sum[...]
    up_pre = up_pre + up_sum[...]
    hidden_grad = hidden_grad + down_sum[...]
    gate_weight, up_weight = weights[:2]
    my_core = lax.rem(me[0], 2)
    gate_sigmoid = jax.nn.sigmoid(gate_pre)
    gate_active = gate_pre * gate_sigmoid
    hidden_held[...] = (gate_active * up_pre).astype(BF16)
    gate_grad = (hidden_grad * up_pre * silu_slope(gate_pre, gate_sigmoid)).astype(BF16)
    up_grad = (hidden_grad * gate_active).astype(BF16)
    up_held[...] = up_grad
    sends[2].start()
    sends[3].start()
    partial_rows(given, gate_grad, up_grad, gate_weight, up_weight, 1 - my_core)
    gate_out[...] = gate_grad
    up_out[...] = up_grad
    for send in sends:
        send.wait()


def rest_products(me, mine, shared, early, slots, blocks):
    batches = [b.shape[0] for b in shared]
    experts, _, channels = early[0].shape
    count, hidden = early[2].shape
    first = 1 + len(mine) + len(shared)
    return pl.pallas_call(
        functools.partial(rest_body, blocks=blocks, slots=slots, batches=batches),
        in_specs=whole(1, pltpu.SMEM) + whole(len(mine) + len(shared) + 8),
        out_specs=whole(5) + whole(4, pl.ANY),
        out_shape=(
            *[pltpu.VMEM((experts, slots, channels), BF16)] * 2,
            pltpu.VMEM((blocks // 2, count, channels // blocks), BF16),
            *[pltpu.VMEM((count, hidden), BF16)] * 2,
            *[pltpu.HBM((experts, slots, channels), BF16)] * 2,
            *[pltpu.HBM((count, hidden), BF16)] * 2,
        ),
        scratch_shapes=[pltpu.VMEM((count, hidden), BF16)] * 2 + [pltpu.SemaphoreType.DMA((4,))],
        input_output_aliases={first: 0, first + 1: 1},
        cost_estimate=pl.CostEstimate(
            flops=6 * count * hidden * channels,
            transcendentals=count * hidden,
            bytes_accessed=12 * 1024 * 1024,
        ),
        compiler_params=pltpu.CompilerParams(vmem_limit_bytes=12 * 1024 * 1024),
        name="rest_products",
    )(me, *mine, *shared, *near(*early))


def along_chips(value, steps):
    count = lax.axis_size("chip")
    return lax.ppermute(value, "chip", [(y, (y + steps) % count) for y in range(count)])


def from_after(value):
    count = lax.axis_size("sp")
    return lax.ppermute(value, "sp", [(source, source - 1) for source in range(1, count)])


def to_other_core(value):
    return lax.ppermute(value, "core", [(0, 1), (1, 0)])


def ring_order(chips):
    return [0, *[k for step in range(1, chips // 2) for k in (-step, step)], -(chips // 2)]


def all_blocks(own):
    chips = lax.axis_size("chip")
    arrived = [own]
    for n, steps in enumerate(ring_order(chips)[1:]):
        arrived.append(along_chips(arrived[max(0, n - 1)], 1 if steps < 0 else -1))
    shared, at = ([], 0)
    for size in BATCHES[:-1]:
        shared.append(to_other_core(jnp.stack(arrived[at : at + size])))
        at += size
    count = lax.axis_size(TP)
    across = [(t, ((t - 2) % count) ^ 1) for t in range(count)]
    shared.append(lax.ppermute(arrived[-2], TP, across)[None])
    return arrived, shared


def added_up(kept, other):
    both = kept.astype(F32) + other.astype(F32)
    arrived = lax.all_to_all(both.astype(BF16), "chip", split_axis=0, concat_axis=0, tiled=True)
    return arrived


def affine(value, mean, rstd, gain, shift):
    normed = (value.astype(F32) - mean[:, None]) * rstd[:, None]
    return normed, normed * gain[None, :] + shift[None, :]


def sent_to_all(value, axis):
    copies = jnp.broadcast_to(value, (lax.axis_size(axis), *value.shape))
    return lax.all_to_all(copies, axis, split_axis=0, concat_axis=0, tiled=True)


def steps(
    moe_in,
    cotangent,
    routes,
    route_weight,
    w_gate,
    w_up,
    w_down,
    conv_pre,
    norm_mean,
    norm_rstd,
    ln_gain,
    ln_shift,
    taps,
    w_proj,
):
    devices = lax.axis_size("sp")
    blocks = lax.axis_size(TP)
    local_tokens = routes.shape[0]
    channels = moe_in.shape[1]
    capacity = 5 * local_tokens // (2 * devices)
    slots = capacity + 1
    me = lax.axis_index(TP).astype(jnp.int32).reshape(1)
    sent, place = send_rows(routes.T, route_weight.T, moe_in, cotangent, devices, slots)
    own = lax.all_to_all(sent, "sp", split_axis=0, concat_axis=0, tiled=True)
    proj = sent_to_all(w_proj, "sp").reshape(-1, channels)
    held = held_weights((w_gate, w_up, w_down))
    mine, others = all_blocks(own)
    done = sum(BATCHES[:EARLY])
    early = first_products(
        me, mine[:done], others[:EARLY], held, slots, blocks
    )
    _, _, given, gate_rows, up_rows, rows, routed, hidden, up_grad = rest_products(
        me, mine[done:], others[EARLY:], (*early, *held), slots, blocks
    )
    rim = 8 * (-(-(taps.shape[0] - 1) // 8))
    rim_cotangent, rim_pre = from_after(jnp.stack([cotangent[:rim], conv_pre[:rim]]))
    facts = [routes[:rim, 0].astype(F32), routes[:rim, 1].astype(F32)]
    facts = from_after(jnp.stack([*facts, norm_mean[:rim], norm_rstd[:rim]]))
    rim_place = rim_places(facts[:2].astype(jnp.int32), devices, slots)
    other = to_other_core(given)
    kept = kept_products(me, gate_rows, up_rows, held[0], held[1], blocks)
    shared = summed(added_up(kept, other), devices)
    returned = lax.all_to_all(shared, "sp", split_axis=0, concat_axis=0, tiled=True)
    grad_up = dot(up_grad, rows.reshape(-1, rows.shape[2]), 0, 0).astype(BF16)[None]
    grad_down = dot(hidden, routed.reshape(-1, routed.shape[2]), 0, 0).astype(BF16)[None]
    stream, grad_stream = combined(returned, place, rim_place, cotangent, rim_cotangent)
    columns = lax.all_gather(stream, TP, axis=1, tiled=True)
    own_act = affine(conv_pre, norm_mean, norm_rstd, ln_gain, ln_shift)[1]
    activated = (own_act * jax.nn.sigmoid(own_act)).astype(BF16)
    proj_part = dot(columns[:local_tokens], activated, 0, 0).astype(BF16)
    proj_part = proj_part.reshape(devices, -1, channels)
    proj_parts = lax.all_to_all(proj_part, "sp", split_axis=0, concat_axis=0, tiled=True)
    mean = jnp.concatenate([norm_mean, facts[2]])
    rstd = jnp.concatenate([norm_rstd, facts[3]])
    wide_pre = jnp.concatenate([conv_pre, rim_pre], axis=0)
    normed, pre_act = affine(wide_pre, mean, rstd, ln_gain, ln_shift)
    act_sigmoid = jax.nn.sigmoid(pre_act)
    act_grad = dot(columns, proj, 1, 0)
    normed_grad = act_grad * silu_slope(pre_act, act_sigmoid) * ln_gain[None, :]
    sums = jnp.stack([jnp.sum(normed_grad, axis=1), jnp.sum(normed_grad * normed, axis=1)])
    spare = -sums.shape[1] % 128
    sums = jnp.pad(sums, ((0, 0), (0, spare))).reshape(-1)
    sums = lax.all_gather(sums, TP, axis=0, tiled=False)
    sums = jnp.sum(sums, axis=0)
    first_sum, second_sum = sums.reshape(2, -1)[:, : local_tokens + rim]
    width = channels * blocks
    extended = rstd[:, None] * (
        normed_grad - first_sum[:, None] / width - normed * (second_sum[:, None] / width)
    )
    lag_count = taps.shape[0]
    grad_conv = jnp.zeros((local_tokens, channels), F32)
    for lag in range(lag_count):
        grad_conv = grad_conv + taps[lag][None, :] * extended[lag : lag + local_tokens]
    grad_proj = jnp.sum(proj_parts.astype(F32), axis=0)
    return (grad_up, grad_down, grad_stream, grad_proj, grad_conv.astype(BF16))


def solution(mesh):
    placed = (
        P("sp", TP),
        P("sp", TP),
        P("sp", None),
        P("sp", None),
        P("sp", TP, None),
        P("sp", TP, None),
        P("sp", TP, None),
        P("sp", TP),
        P("sp"),
        P("sp"),
        P(TP),
        P(TP),
        P(None, TP),
        P("sp", TP),
    )
    lines = jax.sharding.Mesh(
        mesh.devices.reshape(mesh.devices.shape[0], -1, 2), ("sp", "chip", "core")
    )
    return jax.shard_map(
        steps,
        mesh=lines,
        in_specs=placed,
        out_specs=(
            P("sp", TP, None),
            P("sp", TP, None),
            P("sp", TP),
            P("sp", TP),
            P("sp", TP),
        ),
        check_vma=False,
    )
```

```python
import functools
import jax
import jax.numpy as jnp
from jax import lax
from jax.experimental import pallas as pl
from jax.experimental.pallas import tpu as pltpu
from jax.sharding import PartitionSpec as P


TP = ("chip", "core")
BATCHES = (3, 2, 2, 1)
EARLY = 2
BF16 = jnp.bfloat16
F32 = jnp.float32


def dot(a, b, a_dim, b_dim):
    return lax.dot_general(a, b, (((a_dim,), (b_dim,)), ((), ())), preferred_element_type=F32)


def silu_slope(pre_value, sigmoid_value):
    return sigmoid_value * (1.0 + pre_value * (1.0 - sigmoid_value))


def far(*arrays):
    return tuple(pltpu.with_memory_space_constraint(a, pltpu.HBM) for a in arrays)


def near(*arrays):
    return tuple(pltpu.with_memory_space_constraint(a, pltpu.VMEM) for a in arrays)


def whole(count, space=pltpu.VMEM):
    return [pl.BlockSpec(memory_space=space)] * count


def places(routes, weights, experts, slots):
    top, tokens = routes.shape
    expert = lax.broadcasted_iota(jnp.int32, (experts, tokens), 0)
    named = [(expert == routes[k : k + 1, :]).astype(F32) for k in range(top)]
    before = lax.broadcasted_iota(jnp.int32, (tokens, tokens), 0) < lax.broadcasted_iota(
        jnp.int32, (tokens, tokens), 1
    )
    both = functools.reduce(jnp.add, named)
    earlier = dot(both.astype(BF16), before.astype(F32).astype(BF16), 1, 0)
    position = lax.broadcasted_iota(jnp.int32, (experts * slots, tokens), 0)
    place = jnp.zeros((experts * slots, tokens), F32)
    weight = jnp.zeros((experts * slots, 1), F32)
    for k in range(top):
        slot = jnp.sum(earlier * named[k], axis=0, keepdims=True).astype(jnp.int32)
        hit = (position == routes[k : k + 1, :] * slots + slot).astype(F32)
        place = place + hit
        if weights is not None:
            weight = weight + jnp.sum(hit * weights[k : k + 1, :], axis=1, keepdims=True)
    return place, weight


def send_body(routes, weights, rows, cotangent, sent, place_out, *, experts, slots):
    place, weight = places(routes, weights, experts, slots)
    place = place.astype(BF16)
    place_out[...] = place
    channels = rows.shape[1]
    sent[:, :slots, :] = dot(place, rows[...], 1, 0).astype(BF16).reshape(experts, slots, channels)
    routed = (weight * dot(place, cotangent[...], 1, 0)).astype(BF16)
    sent[:, slots:, :] = routed.reshape(experts, slots, channels)


def send_rows(routes, weights, rows, cotangent, experts, slots):
    tokens, channels = rows.shape
    return pl.pallas_call(
        functools.partial(send_body, experts=experts, slots=slots),
        in_specs=whole(4),
        out_specs=whole(2),
        out_shape=(
            jax.ShapeDtypeStruct((experts, 2 * slots, channels), BF16),
            jax.ShapeDtypeStruct((experts * slots, tokens), BF16),
        ),
        name="send_rows",
    )(routes, weights, rows, cotangent)


def rim_body(routes, place_out, *, experts, slots):
    place, _ = places(routes, None, experts, slots)
    place_out[...] = place.astype(BF16)


def rim_places(routes, experts, slots):
    return pl.pallas_call(
        functools.partial(rim_body, experts=experts, slots=slots),
        in_specs=whole(1),
        out_specs=whole(1)[0],
        out_shape=pltpu.VMEM((experts * slots, routes.shape[1]), BF16),
        compiler_params=pltpu.CompilerParams(vmem_limit_bytes=12 * 1024 * 1024),
        name="rim_places",
    )(routes)


def summed_body(arrived, out):
    experts, both, width = out.shape
    total = functools.reduce(jnp.add, [part[...].astype(F32) for part in [arrived.at[k] for k in range(arrived.shape[0])]])
    spread = used_slots(experts, both // 2, 1)
    total = dot(spread, total.astype(BF16), 1, 0).astype(BF16).reshape(experts, both // 2, width)
    out[:, : both // 2, :] = total
    out[: experts - 1, both // 2 :, :] = total[1:]
    out[experts - 1 :, both // 2 :, :] = total[:1]


def summed(arrived, experts):
    _, count, width = arrived.shape
    return pl.pallas_call(
        summed_body,
        in_specs=whole(1),
        out_specs=whole(1)[0],
        out_shape=pltpu.VMEM((experts, 2 * (count // experts + 1), width), BF16),
        compiler_params=pltpu.CompilerParams(vmem_limit_bytes=12 * 1024 * 1024),
        name="summed",
    )(arrived)


def combined_body(returned, place, rim_place, cotangent, rim_cotangent, out, own_out):
    _, both, width = returned.shape
    tokens = cotangent.shape[0]
    mine = returned[:, : both // 2, :].reshape(-1, width)
    after = returned[:, both // 2 :, :].reshape(-1, width)
    own = (cotangent[...].astype(F32) + dot(place[...], mine, 0, 0)).astype(BF16)
    out[:tokens, :] = own
    own_out[...] = own
    rim = rim_cotangent[...].astype(F32) + dot(rim_place[...], after, 0, 0)
    out[tokens:, :] = rim.astype(BF16)


def combined(returned, place, rim_place, cotangent, rim_cotangent):
    tokens = cotangent.shape[0] + rim_cotangent.shape[0]
    return pl.pallas_call(
        combined_body,
        in_specs=whole(5),
        out_specs=whole(2),
        out_shape=(
            pltpu.VMEM((tokens, cotangent.shape[1]), BF16),
            jax.ShapeDtypeStruct(cotangent.shape, BF16),
        ),
        compiler_params=pltpu.CompilerParams(vmem_limit_bytes=12 * 1024 * 1024),
        name="combined",
    )(returned, place, rim_place, cotangent, rim_cotangent)


def columns(chip, core, width):
    return pl.ds(pl.multiple_of((2 * chip + core) * width, width), width)


def put_blocks(me, steps, mine, others, rows, routed, blocks, slots):
    chips = blocks // 2
    width = mine[0].shape[-1]
    my_chip, my_core = (me[0] // 2, lax.rem(me[0], 2))
    found = []
    for step, part, (batch, at) in zip(steps, mine, others):
        chip = lax.rem(my_chip + step + chips, chips)
        for core, value in ((my_core, part), (1 - my_core, batch.at[at])):
            cols = columns(chip, core, width)
            rows[:, :, cols] = value[:, :slots, :]
            routed[:, :, cols] = value[:, slots:, :]
        found.append(pl.ds(pl.multiple_of(chip * 2 * width, 2 * width), 2 * width))
    return found


def products(rows, routed, weights, found):
    sums = [None] * 3
    for cols in found:
        for n, (left, weight) in enumerate(zip((rows, rows, routed), weights)):
            taken = left[..., cols].reshape(-1, cols.size)
            part = dot(taken, weight[:, cols], 1, 1)
            sums[n] = part if sums[n] is None else sums[n] + part
    return sums


def first_body(me, *refs, blocks, slots, batches):
    chips = blocks // 2
    count = sum(batches)
    mine, shared = (refs[:count], refs[count : count + len(batches)])
    weights = refs[count + len(batches) : count + len(batches) + 3]
    rows, routed, *sums, held0, held1, held2, sems, weight_sems = refs[count + len(batches) + 3 :]
    others = [(batch, at) for batch, size in zip(shared, batches) for at in range(size)]
    held = (held0, held1, held2)
    width = mine[0].shape[-1]
    my_chip, my_core = (me[0] // 2, lax.rem(me[0], 2))
    copies = [
        pltpu.make_async_copy(weight.at[0], keep, weight_sems.at[n])
        for n, (weight, keep) in enumerate(zip(weights, held))
    ]
    found = []
    for n, (step, (batch, at)) in enumerate(zip(ring_order(chips), others)):
        chip = lax.rem(my_chip + step + chips, chips)
        for i, (core, source) in enumerate(((my_core, mine[n]), (1 - my_core, batch.at[at]))):
            cols = columns(chip, core, width)
            for k, target in enumerate((rows, routed)):
                part = source.at[:, pl.ds(k * slots, slots), :]
                copies.append(pltpu.make_async_copy(part, target.at[:, :, cols], sems.at[n, i, k]))
        found.append(pl.ds(pl.multiple_of(chip * 2 * width, 2 * width), 2 * width))
    for copy in copies:
        copy.start()
    for copy in copies[:3]:
        copy.wait()
    totals = [None] * 3
    for n in range(count):
        for copy in copies[3 + 4 * n : 7 + 4 * n]:
            copy.wait()
        parts = products(rows, routed, held, found[n : n + 1])
        totals = [p if t is None else t + p for t, p in zip(totals, parts)]
    for out, value in zip(sums, totals):
        out[...] = value


def first_products(me, mine, shared, weights, slots, blocks):
    batches = [b.shape[0] for b in shared]
    experts, _, _ = mine[0].shape
    count, hidden, channels = (experts * slots, weights[0].shape[1], weights[0].shape[2])
    return pl.pallas_call(
        functools.partial(first_body, blocks=blocks, slots=slots, batches=batches),
        in_specs=whole(1, pltpu.SMEM)
        + whole(len(mine) + len(shared) + 3, pltpu.HBM),
        out_specs=whole(8),
        scratch_shapes=[
            pltpu.SemaphoreType.DMA((len(mine), 2, 2)),
            pltpu.SemaphoreType.DMA((3,)),
        ],
        out_shape=(
            *[pltpu.VMEM((experts, slots, channels), BF16)] * 2,
            *[pltpu.VMEM((count, hidden), F32)] * 3,
            *[pltpu.VMEM((hidden, channels), BF16)] * 3,
        ),
        cost_estimate=pl.CostEstimate(
            flops=4 * count * hidden * channels, transcendentals=0, bytes_accessed=12 * 1024 * 1024
        ),
        compiler_params=pltpu.CompilerParams(vmem_limit_bytes=12 * 1024 * 1024),
        name="first_products",
    )(me, *far(*mine, *shared, *weights))


def used_slots(experts, slots, row_dim):
    shape = [experts * slots] * 2
    shape[row_dim] = experts * (slots - 1)
    row = lax.broadcasted_iota(jnp.int32, shape, row_dim)
    place = lax.broadcasted_iota(jnp.int32, shape, 1 - row_dim)
    expert = place // slots
    used = (place - expert == row) & (place - expert * slots < slots - 1)
    return used.astype(F32).astype(BF16)


def partial_rows(out, gate_grad, up_grad, gate_weight, up_weight, core):
    chips, _, width = out.shape
    for j in range(0, chips, 2):
        gate_cols, up_cols = (
            jnp.concatenate([weight[:, columns(j + i, core, width)] for i in (0, 1)], axis=1)
            for weight in (gate_weight, up_weight)
        )
        both = dot(gate_grad, gate_cols, 1, 0) + dot(up_grad, up_cols, 1, 0)
        for i in (0, 1):
            out[j + i] = both[:, i * width : (i + 1) * width].astype(BF16)


def kept_body(me, gate_grad, up_grad, gate_weight, up_weight, out):
    core = lax.rem(me[0], 2)
    partial_rows(out, gate_grad[...], up_grad[...], gate_weight, up_weight, core)


def kept_products(me, gate_grad, up_grad, gate_weight, up_weight, blocks):
    count, hidden = gate_grad.shape
    channels = gate_weight.shape[1]
    return pl.pallas_call(
        kept_body,
        in_specs=whole(1, pltpu.SMEM) + whole(4),
        out_specs=whole(1)[0],
        out_shape=pltpu.VMEM((blocks // 2, count, channels // blocks), BF16),
        cost_estimate=pl.CostEstimate(
            flops=2 * count * hidden * channels, transcendentals=0, bytes_accessed=4 * 1024 * 1024
        ),
        compiler_params=pltpu.CompilerParams(vmem_limit_bytes=12 * 1024 * 1024),
        name="kept_products",
    )(me, *near(gate_grad, up_grad, gate_weight, up_weight))


def rest_body(me, *refs, blocks, slots, batches):
    chips = blocks // 2
    count = sum(batches)
    mine, shared = (refs[:count], refs[count : count + len(batches)])
    _, _, gate_sum, up_sum, down_sum, *weights = refs[count + len(batches) : count + len(batches) + 8]
    outs = refs[count + len(batches) + 8 :]
    rows, routed, given, gate_out, up_out, *far_outs = outs[:9]
    hidden_held, up_held, sems = outs[9:]
    sends = [
        pltpu.make_async_copy(held, out, sems.at[n])
        for n, (held, out) in enumerate(zip((rows, routed, hidden_held, up_held), far_outs))
    ]
    others = [(batch, at) for batch, size in zip(shared, batches) for at in range(size)]
    steps = ring_order(chips)[-count:]
    found = put_blocks(me, steps, mine, others, rows, routed, blocks, slots)
    sends[0].start()
    sends[1].start()
    gate_pre, up_pre, hidden_grad = products(rows, routed, weights, found)
    gate_pre = gate_pre + gate_sum[...]
    up_pre = up_pre + up_sum[...]
    hidden_grad = hidden_grad + down_sum[...]
    gate_weight, up_weight = weights[:2]
    my_core = lax.rem(me[0], 2)
    gate_sigmoid = jax.nn.sigmoid(gate_pre)
    gate_active = gate_pre * gate_sigmoid
    hidden_held[...] = (gate_active * up_pre).astype(BF16)
    gate_grad = (hidden_grad * up_pre * silu_slope(gate_pre, gate_sigmoid)).astype(BF16)
    up_grad = (hidden_grad * gate_active).astype(BF16)
    up_held[...] = up_grad
    sends[2].start()
    sends[3].start()
    used = used_slots(rows.shape[0], slots, 0)
    gate_rows = dot(used, gate_grad, 1, 0).astype(BF16)
    up_rows = dot(used, up_grad, 1, 0).astype(BF16)
    partial_rows(given, gate_rows, up_rows, gate_weight, up_weight, 1 - my_core)
    gate_out[...] = gate_rows
    up_out[...] = up_rows
    for send in sends:
        send.wait()


def rest_products(me, mine, shared, early, slots, blocks):
    batches = [b.shape[0] for b in shared]
    experts, _, channels = early[0].shape
    count, hidden = early[2].shape
    first = 1 + len(mine) + len(shared)
    return pl.pallas_call(
        functools.partial(rest_body, blocks=blocks, slots=slots, batches=batches),
        in_specs=whole(1, pltpu.SMEM) + whole(len(mine) + len(shared) + 8),
        out_specs=whole(5) + whole(4, pl.ANY),
        out_shape=(
            *[pltpu.VMEM((experts, slots, channels), BF16)] * 2,
            pltpu.VMEM((blocks // 2, count - experts, channels // blocks), BF16),
            *[pltpu.VMEM((count - experts, hidden), BF16)] * 2,
            *[pltpu.HBM((experts, slots, channels), BF16)] * 2,
            *[pltpu.HBM((count, hidden), BF16)] * 2,
        ),
        scratch_shapes=[pltpu.VMEM((count, hidden), BF16)] * 2 + [pltpu.SemaphoreType.DMA((4,))],
        input_output_aliases={first: 0, first + 1: 1},
        cost_estimate=pl.CostEstimate(
            flops=6 * count * hidden * channels,
            transcendentals=count * hidden,
            bytes_accessed=12 * 1024 * 1024,
        ),
        compiler_params=pltpu.CompilerParams(vmem_limit_bytes=12 * 1024 * 1024),
        name="rest_products",
    )(me, *mine, *shared, *near(*early))


def along_chips(value, steps):
    count = lax.axis_size("chip")
    return lax.ppermute(value, "chip", [(y, (y + steps) % count) for y in range(count)])


def from_after(value):
    count = lax.axis_size("sp")
    return lax.ppermute(value, "sp", [(source, source - 1) for source in range(1, count)])


def to_other_core(value):
    return lax.ppermute(value, "core", [(0, 1), (1, 0)])


def ring_order(chips):
    return [0, *[k for step in range(1, chips // 2) for k in (-step, step)], -(chips // 2)]


def all_blocks(own):
    chips = lax.axis_size("chip")
    arrived = [own]
    for n, steps in enumerate(ring_order(chips)[1:]):
        arrived.append(along_chips(arrived[max(0, n - 1)], 1 if steps < 0 else -1))
    shared, at = ([], 0)
    for size in BATCHES[:-1]:
        shared.append(to_other_core(jnp.stack(arrived[at : at + size])))
        at += size
    count = lax.axis_size(TP)
    across = [(t, ((t - 2) % count) ^ 1) for t in range(count)]
    shared.append(lax.ppermute(arrived[-2], TP, across)[None])
    return arrived, shared


def added_up(kept, other):
    both = kept.astype(F32) + other.astype(F32)
    arrived = lax.all_to_all(both.astype(BF16), "chip", split_axis=0, concat_axis=0, tiled=True)
    return arrived


def affine(value, mean, rstd, gain, shift):
    normed = (value.astype(F32) - mean[:, None]) * rstd[:, None]
    return normed, normed * gain[None, :] + shift[None, :]


def sent_to_all(value, axis):
    copies = jnp.broadcast_to(value, (lax.axis_size(axis), *value.shape))
    return lax.all_to_all(copies, axis, split_axis=0, concat_axis=0, tiled=True)


def steps(
    moe_in,
    cotangent,
    routes,
    route_weight,
    w_gate,
    w_up,
    w_down,
    conv_pre,
    norm_mean,
    norm_rstd,
    ln_gain,
    ln_shift,
    taps,
    w_proj,
):
    devices = lax.axis_size("sp")
    blocks = lax.axis_size(TP)
    local_tokens = routes.shape[0]
    channels = moe_in.shape[1]
    capacity = 5 * local_tokens // (2 * devices)
    slots = capacity + 1
    me = lax.axis_index(TP).astype(jnp.int32).reshape(1)
    sent, place = send_rows(routes.T, route_weight.T, moe_in, cotangent, devices, slots)
    own = lax.all_to_all(sent, "sp", split_axis=0, concat_axis=0, tiled=True)
    proj = sent_to_all(w_proj, "sp").reshape(-1, channels)
    mine, others = all_blocks(own)
    done = sum(BATCHES[:EARLY])
    early = first_products(me, mine[:done], others[:EARLY], (w_gate, w_up, w_down), slots, blocks)
    _, _, given, gate_rows, up_rows, rows, routed, hidden, up_grad = rest_products(
        me, mine[done:], others[EARLY:], early, slots, blocks
    )
    rim = 8 * (-(-(taps.shape[0] - 1) // 8))
    rim_cotangent, rim_pre = from_after(jnp.stack([cotangent[:rim], conv_pre[:rim]]))
    facts = [routes[:rim, 0].astype(F32), routes[:rim, 1].astype(F32)]
    facts = from_after(jnp.stack([*facts, norm_mean[:rim], norm_rstd[:rim]]))
    rim_place = rim_places(facts[:2].astype(jnp.int32), devices, slots)
    other = to_other_core(given)
    kept = kept_products(me, gate_rows, up_rows, early[5], early[6], blocks)
    shared = summed(added_up(kept, other), devices)
    returned = lax.all_to_all(shared, "sp", split_axis=0, concat_axis=0, tiled=True)
    grad_up = dot(up_grad, rows.reshape(-1, rows.shape[2]), 0, 0).astype(BF16)[None]
    grad_down = dot(hidden, routed.reshape(-1, routed.shape[2]), 0, 0).astype(BF16)[None]
    stream, grad_stream = combined(returned, place, rim_place, cotangent, rim_cotangent)
    columns = lax.all_gather(stream, TP, axis=1, tiled=True)
    own_act = affine(conv_pre, norm_mean, norm_rstd, ln_gain, ln_shift)[1]
    activated = (own_act * jax.nn.sigmoid(own_act)).astype(BF16)
    proj_part = dot(columns[:local_tokens], activated, 0, 0).astype(BF16)
    proj_part = proj_part.reshape(devices, -1, channels)
    proj_parts = lax.all_to_all(proj_part, "sp", split_axis=0, concat_axis=0, tiled=True)
    mean = jnp.concatenate([norm_mean, facts[2]])
    rstd = jnp.concatenate([norm_rstd, facts[3]])
    wide_pre = jnp.concatenate([conv_pre, rim_pre], axis=0)
    normed, pre_act = affine(wide_pre, mean, rstd, ln_gain, ln_shift)
    act_sigmoid = jax.nn.sigmoid(pre_act)
    act_grad = dot(columns, proj, 1, 0)
    normed_grad = act_grad * silu_slope(pre_act, act_sigmoid) * ln_gain[None, :]
    sums = jnp.stack([jnp.sum(normed_grad, axis=1), jnp.sum(normed_grad * normed, axis=1)])
    spare = -sums.shape[1] % 128
    sums = jnp.pad(sums, ((0, 0), (0, spare))).reshape(-1)
    sums = lax.all_gather(sums, TP, axis=0, tiled=False)
    sums = jnp.sum(sums, axis=0)
    first_sum, second_sum = sums.reshape(2, -1)[:, : local_tokens + rim]
    width = channels * blocks
    extended = rstd[:, None] * (
        normed_grad - first_sum[:, None] / width - normed * (second_sum[:, None] / width)
    )
    lag_count = taps.shape[0]
    grad_conv = jnp.zeros((local_tokens, channels), F32)
    for lag in range(lag_count):
        grad_conv = grad_conv + taps[lag][None, :] * extended[lag : lag + local_tokens]
    grad_proj = jnp.sum(proj_parts.astype(F32), axis=0)
    return (grad_up, grad_down, grad_stream, grad_proj, grad_conv.astype(BF16))


def solution(mesh):
    placed = (
        P("sp", TP),
        P("sp", TP),
        P("sp", None),
        P("sp", None),
        P("sp", TP, None),
        P("sp", TP, None),
        P("sp", TP, None),
        P("sp", TP),
        P("sp"),
        P("sp"),
        P(TP),
        P(TP),
        P(None, TP),
        P("sp", TP),
    )
    lines = jax.sharding.Mesh(
        mesh.devices.reshape(mesh.devices.shape[0], -1, 2), ("sp", "chip", "core")
    )
    return jax.shard_map(
        steps,
        mesh=lines,
        in_specs=placed,
        out_specs=(
            P("sp", TP, None),
            P("sp", TP, None),
            P("sp", TP),
            P("sp", TP),
            P("sp", TP),
        ),
        check_vma=False,
    )
```
